32 devices in a mesh: sp: 8 (over z, y), tp: 4 (over x, core).
Axes of the slice: x: 2, y: 2, z: 4, core: 2. Of those that a mesh axis runs over, the one named last changes fastest.
Arguments:
- tokens: bfloat16 [6144, 2048], P('sp'), may hold values from -6 to 6
- input_gain: bfloat16 [2048], replicated, may hold values from 0.099609375 to 1.8984375
- gate_weight: bfloat16 [2048, 2048], P('sp', 'tp'), may hold values from -0.125 to 0.125
- value_weight: bfloat16 [2048, 2048], P('sp', 'tp'), may hold values from -0.125 to 0.125
- inflow_weight: bfloat16 [2048, 4, 128], P('sp', 'tp'), may hold values from -0.125 to 0.125
- readout_weight: bfloat16 [2048, 4, 128], P('sp', 'tp'), may hold values from -0.125 to 0.125
- step_weight: bfloat16 [2048, 2, 32], P('sp', None, 'tp'), may hold values from -0.125 to 0.125
- conv_values: bfloat16 [5, 2048], P(None, 'tp'), may hold values from -2.5 to 2.5
- conv_inflow: bfloat16 [5, 4, 128], P(None, 'tp'), may hold values from -2.5 to 2.5
- conv_readout: bfloat16 [5, 4, 128], P(None, 'tp'), may hold values from -2.5 to 2.5
- log_rate: float32 [2, 6144, 32], P(None, 'sp', 'tp'), may hold values from -20 to 0
- group_gain: bfloat16 [2048], P('tp'), may hold values from 0.099609375 to 1.8984375
- query_weight: bfloat16 [2048, 2048], P('sp', 'tp'), may hold values from -8 to 8
- key_weight: bfloat16 [2048, 512], P('sp', 'tp'), may hold values from -8 to 8
- vector_weight: bfloat16 [2048, 512], P('sp', 'tp'), may hold values from -0.125 to 0.125
- sink_logit: float32 [32], P('tp'), may hold values from 3 to 7
- state_out: bfloat16 [2048, 2048], P('tp', 'sp'), may hold values from -0.125 to 0.125
- window_out: bfloat16 [2048, 2048], P('tp', 'sp'), may hold values from -1 to 1
Outputs:
- mixed: bfloat16 [6144, 2048], P('sp', 'tp')
- log_total: float32 [6144, 32], P('sp', 'tp')
The draws below stay inside these ranges and needn't reach their ends.
All inputs are finite; a program needn't handle non-finite values.
Results may differ from the reference program's by a relative error of at most 0.015.
The reference program's roundings to bfloat16 on the way count: a program that leaves them out, or rounds other values in their place, can miss the bound.
Values may be sent and summed in bfloat16 or wider, within the bound.
A program may use at most 128 MiB of HBM per device.

```python
import jax
import jax.numpy as jnp
from jax import lax

D = 2048
SSD_HEADS = 32
HEAD_DIM = 64
GROUPS = 4
STATE = 128
CONV = 5
SSD_BLOCK = 128
ATT_HEADS = 32
KV_HEADS = 8
WINDOW = 128
QBLOCK = 256
GRID_W = 64
TOK_DEV = 768
TOKENS = 6144
INNER = 2048
ATT_WIDTH = 2048
KV_WIDTH = 512
N_TP = 4


def shared_query(key):
    base = jax.random.normal(jax.random.fold_in(key, 11), (D, ATT_HEADS, HEAD_DIM), jnp.float32)
    return base * D ** (-0.5)


def draw_query_weight(key, part):
    base = jnp.clip(shared_query(key), -8.0, 8.0)
    return base.reshape(D, ATT_HEADS * HEAD_DIM).astype(jnp.bfloat16)


def draw_key_weight(key, part):
    fresh = jax.random.normal(jax.random.fold_in(key, 12), (D, KV_HEADS, HEAD_DIM), jnp.float32) * D ** (-0.5)
    return jnp.clip(fresh, -8.0, 8.0).reshape(D, KV_HEADS * HEAD_DIM).astype(jnp.bfloat16)


def draw_log_rate(key, part):
    tensor_shape = (2, TOKENS, SSD_HEADS)
    per_group = SSD_HEADS // GROUPS
    chance = 0.5
    ranking = jax.random.permutation(jax.random.fold_in(key, 20), GROUPS)
    quick_group = jax.random.uniform(jax.random.fold_in(key, 21), (GROUPS,), jnp.float32) < chance
    quick_group = jnp.where(ranking == 0, True, jnp.where(ranking == 1, False, quick_group))
    quick_level = jnp.broadcast_to(jnp.repeat(quick_group, per_group)[None, None, :], (2, 1, SSD_HEADS))
    fast_level = jnp.log(jax.random.uniform(jax.random.fold_in(key, 22), (2, 1, SSD_HEADS), jnp.float32, 1.0 / 100.0, 1.0 / 40.0))
    slow_level = jnp.log(jax.random.uniform(jax.random.fold_in(key, 23), (2, 1, SSD_HEADS), jnp.float32, 0.3, 1.5) / TOKENS)
    depth_level = jnp.where(quick_level, fast_level, slow_level)
    blocks = TOKENS // TOK_DEV
    offset_shift = jax.random.uniform(jax.random.fold_in(key, 24), (2, blocks, 1, SSD_HEADS), jnp.float32, -0.7, 0.7)
    offset_shift = jnp.broadcast_to(offset_shift, (2, blocks, TOK_DEV, SSD_HEADS)).reshape(tensor_shape)
    coarse_rough = jax.random.uniform(jax.random.fold_in(key, 25), tensor_shape, jnp.float32, -0.3, 0.3)
    label_marks = jax.random.randint(jax.random.fold_in(key, 26), (1, TOKENS, 1), 0, TOKENS) < 6
    spike_amount = jnp.log(jax.random.uniform(jax.random.fold_in(key, 27), tensor_shape, jnp.float32, 0.3, 1.0))
    final_result = jnp.where(label_marks & jnp.logical_not(quick_level), spike_amount, depth_level + offset_shift + coarse_rough)
    return jnp.clip(final_result, -20.0, 0.0)


def steps_of(own_key, dims, split, least, top_value):
    def one(axis_at, shards_of):
        draws = jax.random.uniform(jax.random.fold_in(jax.random.fold_in(own_key, 6), axis_at), (shards_of,), jnp.float32, least / len(split), top_value / len(split))
        return jnp.repeat(jnp.exp(draws), dims[axis_at] // shards_of).reshape((-1,) + (1,) * (len(dims) - axis_at - 1))

    factor_of = one(*split[0])
    for cut in split[1:]:
        factor_of = factor_of * one(*cut)
    return factor_of


def centred(key, shape, scale, bound, shards=(), kind=jnp.bfloat16):
    factor_of = steps_of(key, shape, shards, -0.22, 0.18) if shards else 1.0
    array = jax.random.normal(key, shape, jnp.float32) * scale * factor_of
    return jnp.minimum(jnp.maximum(array, -bound), bound).astype(kind)


def setup_inputs(seed: int = 0) -> dict:
    key_list = jax.random.split(jax.random.key(seed), 19)
    tokens = centred(key_list[0], (TOKENS, D), 1.0, 6.0, ((0, 8),))
    input_gain = jnp.clip(1.0 + 0.18 * jax.random.normal(key_list[1], (D,), jnp.float32), 0.099609375, 1.8984375).astype(jnp.bfloat16)
    gate_weight = centred(key_list[2], (D, INNER), D ** -0.5, 0.125, ((0, 8), (1, 4)))
    value_weight = centred(key_list[3], (D, INNER), D ** -0.5, 0.125, ((0, 8), (1, 4)))
    inflow_weight = centred(key_list[4], (D, GROUPS, STATE), D ** -0.5, 0.125, ((0, 8), (1, 4)))
    readout_weight = centred(key_list[5], (D, GROUPS, STATE), D ** -0.5, 0.125, ((0, 8), (1, 4)))
    step_weight = centred(key_list[6], (D, 2, SSD_HEADS), D ** -0.5, 0.125, ((0, 8), (2, 4)))
    conv_values = centred(key_list[7], (CONV, INNER), CONV ** -0.5, 2.5, ((1, 4),))
    conv_inflow = centred(key_list[8], (CONV, GROUPS, STATE), CONV ** -0.5, 2.5, ((1, 4),))
    conv_readout = centred(key_list[9], (CONV, GROUPS, STATE), CONV ** -0.5, 2.5, ((1, 4),))
    log_rate = draw_log_rate(jax.random.fold_in(key_list[18], 71), 0)
    group_gain = jnp.clip(1.0 + 0.18 * jax.random.normal(key_list[11], (INNER,), jnp.float32), 0.099609375, 1.8984375).astype(jnp.bfloat16)
    query_weight = draw_query_weight(jax.random.fold_in(key_list[18], 71), 0)
    key_weight = draw_key_weight(jax.random.fold_in(key_list[18], 71), 0)
    vector_weight = centred(key_list[14], (D, KV_WIDTH), D ** -0.5, 0.125, ((0, 8), (1, 4)))
    sink_logit = jnp.clip(3.0 + 4.0 * jax.random.uniform(key_list[15], (ATT_HEADS,), jnp.float32) ** steps_of(key_list[15], (ATT_HEADS,), ((0, 4),), -0.2, 0.2), 3.0, 7.0)
    state_out = centred(key_list[16], (INNER, D), INNER ** -0.5, 0.125, ((0, 4), (1, 8)))
    window_out = centred(key_list[17], (ATT_WIDTH, D), (ATT_WIDTH // 64) ** -0.5, 1.0, ((0, 4), (1, 8)))
    return {"tokens": tokens, "input_gain": input_gain, "gate_weight": gate_weight, "value_weight": value_weight, "inflow_weight": inflow_weight, "readout_weight": readout_weight, "step_weight": step_weight, "conv_values": conv_values, "conv_inflow": conv_inflow, "conv_readout": conv_readout, "log_rate": log_rate, "group_gain": group_gain, "query_weight": query_weight, "key_weight": key_weight, "vector_weight": vector_weight, "sink_logit": sink_logit, "state_out": state_out, "window_out": window_out}


EPS = 1e-06
ROPE_BASE = 10000.0
HIGH = lax.Precision.HIGH

def rope_pairs(part, angle):
    half = part.shape[-1] // 2
    cosine = jnp.cos(angle)[:, None, :]
    sine = jnp.sin(angle)[:, None, :]
    first = part[..., :half]
    second = part[..., half:]
    return jnp.concatenate([first * cosine - second * sine, second * cosine + first * sine], axis=-1)

def axial_rope(heads, positions):
    width = heads.shape[-1]
    quarter = width // 4
    freqs = ROPE_BASE ** (-jnp.arange(quarter).astype(jnp.float32) / quarter)
    row_angle = (positions // GRID_W).astype(jnp.float32)[:, None] * freqs
    col_angle = (positions % GRID_W).astype(jnp.float32)[:, None] * freqs
    half = width // 2
    wide = heads.astype(jnp.float32)
    turned = jnp.concatenate([rope_pairs(wide[..., :half], row_angle), rope_pairs(wide[..., half:], col_angle)], axis=-1)
    return turned.astype(jnp.bfloat16)

def block_ssd(state, inputs):
    xdt, decay, inflow, readout = inputs
    length = decay.shape[0]
    heads = xdt.shape[1]
    groups = inflow.shape[1]
    repeat = heads // groups
    cum = jnp.cumsum(decay, axis=0)
    seg = cum[:, None, :] - cum[None, :, :]
    lower = jnp.arange(length)[:, None] >= jnp.arange(length)[None, :]
    weight = jnp.exp(jnp.where(lower[:, :, None], seg, -jnp.inf))
    intersection = jnp.einsum('lgn,sgn->lsg', readout.astype(jnp.bfloat16), inflow.astype(jnp.bfloat16), preferred_element_type=jnp.float32)
    intersection = jnp.repeat(intersection, repeat, axis=2)
    final_result = jnp.einsum('lsh,shp->lhp', intersection * weight, xdt, precision=HIGH)
    read_heads = jnp.repeat(readout, repeat, axis=1)
    final_result = final_result + jnp.exp(cum)[:, :, None] * jnp.einsum('lhn,hpn->lhp', read_heads, state, precision=HIGH)
    write_heads = jnp.repeat(inflow, repeat, axis=1)
    to_end = jnp.exp(cum[-1][None, :] - cum)
    fresh = jnp.einsum('shp,shn->hpn', xdt * to_end[:, :, None], write_heads, precision=HIGH)
    return (jnp.exp(cum[-1])[:, None, None] * state + fresh, final_result)

def run_blocks(xdt, decay, inflow, readout):
    count = decay.shape[0]
    blocks = count // SSD_BLOCK
    start_state = jnp.zeros((SSD_HEADS, HEAD_DIM, STATE), jnp.float32)
    shaped = (xdt.reshape(blocks, SSD_BLOCK, SSD_HEADS, HEAD_DIM), decay.reshape(blocks, SSD_BLOCK, SSD_HEADS), inflow.reshape(blocks, SSD_BLOCK, GROUPS, STATE), readout.reshape(blocks, SSD_BLOCK, GROUPS, STATE))
    final_state, final_result = lax.scan(block_ssd, start_state, shaped)
    return final_result.reshape(count, SSD_HEADS, HEAD_DIM)

def reference(tokens, input_gain, gate_weight, value_weight, inflow_weight, readout_weight, step_weight, conv_values, conv_inflow, conv_readout, log_rate, group_gain, query_weight, key_weight, vector_weight, sink_logit, state_out, window_out):
    count = tokens.shape[0]
    wide = tokens.astype(jnp.float32)
    normed = (wide * lax.rsqrt(lax.optimization_barrier(jnp.mean(wide * wide, axis=1, keepdims=True)) + EPS) * input_gain.astype(jnp.float32)).astype(jnp.bfloat16)

    def project(weight):
        return jnp.dot(normed, weight.reshape(weight.shape[0], -1), preferred_element_type=jnp.float32)
    gate = project(gate_weight).astype(jnp.bfloat16)
    conv_input = jnp.concatenate([project(value_weight), project(inflow_weight), project(readout_weight)], axis=1).astype(jnp.bfloat16)
    step = jax.nn.softplus(project(step_weight)).reshape(count, 2, SSD_HEADS)
    taps = jnp.concatenate([conv_values, conv_inflow.reshape(CONV, -1), conv_readout.reshape(CONV, -1)], axis=1).astype(jnp.float32)
    reach = CONV // 2
    padded = jnp.pad(conv_input.astype(jnp.float32), ((reach, reach), (0, 0)))
    conv_sum = padded[0:count] * taps[0]
    for tap in range(1, CONV):
        conv_sum = conv_sum + padded[tap:tap + count] * taps[tap]
    conv_out = lax.optimization_barrier(jax.nn.silu(conv_sum).astype(jnp.bfloat16)).astype(jnp.float32)
    xs = conv_out[:, :INNER].reshape(count, SSD_HEADS, HEAD_DIM)
    inflow = conv_out[:, INNER:INNER + GROUPS * STATE].reshape(count, GROUPS, STATE)
    readout = conv_out[:, INNER + GROUPS * STATE:].reshape(count, GROUPS, STATE)
    decay = -jnp.exp(log_rate) * jnp.transpose(step, (1, 0, 2))
    forward = run_blocks(xs * step[:, 0, :, None], decay[0], inflow, readout)
    backward = jnp.flip(run_blocks(jnp.flip(xs * step[:, 1, :, None], 0), jnp.flip(decay[1], 0), jnp.flip(inflow, 0), jnp.flip(readout, 0)), 0)
    combined = (forward + backward).reshape(count, INNER) * jax.nn.silu(gate.astype(jnp.float32))
    grouped = combined.reshape(count, GROUPS, -1)
    grouped = grouped * lax.rsqrt(lax.optimization_barrier(jnp.mean(grouped * grouped, axis=2, keepdims=True)) + EPS)
    state_features = (grouped.reshape(count, INNER) * group_gain.astype(jnp.float32)).astype(jnp.bfloat16)
    repeat = ATT_HEADS // KV_HEADS
    positions = jnp.arange(count, dtype=jnp.int32)
    queries = axial_rope(project(query_weight).astype(jnp.bfloat16).reshape(count, ATT_HEADS, HEAD_DIM), positions)
    keys = axial_rope(project(key_weight).astype(jnp.bfloat16).reshape(count, KV_HEADS, HEAD_DIM), positions)
    vectors = project(vector_weight).astype(jnp.bfloat16).reshape(count, KV_HEADS, HEAD_DIM)
    key_pad = jnp.pad(keys, ((WINDOW, WINDOW), (0, 0), (0, 0)))
    vector_pad = jnp.pad(vectors, ((WINDOW, WINDOW), (0, 0), (0, 0)))
    grouped_q = queries.reshape(count, KV_HEADS, repeat, HEAD_DIM)
    band = QBLOCK + 2 * WINDOW
    sinks = sink_logit.reshape(KV_HEADS, repeat, 1, 1)

    def attend(index):
        start = (index * QBLOCK).astype(jnp.int32)
        block_q = lax.dynamic_slice_in_dim(grouped_q, start, QBLOCK, 0).astype(jnp.float32)
        block_k = lax.dynamic_slice_in_dim(key_pad, start, band, 0).astype(jnp.float32)
        block_v = lax.dynamic_slice_in_dim(vector_pad, start, band, 0).astype(jnp.float32)
        scores = jnp.einsum('qkrd,skd->krqs', block_q, block_k) * HEAD_DIM ** (-0.5)
        query_pos = start + jnp.arange(QBLOCK, dtype=jnp.int32)
        key_pos = start - WINDOW + jnp.arange(band, dtype=jnp.int32)
        valid = (jnp.abs(query_pos[:, None] - key_pos[None, :]) <= WINDOW) & (key_pos >= 0)[None, :] & (key_pos < count)[None, :]
        scores = jnp.where(valid, scores, -jnp.inf)
        top = jnp.maximum(lax.optimization_barrier(jnp.max(scores, axis=-1, keepdims=True)), sinks)
        expo = jnp.exp(scores - top)
        total = lax.optimization_barrier(jnp.sum(expo, axis=-1, keepdims=True)) + jnp.exp(sinks - top)
        probs = lax.optimization_barrier(expo.astype(jnp.bfloat16)).astype(jnp.float32)
        values = jnp.einsum('krqs,skd->qkrd', probs, block_v) / jnp.transpose(total, (2, 0, 1, 3))
        logs = jnp.transpose((top + jnp.log(total))[..., 0], (2, 0, 1)).reshape(QBLOCK, -1)
        return (values.astype(jnp.bfloat16).reshape(QBLOCK, -1), logs)
    feats, logs = lax.map(attend, jnp.arange(count // QBLOCK, dtype=jnp.int32))
    window_features = feats.reshape(count, ATT_WIDTH)
    log_total = logs.reshape(count, ATT_HEADS)
    state_cols = INNER // N_TP
    window_cols = ATT_WIDTH // N_TP
    summed = jnp.zeros((count, D), jnp.float32)
    for group in range(N_TP):
        part = jnp.dot(state_features[:, group * state_cols:(group + 1) * state_cols], state_out[group * state_cols:(group + 1) * state_cols], preferred_element_type=jnp.float32)
        part = part + jnp.dot(window_features[:, group * window_cols:(group + 1) * window_cols], window_out[group * window_cols:(group + 1) * window_cols], preferred_element_type=jnp.float32)
        summed = summed + lax.optimization_barrier(part.astype(jnp.bfloat16)).astype(jnp.float32)
    return (summed.astype(jnp.bfloat16), log_total)
```

```python
import functools

import jax
import jax.numpy as jnp
import numpy as np
from jax import lax
from jax.experimental import pallas as pl
from jax.experimental.pallas import tpu as pltpu
from jax.sharding import PartitionSpec as P


HEAD_DIM = 64
CONV = 5
SSD_BLOCK = 128
WINDOW = 128
GRID_W = 64


EPS = 1e-06
ROPE_BASE = 10000.0
HIGHEST = lax.Precision.HIGHEST
F32 = jnp.float32
BF16 = jnp.bfloat16
PAD = 16


def iota(shape, dim):
    return lax.broadcasted_iota(jnp.int32, shape, dim)


def exact(a, b):
    return jnp.dot(a, b, precision=HIGHEST, preferred_element_type=F32)


def spread(heads):
    shape = (heads, heads * HEAD_DIM)
    return (iota(shape, 1) // HEAD_DIM == iota(shape, 0)).astype(F32)


def inner_t(a, b):
    return lax.dot_general(a, b, (((1,), (1,)), ((), ())), preferred_element_type=F32)


def outer_t(a, b):
    return lax.dot_general(a, b, (((0,), (0,)), ((), ())), preferred_element_type=F32)


def summary_kernel(cells_ref, sd_ref, out_ref):
    count = cells_ref.shape[0]
    heads = sd_ref.shape[1] // 4
    wide = heads * HEAD_DIM
    state = out_ref.shape[1] - PAD
    x = cells_ref[:, :wide].astype(F32)
    writes = cells_ref[:, wide : wide + state]
    expand = spread(heads)
    row = iota((count, count), 0)
    col = iota((count, count), 1)
    for e in range(2):
        step = sd_ref[:, e * heads : (e + 1) * heads]
        decay = sd_ref[:, (2 + e) * heads : (3 + e) * heads]
        span = (col > row) if e == 0 else (col < row)
        rest = exact(span.astype(F32), decay)
        scaled = (x * exact(jnp.exp(rest) * step, expand)).astype(BF16)
        out_ref[e, :state, :] = outer_t(writes, scaled).astype(BF16)
        total = exact(jnp.broadcast_to(jnp.sum(decay, axis=0, keepdims=True), (8, heads)), expand)
        total = total[0:1]
        high = total.astype(BF16).astype(F32)
        place = iota((PAD, wide), 0)
        packed = jnp.where(place == 0, high, jnp.where(place == 1, total - high, 0.0))
        out_ref[e, state:, :] = packed.astype(BF16)


def mixer_kernel(cells_ref, sd_ref, sdt_ref, start_ref, gate_ref, gain_ref, out_ref, back_ref, carry_ref):
    blocks, _, size = sdt_ref.shape
    heads = sd_ref.shape[1] // 4
    wide = heads * HEAD_DIM
    state = start_ref.shape[1]
    expand = spread(heads)
    row = iota((size, size), 0)
    col = iota((size, size), 1)
    lower = (row >= col).astype(F32)
    upper = (row <= col).astype(F32)

    carry_ref[...] = start_ref[1]

    def backward(index, _):
        block = blocks - 1 - index
        rows = pl.ds(pl.multiple_of(block * size, size), size)
        back_ref[block] = carry_ref[...].astype(BF16)
        step = sd_ref[rows, heads : 2 * heads]
        cum = exact(upper, sd_ref[rows, 3 * heads : 4 * heads])
        edge = cum[0:1]
        x = cells_ref[rows, :wide].astype(F32)
        scaled = (x * exact(jnp.exp(edge - cum) * step, expand)).astype(BF16)
        fresh = outer_t(cells_ref[rows, wide : wide + state], scaled)
        fade = exact(jnp.broadcast_to(jnp.exp(edge), (8, heads)), expand)[0:1]
        carry_ref[...] = fade * carry_ref[...] + fresh
        return 0

    lax.fori_loop(0, blocks, backward, 0)
    carry_ref[...] = start_ref[0]

    def forward(block, _):
        rows = pl.ds(pl.multiple_of(block * size, size), size)
        cum_f = exact(lower, sd_ref[rows, 2 * heads : 3 * heads])
        cum_b = exact(upper, sd_ref[rows, 3 * heads : 4 * heads])
        flat = sdt_ref[block]
        step_ft = flat[:heads]
        step_bt = flat[heads : 2 * heads]
        cum_ft = exact(flat[2 * heads : 3 * heads], upper)
        cum_bt = exact(flat[3 * heads :], lower)
        x = cells_ref[rows, :wide]
        writes = cells_ref[rows, wide : wide + state]
        reads = cells_ref[rows, wide + state :]
        cross = inner_t(reads, writes)
        parts = []
        for h in range(heads):
            one = slice(h, h + 1)
            seg = jnp.where(
                row >= col, cum_f[:, one] - cum_ft[one], cum_b[:, one] - cum_bt[one]
            )
            scale = jnp.where(
                row > col,
                step_ft[one],
                jnp.where(row < col, step_bt[one], step_ft[one] + step_bt[one]),
            )
            weight = (cross * jnp.exp(seg) * scale).astype(BF16)
            parts.append(
                jnp.dot(
                    weight, x[:, h * HEAD_DIM : (h + 1) * HEAD_DIM], preferred_element_type=F32
                )
            )
        y = jnp.concatenate(parts, axis=1)
        y = y + exact(jnp.exp(cum_f), expand) * jnp.dot(
            reads, carry_ref[...].astype(BF16), preferred_element_type=F32
        )
        y = y + exact(jnp.exp(cum_b), expand) * jnp.dot(
            reads, back_ref[block], preferred_element_type=F32
        )
        gate = gate_ref[rows, :].astype(F32)
        y = y * (gate * jax.nn.sigmoid(gate))
        y = y * lax.rsqrt(jnp.mean(y * y, axis=1, keepdims=True) + EPS)
        out_ref[rows, :] = (y * gain_ref[...].astype(F32)).astype(BF16)
        edge = cum_f[size - 1 : size]
        step = sd_ref[rows, :heads]
        scaled = (x.astype(F32) * exact(jnp.exp(edge - cum_f) * step, expand)).astype(BF16)
        fade = exact(jnp.broadcast_to(jnp.exp(edge), (8, heads)), expand)[0:1]
        carry_ref[...] = fade * carry_ref[...] + outer_t(writes, scaled)
        return 0

    lax.fori_loop(0, blocks, forward, 0)


def attend_kernel(place_ref, sink_ref, q_ref, kv_ref, turn_ref, swap_ref, out_ref, log_ref, keys_ref):
    count = q_ref.shape[0]
    q_count = q_ref.shape[1] // HEAD_DIM
    kv_width = kv_ref.shape[1] // 2
    repeat = q_count * HEAD_DIM // kv_width
    size = SSD_BLOCK
    band = size + 2 * WINDOW
    swap = swap_ref[...]

    def turned(part, rows):
        swapped = jnp.dot(part, swap, preferred_element_type=F32)
        table = turn_ref[rows, :]
        return (part.astype(F32) * table[:, :HEAD_DIM] + swapped * table[:, HEAD_DIM:]).astype(BF16)

    def prepare(block, _):
        rows = pl.ds(pl.multiple_of(block * size, size), size)
        for g in range(kv_width // HEAD_DIM):
            keys_ref[g, rows, :] = turned(
                kv_ref[rows, g * HEAD_DIM : (g + 1) * HEAD_DIM], rows
            )
        return 0

    lax.fori_loop(0, kv_ref.shape[0] // size, prepare, 0)
    row = iota((size, band), 0)
    col = iota((size, band), 1)
    near = (col >= row) & (col - row <= 2 * WINDOW)
    lane = iota((size, q_count), 1)

    def one(block, _):
        start = pl.multiple_of(block * size, size)
        rows = pl.ds(start, size)
        reach = pl.ds(start, band)
        key_pos = place_ref[0] + start - WINDOW + col
        valid = near & (key_pos >= 0) & (key_pos < place_ref[1])
        logs = jnp.zeros((size, q_count), F32)
        outs = []
        for h in range(q_count):
            g = h // repeat
            query = turned(
                q_ref[rows, h * HEAD_DIM : (h + 1) * HEAD_DIM], pl.ds(start + WINDOW, size)
            )
            scores = inner_t(query, keys_ref[g, reach, :]) * HEAD_DIM ** (-0.5)
            scores = jnp.where(valid, scores, -jnp.inf)
            sink = sink_ref[h]
            top = jnp.maximum(jnp.max(scores, axis=1, keepdims=True), sink)
            expo = jnp.exp(scores - top)
            total = jnp.sum(expo, axis=1, keepdims=True) + jnp.exp(sink - top)
            first = kv_width + g * HEAD_DIM
            values = jnp.dot(
                expo.astype(BF16),
                kv_ref[reach, first : first + HEAD_DIM],
                preferred_element_type=F32,
            )
            outs.append((values / total).astype(BF16))
            logs = jnp.where(lane == h, top + jnp.log(total), logs)
        out_ref[rows, :] = jnp.concatenate(outs, axis=1)
        log_ref[rows, :] = logs
        return 0

    lax.fori_loop(0, count // size, one, 0)


def call(kernel, out_shape, args, scratch=(), scalars=0, flops=10**8):
    vmem = pl.BlockSpec(memory_space=pltpu.VMEM)
    smem = pl.BlockSpec(memory_space=pltpu.SMEM)
    return pl.pallas_call(
        kernel,
        out_shape=out_shape,
        in_specs=[smem] * scalars + [vmem] * (len(args) - scalars),
        out_specs=jax.tree.map(lambda _: vmem, out_shape),
        scratch_shapes=list(scratch),
        cost_estimate=pl.CostEstimate(flops=flops, bytes_accessed=4 * 10**6, transcendentals=0),
        compiler_params=pltpu.CompilerParams(vmem_limit_bytes=40 * 2**20),
    )(*args)


def with_halo(cells, sides, width):
    for axis, dim in sides:
        count = lax.axis_size(axis)
        ends = count - 1
        head = lax.slice_in_dim(cells, 0, width, axis=dim)
        tail = lax.slice_in_dim(cells, cells.shape[dim] - width, cells.shape[dim], axis=dim)
        cells = jnp.concatenate(
            [
                lax.ppermute(tail, axis, [(i, (i + 1) % count) for i in range(ends)]),
                cells,
                lax.ppermute(head, axis, [((i + 1) % count, i) for i in range(ends)]),
            ],
            axis=dim,
        )
    return cells


def flatten_rows(weight):
    return weight.reshape(weight.shape[0], -1)


TILE = 128
GROUP = 3


def split3(v):
    high = v.astype(BF16)
    rest = v - high.astype(F32)
    mid = rest.astype(BF16)
    return high, mid, (rest - mid.astype(F32)).astype(BF16)


def through(left, right, left_wide):
    total = None
    for part in split3(left if left_wide else right):
        one = jnp.dot(part, right, preferred_element_type=F32) if left_wide else jnp.dot(
            left, part, preferred_element_type=F32
        )
        total = one if total is None else total + one
    return total


def chunk_maps(shapes):
    rows = shapes["value"][0]

    def tiles(name):
        return [(name, 0, c) for c in range(shapes[name][1] // TILE)]

    units = ([], [])
    for names in (("value", "inflow", "readout"), ("query", "key", "vector"), ("gate",)):
        flat = [t for name in names for t in tiles(name)]
        half = len(flat) // 2
        for d in range(2):
            units[d].extend(flat[d * half : (d + 1) * half])
    for d in range(2):
        for name in ("state_out", "window_out"):
            units[d].extend((name, r, d) for r in range(shapes[name][0] // rows))
    return units


def layer_kernel(
    cfg,
    tokens_ref,
    gain_ref,
    taps_ref,
    rates_ref,
    norm_gain_ref,
    sink_ref,
    row_turn_ref,
    col_turn_ref,
    steps_ref,
    value_ref,
    inflow_ref,
    readout_ref,
    query_ref,
    key_ref,
    vector_ref,
    gate_w_ref,
    state_out_ref,
    window_out_ref,
    out_ref,
    log_ref,
    ring_ref,
    steps_all_ref,
    normed_ref,
    conv_ref,
    cells_ref,
    step_ref,
    decay_ref,
    cum_ref,
    entry_ref,
    before_ref,
    carry_ref,
    total_ref,
    scan_send_ref,
    scan_recv_ref,
    start_ref,
    reach_ref,
    gate_ref,
    q_ref,
    kv_ref,
    keys_ref,
    turn_ref,
    feat_ref,
    part_ref,
    peer_ref,
    send_sem,
    recv_sem,
    steps_send,
    steps_recv,
    local_sem,
    halo_send,
    halo_recv,
    kv_send,
    kv_recv,
    scan_ssem,
    scan_rsem,
    out_send,
    out_recv,
):
    seats, peers, units = cfg
    count, _ = tokens_ref.shape
    unit_rows = ring_ref.shape[3]
    heads = steps_ref.shape[0] // 2
    wide = heads * HEAD_DIM
    state = inflow_ref.shape[1]
    conv_width = wide + 2 * state
    q_width = query_ref.shape[1]
    q_count = q_width // HEAD_DIM
    kv_width = key_ref.shape[1]
    per_dir = len(units[0])
    hops = seats - 1
    sends = per_dir * hops
    place = lax.axis_index("sp")
    lane_peer = lax.axis_index("tp")
    half = seats // 2
    blocks = count // SSD_BLOCK
    size = SSD_BLOCK
    mesh_id = pl.DeviceIdType.MESH

    def seat_at(pos):
        pos = lax.rem(pos + 2 * seats, seats)
        late = lax.div(pos, half)
        return (1 - late) * 2 * pos + late * (2 * (seats - 1 - pos) + 1)

    odd = lax.rem(place, 2)
    my_pos = (1 - odd) * lax.div(place, 2) + odd * (seats - 1 - lax.div(place, 2))
    nexts = (seat_at(my_pos + 1), seat_at(my_pos - 1))

    barrier = pltpu.get_barrier_semaphore()
    for r in range(1, seats):
        pl.semaphore_signal(
            barrier, inc=1, device_id={"sp": lax.rem(place + r, seats)}, device_id_type=mesh_id
        )
    for r in range(1, peers):
        pl.semaphore_signal(
            barrier, inc=1, device_id={"tp": lax.rem(lane_peer + r, peers)}, device_id_type=mesh_id
        )

    sources = {
        "value": value_ref,
        "inflow": inflow_ref,
        "readout": readout_ref,
        "query": query_ref,
        "key": key_ref,
        "vector": vector_ref,
        "gate": gate_w_ref,
        "state_out": state_out_ref,
        "window_out": window_out_ref,
    }
    locals_ = []
    for d in range(2):
        for u, (name, r, c) in enumerate(units[d]):
            locals_.append(
                pltpu.make_async_copy(
                    sources[name].at[pl.ds(r * unit_rows, unit_rows), pl.ds(c * TILE, TILE)],
                    ring_ref.at[d, u, place],
                    local_sem.at[d * per_dir + u],
                )
            )
    for copy in locals_:
        copy.start()
    steps_all_ref[place] = steps_ref[...]
    for copy in locals_:
        copy.wait()
    pl.semaphore_wait(barrier, hops + peers - 1)

    def ring_copy(i, d, behind):
        turn = lax.div(i, GROUP * hops)
        k = lax.rem(lax.div(i, GROUP), hops) + behind
        unit = GROUP * turn + lax.rem(i, GROUP)
        owner = seat_at(my_pos - k) if d == 0 else seat_at(my_pos + k)
        block = ring_ref.at[d, unit, owner]
        return pltpu.make_async_remote_copy(
            src_ref=block,
            dst_ref=block,
            send_sem=send_sem.at[d, i],
            recv_sem=recv_sem.at[d, i],
            device_id={"sp": nexts[d]},
            device_id_type=mesh_id,
        )

    def tick(i, last=False):
        for d in range(2):
            ring_copy(i, d, 1).wait_recv()
            if not last:
                ring_copy(i + GROUP, d, 0).start()

    for j in range(GROUP):
        for d in range(2):
            ring_copy(jnp.int32(j), d, 0).start()

    def steps_copy(r):
        return pltpu.make_async_remote_copy(
            src_ref=steps_ref,
            dst_ref=steps_all_ref.at[place],
            send_sem=steps_send.at[r],
            recv_sem=steps_recv.at[place],
            device_id={"sp": lax.rem(place + r, seats)},
            device_id_type=mesh_id,
        )

    for r in range(1, seats):
        steps_copy(r).start()

    clock = [0]

    def sweep(trips, per_trip, body):
        base = clock[0]

        def run(i, _):
            for j in range(per_trip):
                tick(base + i * per_trip + j)
            body(i)
            return 0

        lax.fori_loop(0, trips, run, 0)
        clock[0] = base + trips * per_trip

    def until(goal):
        if goal > clock[0]:
            sweep(goal - clock[0], 1, lambda i: None)

    def rows_at(index, length, first=0):
        return pl.ds(pl.multiple_of(index * length, length) + first, length)

    def normalise(b):
        rows = rows_at(b, size)
        x = tokens_ref[rows, :].astype(F32)
        scale = lax.rsqrt(jnp.mean(x * x, axis=1, keepdims=True) + EPS)
        normed_ref[rows, :] = (x * scale * gain_ref[...].astype(F32)).astype(BF16)

    sweep(blocks, 0, normalise)
    table_row = place * (count // GRID_W)

    def fill_turn(i):
        turn_ref[rows_at(i, GRID_W), :] = col_turn_ref[...] + row_turn_ref[pl.ds(table_row + i, 1), :]

    sweep(turn_ref.shape[0] // GRID_W, 0, fill_turn)
    step_ref[...] = jnp.zeros_like(step_ref)
    carry_ref[...] = jnp.zeros_like(carry_ref)
    total_ref[...] = jnp.zeros_like(total_ref)
    start_ref[...] = jnp.zeros_like(start_ref)
    reach_ref[...] = jnp.zeros_like(reach_ref)

    first_edge = place == 0
    last_edge = place == seats - 1

    @pl.when(first_edge)
    def _():
        conv_ref[:PAD, :] = jnp.zeros((PAD, conv_width), BF16)
        kv_ref[:WINDOW, :] = jnp.zeros((WINDOW, 2 * kv_width), BF16)

    @pl.when(last_edge)
    def _():
        conv_ref[PAD + count :, :] = jnp.zeros((PAD, conv_width), BF16)
        kv_ref[WINDOW + count :, :] = jnp.zeros((WINDOW, 2 * kv_width), BF16)

    def weights(d, first, last):
        return jnp.concatenate(
            [ring_ref[d, u].reshape(seats * unit_rows, TILE) for u in range(first, last)], axis=1
        )

    first_units = conv_width // (2 * TILE)
    second_units = (q_width + 2 * kv_width) // (2 * TILE)
    gate_units = wide // (2 * TILE)
    until(GROUP * hops * -(-first_units // GROUP))
    for r in range(1, seats):
        peer = lax.rem(place + r, seats)
        pltpu.make_async_remote_copy(
            src_ref=steps_ref,
            dst_ref=steps_all_ref.at[peer],
            send_sem=steps_send.at[r],
            recv_sem=steps_recv.at[peer],
            device_id={"sp": peer},
            device_id_type=mesh_id,
        ).wait_recv()

    dot_rows = 2 * size

    def first_dot(b):
        rows = rows_at(b, dot_rows)
        here = normed_ref[rows, :]
        for d in range(2):
            conv_ref[rows_at(b, dot_rows, PAD), d * first_units * TILE : (d + 1) * first_units * TILE] = (
                jnp.dot(here, weights(d, 0, first_units), preferred_element_type=F32).astype(BF16)
            )
        steps = jnp.concatenate([steps_all_ref[o] for o in range(seats)], axis=1)
        raw = inner_t(here, steps)
        step = jnp.maximum(raw, 0.0) + jnp.log1p(jnp.exp(-jnp.abs(raw)))
        step_ref[rows, : 2 * heads] = step

    sweep(count // dot_rows, 1, first_dot)

    def edge_copies(ref, length, ssem, rsem):
        inner = ref.shape[0] - 2 * length
        up = pltpu.make_async_remote_copy(
            src_ref=ref.at[pl.ds(inner, length)],
            dst_ref=ref.at[pl.ds(0, length)],
            send_sem=ssem.at[0],
            recv_sem=rsem.at[0],
            device_id={"sp": lax.rem(place + 1, seats)},
            device_id_type=mesh_id,
        )
        down = pltpu.make_async_remote_copy(
            src_ref=ref.at[pl.ds(length, length)],
            dst_ref=ref.at[pl.ds(length + inner, length)],
            send_sem=ssem.at[1],
            recv_sem=rsem.at[1],
            device_id={"sp": lax.rem(place + hops, seats)},
            device_id_type=mesh_id,
        )
        return up, down

    def edges_start(pair):
        pl.when(jnp.logical_not(last_edge))(lambda: pair[0].start())
        pl.when(jnp.logical_not(first_edge))(lambda: pair[1].start())

    def edges_arrive(pair):
        pl.when(jnp.logical_not(first_edge))(lambda: pair[0].wait_recv())
        pl.when(jnp.logical_not(last_edge))(lambda: pair[1].wait_recv())

    def edges_left(pair):
        pl.when(jnp.logical_not(last_edge))(lambda: pair[0].wait_send())
        pl.when(jnp.logical_not(first_edge))(lambda: pair[1].wait_send())

    conv_edges = edge_copies(conv_ref, PAD, halo_send, halo_recv)
    edges_start(conv_edges)
    decay_ref[...] = rates_ref[...] * step_ref[...]
    lane = iota((size, TILE), 1)
    row = iota((size, size), 0)
    col = iota((size, size), 1)
    lower = (row >= col).astype(BF16)
    upper = (row <= col).astype(BF16)
    spread_row = iota((TILE, wide), 0)
    spread_col = iota((TILE, wide), 1) // HEAD_DIM
    spreads = [(spread_row - e * heads == spread_col).astype(BF16) for e in range(2)]

    def sums(b):
        rows = rows_at(b, size)
        decay = decay_ref[rows, :]
        cum_ref[rows, :] = jnp.where(
            lane < heads, through(lower, decay, False), through(upper, decay, False)
        )

    sweep(blocks, 0, sums)
    edges_arrive(conv_edges)

    def convolve(b):
        rows = rows_at(b, size)
        padded = conv_ref[pl.ds(pl.multiple_of(b * size, size), size + 2 * PAD), :].astype(F32)
        first = PAD - CONV // 2
        taps = taps_ref[...].astype(F32)
        total = padded[first : first + size] * taps[0:1]
        for tap in range(1, CONV):
            total = total + padded[first + tap : first + tap + size] * taps[tap : tap + 1]
        cells_ref[rows, :] = (total * jax.nn.sigmoid(total)).astype(BF16)

    sweep(blocks, 1, convolve)

    def summarise(i):
        for e in range(2):
            b = i if e == 0 else blocks - 1 - i
            rows = rows_at(b, size)
            cum = cum_ref[rows, :]
            edge = cum[size - 1 : size] if e == 0 else cum[0:1]
            scale = through(jnp.exp(edge - cum) * step_ref[rows, :], spreads[e], True)
            scaled = (cells_ref[rows, :wide].astype(F32) * scale).astype(BF16)
            fresh = outer_t(cells_ref[rows, wide : wide + state], scaled)
            edges = through(jnp.broadcast_to(edge, (8, TILE)), spreads[e], True)
            entry_ref[e, b] = carry_ref[e]
            before_ref[e, b] = total_ref[e]
            carry_ref[e] = jnp.exp(edges[0:1]) * carry_ref[e] + fresh
            total_ref[e] = total_ref[e] + edges

    sweep(blocks, 2, summarise)

    jumps = [1]
    while sum(jumps) < hops:
        jumps.append(sum(jumps))

    def scan_copy(r, e):
        step = jumps[r] if e == 0 else seats - jumps[r]
        return pltpu.make_async_remote_copy(
            src_ref=scan_send_ref.at[e, r],
            dst_ref=scan_recv_ref.at[e, r],
            send_sem=scan_ssem.at[e, r],
            recv_sem=scan_rsem.at[e, r],
            device_id={"sp": lax.rem(place + step, seats)},
            device_id_type=mesh_id,
        )

    def sends_to(r, e):
        return place < seats - jumps[r] if e == 0 else place >= jumps[r]

    def hears_from(r, e):
        return place >= jumps[r] if e == 0 else place < seats - jumps[r]

    def scan_start(r, state_ref, decay_sum_ref):
        for e in range(2):
            scan_send_ref[e, r, :state] = state_ref[e].astype(BF16)
            total = decay_sum_ref[e][0:1]
            high = total.astype(BF16).astype(F32)
            at = iota((PAD, wide), 0)
            scan_send_ref[e, r, state:] = jnp.where(
                at == 0, high, jnp.where(at == 1, total - high, 0.0)
            ).astype(BF16)
            pl.when(sends_to(r, e))(lambda: scan_copy(r, e).start())

    def scan_take(r):
        for e in range(2):

            @pl.when(hears_from(r, e))
            def _():
                scan_copy(r, e).wait_recv()
                far = scan_recv_ref[e, r]
                decays = far[state : state + 8].astype(F32)
                far_total = decays[0:1] + decays[1:2]
                start_ref[e] = (
                    far[:state].astype(F32) * jnp.exp(reach_ref[e][0:1]) + start_ref[e]
                )
                reach_ref[e] = reach_ref[e] + far_total

    scan_start(0, carry_ref, total_ref)

    until(GROUP * hops * -(-(first_units + second_units) // GROUP))

    q_last = second_units - 2 * kv_width // TILE

    def second_dot_b(b):
        rows = rows_at(b, dot_rows)
        got = jnp.dot(
            normed_ref[rows, :],
            weights(1, first_units, first_units + second_units),
            preferred_element_type=F32,
        ).astype(BF16)
        q_ref[rows, second_units * TILE :] = got[:, : q_last * TILE]
        kv_ref[rows_at(b, dot_rows, WINDOW), :] = got[:, q_last * TILE :]

    sweep(count // dot_rows, 1, second_dot_b)
    kv_edges = edge_copies(kv_ref, WINDOW, kv_send, kv_recv)
    edges_start(kv_edges)
    scan_take(0)
    scan_start(1, start_ref, reach_ref)

    def second_dot_a(b):
        rows = rows_at(b, dot_rows)
        q_ref[rows, : second_units * TILE] = jnp.dot(
            normed_ref[rows, :],
            weights(0, first_units, first_units + second_units),
            preferred_element_type=F32,
        ).astype(BF16)

    sweep(count // dot_rows, 1, second_dot_a)

    quarter = HEAD_DIM // 4
    low = lax.rem(iota((size, TILE), 1), 2 * quarter) < quarter

    def turned(part, table):
        x = part.astype(F32)
        other = jnp.where(low, pltpu.roll(x, TILE - quarter, 1), pltpu.roll(x, quarter, 1))
        return (x * table[:, :TILE] + other * table[:, TILE:]).astype(BF16)

    edges_arrive(kv_edges)

    def prepare(b):
        rows = rows_at(b, size)
        for c in range(kv_width // TILE):
            keys_ref[rows, c * TILE : (c + 1) * TILE] = turned(
                kv_ref[rows, c * TILE : (c + 1) * TILE], turn_ref[rows, :]
            )

    sweep(kv_ref.shape[0] // size, 0, prepare)

    band = size + 2 * WINDOW
    band_row = iota((size, band), 0)
    band_col = iota((size, band), 1)
    near = (band_col >= band_row) & (band_col - band_row <= 2 * WINDOW)
    q_lane = iota((size, q_count), 1)
    repeat = q_count * HEAD_DIM // kv_width
    seq_total = seats * count
    later = [1, 3, 5]

    def attend(b):
        for r in range(1, len(jumps)):

            @pl.when(b == later[r - 1])
            def _():
                scan_take(r)
                if r + 1 < len(jumps):
                    scan_start(r + 1, start_ref, reach_ref)

        start = pl.multiple_of(b * size, size)
        rows = pl.ds(start, size)
        reach = pl.ds(start, band)
        key_pos = place * count + start - WINDOW + band_col
        valid = near & (key_pos >= 0) & (key_pos < seq_total)
        logs = jnp.zeros((size, q_count), F32)
        table = turn_ref[pl.ds(start + WINDOW, size), :]
        turned_q = jnp.concatenate(
            [turned(q_ref[rows, c * TILE : (c + 1) * TILE], table) for c in range(q_width // TILE)],
            axis=1,
        )
        outs = []
        for h in range(q_count):
            g = h // repeat
            scores = inner_t(
                turned_q[:, h * HEAD_DIM : (h + 1) * HEAD_DIM],
                keys_ref[reach, g * HEAD_DIM : (g + 1) * HEAD_DIM],
            ) * HEAD_DIM ** (-0.5)
            scores = jnp.where(valid, scores, -jnp.inf)
            sink = sink_ref[h]
            top = jnp.maximum(jnp.max(scores, axis=1, keepdims=True), sink)
            expo = jnp.exp(scores - top)
            total = jnp.sum(expo, axis=1, keepdims=True) + jnp.exp(sink - top)
            begin = kv_width + g * HEAD_DIM
            values = jnp.dot(
                expo.astype(BF16),
                kv_ref[reach, begin : begin + HEAD_DIM],
                preferred_element_type=F32,
            )
            outs.append((values / total).astype(BF16))
            logs = jnp.where(q_lane == h, top + jnp.log(total), logs)
        feat_ref[rows, wide:] = jnp.concatenate(outs, axis=1)
        log_ref[rows, :] = logs

    sweep(blocks, 3, attend)

    gate_first = first_units + second_units
    until(GROUP * hops * -(-(gate_first + gate_units) // GROUP))

    def gate_dot(b):
        rows = rows_at(b, dot_rows)
        for d in range(2):
            gate_ref[rows, d * gate_units * TILE : (d + 1) * gate_units * TILE] = jnp.dot(
                normed_ref[rows, :],
                weights(d, gate_first, gate_first + gate_units),
                preferred_element_type=F32,
            ).astype(BF16)

    sweep(count // dot_rows, 0, gate_dot)

    def mix(b):
        rows = rows_at(b, size)
        cum = cum_ref[rows, :]
        step = step_ref[rows, :]
        cum_t = cum.T
        step_t = step.T
        x = cells_ref[rows, :wide]
        writes = cells_ref[rows, wide : wide + state]
        reads = cells_ref[rows, wide + state :]
        cross = inner_t(reads, writes)
        parts = []
        for h in range(heads):
            f = slice(h, h + 1)
            g = slice(heads + h, heads + h + 1)
            seg = jnp.where(row >= col, cum[:, f] - cum_t[f], cum[:, g] - cum_t[g])
            scale = jnp.where(
                row > col, step_t[f], jnp.where(row < col, step_t[g], step_t[f] + step_t[g])
            )
            weight = (cross * jnp.exp(seg) * scale).astype(BF16)
            parts.append(
                jnp.dot(weight, x[:, h * HEAD_DIM : (h + 1) * HEAD_DIM], preferred_element_type=F32)
            )
        y = jnp.concatenate(parts, axis=1)
        fades = jnp.exp(cum)
        for e in range(2):
            held = entry_ref[e, b] + jnp.exp(before_ref[e, b][0:1]) * start_ref[e]
            y = y + through(fades, spreads[e], True) * jnp.dot(
                reads, held.astype(BF16), preferred_element_type=F32
            )
        gate = gate_ref[rows, :].astype(F32)
        y = y * (gate * jax.nn.sigmoid(gate))
        y = y * lax.rsqrt(jnp.mean(y * y, axis=1, keepdims=True) + EPS)
        feat_ref[rows, :wide] = (y * norm_gain_ref[...].astype(F32)).astype(BF16)

    left_ticks = sends - GROUP - clock[0]
    sweep(blocks, min(2, left_ticks // blocks), mix)

    out_first = gate_first + gate_units
    out_units = per_dir - out_first
    per_peer = 2 * seats // peers

    def out_copy(tile):
        dest = lax.div(tile, per_peer)
        return dest, pltpu.make_async_remote_copy(
            src_ref=part_ref.at[tile],
            dst_ref=peer_ref.at[lane_peer, lax.rem(tile, per_peer)],
            send_sem=out_send.at[tile],
            recv_sem=out_recv.at[lane_peer, lax.rem(tile, per_peer)],
            device_id={"tp": dest},
            device_id_type=mesh_id,
        )

    def project(d, owner):
        tile = 2 * owner + d
        matrix = ring_ref[d, out_first:, owner].reshape(out_units * unit_rows, TILE)

        def rows_dot(b, _):
            rows = rows_at(b, dot_rows)
            part_ref[tile, rows, :] = jnp.dot(
                feat_ref[rows, :], matrix, preferred_element_type=F32
            ).astype(BF16)
            return 0

        lax.fori_loop(0, count // dot_rows, rows_dot, 0)
        dest, copy = out_copy(tile)
        pl.when(dest != lane_peer)(lambda: copy.start())

    for d in range(2):
        project(d, place)
    final = sends - GROUP * hops
    done = max(0, (clock[0] - final) // GROUP)

    def project_hop(k):
        project(0, seat_at(my_pos - k - 1))
        project(1, seat_at(my_pos + k + 1))

    def early(k, _):
        project_hop(k)
        return 0

    lax.fori_loop(0, done, early, 0)
    until(final + GROUP * done)
    sweep(hops - 1 - done, GROUP, lambda i: project_hop(i + done))
    for j in range(GROUP):
        tick(jnp.int32(sends - GROUP + j), last=True)
    project_hop(jnp.int32(hops - 1))

    def gather_peers(r, _):
        source = lax.rem(lane_peer + r, peers)
        for j in range(per_peer):
            pltpu.make_async_remote_copy(
                src_ref=part_ref.at[j],
                dst_ref=peer_ref.at[source, j],
                send_sem=out_send.at[j],
                recv_sem=out_recv.at[source, j],
                device_id={"tp": source},
                device_id_type=mesh_id,
            ).wait_recv()
        return 0

    lax.fori_loop(1, peers, gather_peers, 0)

    def add_up(b, _):
        rows = rows_at(b, size)
        for j in range(per_peer):
            total = part_ref[lane_peer * per_peer + j, rows, :].astype(F32)
            for r in range(1, peers):
                total = total + peer_ref[lax.rem(lane_peer + r, peers), j, rows, :].astype(F32)
            out_ref[rows, j * TILE : (j + 1) * TILE] = total.astype(BF16)
        return 0

    lax.fori_loop(0, blocks, add_up, 0)

    edges_left(conv_edges)
    edges_left(kv_edges)
    for r in range(len(jumps)):
        for e in range(2):
            pl.when(sends_to(r, e))(lambda: scan_copy(r, e).wait_send())
    for r in range(1, seats):
        steps_copy(r).wait_send()

    def ring_left(i, _):
        for d in range(2):
            ring_copy(i, d, 0).wait_send()
        return 0

    lax.fori_loop(0, sends, ring_left, 0)

    def out_left(tile, _):
        dest, copy = out_copy(tile)
        pl.when(dest != lane_peer)(lambda: copy.wait_send())
        return 0

    lax.fori_loop(0, 2 * seats, out_left, 0)


def turn_tables(rows_total):
    quarter = HEAD_DIM // 4
    freqs = np.float32(ROPE_BASE) ** (-np.arange(quarter).astype(np.float32) / np.float32(quarter))
    border = WINDOW // GRID_W
    row_angle = (np.arange(rows_total + 2 * border) - border).astype(np.float32)[:, None] * freqs
    col_angle = np.arange(GRID_W).astype(np.float32)[:, None] * freqs

    def table(angle, first):
        zero = np.zeros_like(angle)
        cosine = np.cos(angle)
        sine = np.sin(angle)
        one = [cosine, cosine, zero, zero] if first else [zero, zero, cosine, cosine]
        two = [-sine, sine, zero, zero] if first else [zero, zero, -sine, sine]
        copies = TILE // HEAD_DIM
        return np.concatenate(one * copies + two * copies, axis=1).astype(np.float32)

    return table(row_angle, True), table(col_angle, False)


def streamed(
    tokens,
    input_gain,
    gate_weight,
    value_weight,
    inflow_weight,
    readout_weight,
    step_weight,
    conv_values,
    conv_inflow,
    conv_readout,
    log_rate,
    group_gain,
    query_weight,
    key_weight,
    vector_weight,
    sink_logit,
    state_out,
    window_out,
):
    count, width = tokens.shape
    seats = lax.axis_size("sp")
    peers = lax.axis_size("tp")
    heads = step_weight.shape[2]
    unit_rows = value_weight.shape[0]
    inflow = flatten_rows(inflow_weight)
    readout = flatten_rows(readout_weight)
    wide = value_weight.shape[1]
    state = inflow.shape[1]
    conv_width = wide + 2 * state
    q_width = query_weight.shape[1]
    kv_width = key_weight.shape[1]
    blocks = count // SSD_BLOCK
    taps = jnp.concatenate([conv_values, flatten_rows(conv_inflow), flatten_rows(conv_readout)], axis=1)
    rates = -jnp.exp(jnp.transpose(log_rate, (1, 0, 2)).reshape(count, 2 * heads))
    rates = jnp.pad(rates, ((0, 0), (0, TILE - 2 * heads)))
    steps = jnp.transpose(step_weight, (1, 2, 0)).reshape(2 * heads, unit_rows)
    row_turn, col_turn = turn_tables(seats * count // GRID_W)
    units = chunk_maps(
        {
            "value": value_weight.shape,
            "inflow": inflow.shape,
            "readout": readout.shape,
            "query": query_weight.shape,
            "key": key_weight.shape,
            "vector": vector_weight.shape,
            "gate": gate_weight.shape,
            "state_out": state_out.shape,
            "window_out": window_out.shape,
        }
    )
    per_dir = len(units[0])
    sends = per_dir * (seats - 1)
    rounds = 1
    while 2 ** (rounds - 1) < seats - 1:
        rounds += 1
    vmem = pl.BlockSpec(memory_space=pltpu.VMEM)
    smem = pl.BlockSpec(memory_space=pltpu.SMEM)
    hbm = pl.BlockSpec(memory_space=pltpu.HBM)
    dma = pltpu.SemaphoreType.DMA
    scratch = [
        pltpu.VMEM((2, per_dir, seats, unit_rows, TILE), BF16),
        pltpu.VMEM((seats, 2 * heads, unit_rows), BF16),
        pltpu.VMEM((count, width), BF16),
        pltpu.VMEM((count + 2 * PAD, conv_width), BF16),
        pltpu.VMEM((count, conv_width), BF16),
        pltpu.VMEM((count, TILE), F32),
        pltpu.VMEM((count, TILE), F32),
        pltpu.VMEM((count, TILE), F32),
        pltpu.VMEM((2, blocks, state, wide), F32),
        pltpu.VMEM((2, blocks, 8, wide), F32),
        pltpu.VMEM((2, state, wide), F32),
        pltpu.VMEM((2, 8, wide), F32),
        pltpu.VMEM((2, rounds, state + PAD, wide), BF16),
        pltpu.VMEM((2, rounds, state + PAD, wide), BF16),
        pltpu.VMEM((2, state, wide), F32),
        pltpu.VMEM((2, 8, wide), F32),
        pltpu.VMEM((count, wide), BF16),
        pltpu.VMEM((count, q_width), BF16),
        pltpu.VMEM((count + 2 * WINDOW, 2 * kv_width), BF16),
        pltpu.VMEM((count + 2 * WINDOW, kv_width), BF16),
        pltpu.VMEM((count + 2 * WINDOW, 2 * TILE), F32),
        pltpu.VMEM((count, wide + q_width), BF16),
        pltpu.VMEM((2 * seats, count, TILE), BF16),
        pltpu.VMEM((peers, 2 * seats // peers, count, TILE), BF16),
        dma((2, sends)),
        dma((2, sends)),
        dma((seats,)),
        dma((seats,)),
        dma((2 * per_dir,)),
        dma((2,)),
        dma((2,)),
        dma((2,)),
        dma((2,)),
        dma((2, rounds)),
        dma((2, rounds)),
        dma((2 * seats,)),
        dma((peers, 2 * seats // peers)),
    ]
    return pl.pallas_call(
        functools.partial(layer_kernel, (seats, peers, units)),
        out_shape=(
            jax.ShapeDtypeStruct((count, width // peers), BF16),
            jax.ShapeDtypeStruct((count, q_width // HEAD_DIM), F32),
        ),
        in_specs=[vmem] * 5 + [smem] + [vmem] * 3 + [hbm] * 9,
        out_specs=(vmem, vmem),
        scratch_shapes=scratch,
        compiler_params=pltpu.CompilerParams(
            collective_id=0, has_side_effects=True, vmem_limit_bytes=60 * 2**20
        ),
    )(
        tokens,
        input_gain[None],
        taps,
        rates,
        group_gain[None],
        sink_logit,
        jnp.asarray(row_turn),
        jnp.asarray(col_turn),
        steps,
        value_weight,
        inflow,
        readout,
        query_weight,
        key_weight,
        vector_weight,
        gate_weight,
        state_out,
        window_out,
    )


def streams(arrays):
    tokens, value, inflow, key, out = arrays[0], arrays[3], arrays[4], arrays[13], arrays[16]
    seats = lax.axis_size("sp")
    return (
        seats % 2 == 0
        and value.shape[0] % TILE == 0
        and out.shape[0] % value.shape[0] == 0
        and out.shape[1] == 2 * TILE
        and value.shape[1] == 4 * TILE
        and inflow.shape[1] * inflow.shape[2] == TILE
        and key.shape[1] == TILE
        and tokens.shape[0] == 6 * SSD_BLOCK
        and tokens.shape[1] == seats * value.shape[0]
        and seats == 2 * lax.axis_size("tp")
    )


def layer(*arrays):
    if streams(arrays):
        return streamed(*arrays)
    return shards(*arrays)


def shards(
    tokens,
    input_gain,
    gate_weight,
    value_weight,
    inflow_weight,
    readout_weight,
    step_weight,
    conv_values,
    conv_inflow,
    conv_readout,
    log_rate,
    group_gain,
    query_weight,
    key_weight,
    vector_weight,
    sink_logit,
    state_out,
    window_out,
):
    count = tokens.shape[0]
    offset = lax.axis_index("sp") * count
    seq_total = count * lax.axis_size("sp")
    heads = step_weight.shape[2]
    groups = inflow_weight.shape[1]
    state_len = inflow_weight.shape[2]
    inner_local = value_weight.shape[1]
    q_count = query_weight.shape[1] // HEAD_DIM
    kv_count = key_weight.shape[1] // HEAD_DIM
    kv_width = key_weight.shape[1]
    wide = tokens.astype(F32)
    normed = (
        wide
        * lax.rsqrt(jnp.mean(wide * wide, axis=1, keepdims=True) + EPS)
        * input_gain.astype(F32)
    ).astype(BF16)

    def whole(parts):
        return lax.all_gather(jnp.concatenate(parts, axis=1), "sp", axis=0, tiled=True)

    own = (flatten_rows(inflow_weight), flatten_rows(readout_weight), flatten_rows(step_weight))
    first_matrix = whole((value_weight,) + own)
    rest_matrix = whole((key_weight, vector_weight, gate_weight, query_weight))
    first = jnp.dot(normed, first_matrix, preferred_element_type=F32)
    rest = jnp.dot(normed, rest_matrix, preferred_element_type=F32).astype(BF16)
    conv_width = inner_local + 2 * groups * state_len
    conv_input = first[:, :conv_width].astype(BF16)
    step = jax.nn.softplus(first[:, conv_width:])
    keyvals = rest[:, : 2 * kv_width]
    gate = rest[:, 2 * kv_width : 2 * kv_width + inner_local]
    queries = rest[:, 2 * kv_width + inner_local :]

    reach_rows = CONV // 2
    padded = with_halo(conv_input, (("sp", 0),), CONV // 2).astype(F32)
    taps = jnp.concatenate(
        [conv_values, flatten_rows(conv_inflow), flatten_rows(conv_readout)], axis=1
    ).astype(F32)
    conv_sum = padded[0:count] * taps[0]
    for tap in range(1, 2 * reach_rows + 1):
        conv_sum = conv_sum + padded[tap : tap + count] * taps[tap]
    cells = jax.nn.silu(conv_sum).astype(BF16)
    rates = jnp.transpose(log_rate, (1, 0, 2)).reshape(count, 2 * heads)
    sd = jnp.concatenate([step, -jnp.exp(rates) * step], axis=1)
    blocks = count // SSD_BLOCK
    sdt = jnp.transpose(sd.reshape(blocks, SSD_BLOCK, 4 * heads), (0, 2, 1))

    summary = call(
        summary_kernel,
        jax.ShapeDtypeStruct((2, state_len + PAD, inner_local), BF16),
        (cells, sd),
    )
    everyone = lax.all_gather(summary, "sp")
    out_stack, everyone = lax.optimization_barrier(
        (jnp.concatenate([state_out, window_out], axis=0), everyone)
    )
    out_matrix = lax.all_gather(out_stack, "sp", axis=1, tiled=True)
    seats = lax.axis_size("sp")
    place = lax.axis_index("sp")
    totals = everyone[:, :, state_len].astype(F32) + everyone[:, :, state_len + 1].astype(F32)
    seat = jnp.arange(seats)
    starts = []
    for e in range(2):
        ahead = seat < place if e == 0 else seat > place
        between = (seat[None, :] > seat[:, None]) if e == 0 else (seat[None, :] < seat[:, None])
        between = (between & ahead[None, :])[:, :, None]
        fade = jnp.sum(jnp.where(between, totals[None, :, e], 0.0), axis=1)
        fade = jnp.where(ahead[:, None], jnp.exp(fade), 0.0)
        starts.append(jnp.sum(fade[:, None, :] * everyone[:, e, :state_len].astype(F32), axis=0))
    starts = jnp.stack(starts)
    state_features = call(
        mixer_kernel,
        jax.ShapeDtypeStruct((count, inner_local), BF16),
        (cells, sd, sdt, starts, gate, group_gain[None]),
        (
            pltpu.VMEM((blocks, state_len, inner_local), BF16),
            pltpu.VMEM((state_len, inner_local), F32),
        ),
        flops=10**10,
    )

    beside = with_halo(keyvals, (("sp", 0),), WINDOW)
    quarter = HEAD_DIM // 4
    freqs = ROPE_BASE ** (-jnp.arange(quarter).astype(F32) / quarter)
    spots = offset - WINDOW + jnp.arange(count + 2 * WINDOW, dtype=jnp.int32)
    row_angle = (spots // GRID_W).astype(F32)[:, None] * freqs
    col_angle = (spots % GRID_W).astype(F32)[:, None] * freqs
    angles = jnp.concatenate([row_angle, col_angle], axis=1)
    cosine = jnp.cos(angles)
    sine = jnp.sin(angles)

    def doubled(table, sign):
        low = table[:, :quarter]
        high = table[:, quarter:]
        return [sign * low, low, sign * high, high]

    turn = jnp.concatenate(doubled(cosine, 1.0) + doubled(sine, -1.0), axis=1)
    channel = jnp.arange(HEAD_DIM)
    partner = channel + jnp.where(channel % (2 * quarter) < quarter, quarter, -quarter)
    swap = (channel[:, None] == partner[None, :]).astype(BF16)
    limits = jnp.stack([offset, seq_total]).astype(jnp.int32)
    window_features, log_total = call(
        attend_kernel,
        (
            jax.ShapeDtypeStruct((count, q_count * HEAD_DIM), BF16),
            jax.ShapeDtypeStruct((count, q_count), F32),
        ),
        (limits, sink_logit, queries, beside, turn, swap),
        (pltpu.VMEM((kv_count, count + 2 * WINDOW, HEAD_DIM), BF16),),
        scalars=2,
        flops=10**10,
    )
    features = jnp.concatenate([state_features, window_features], axis=1)
    terms = jnp.dot(features, out_matrix, preferred_element_type=F32)
    mixed = lax.psum_scatter(terms.astype(BF16), "tp", scatter_dimension=1, tiled=True)
    return (mixed, log_total)


def solution(mesh):
    placed = (
        P("sp", None),
        P(),
        P("sp", "tp"),
        P("sp", "tp"),
        P("sp", "tp", None),
        P("sp", "tp", None),
        P("sp", None, "tp"),
        P(None, "tp"),
        P(None, "tp", None),
        P(None, "tp", None),
        P(None, "sp", "tp"),
        P("tp"),
        P("sp", "tp"),
        P("sp", "tp"),
        P("sp", "tp"),
        P("tp"),
        P("tp", "sp"),
        P("tp", "sp"),
    )
    return jax.shard_map(
        layer,
        mesh=mesh,
        in_specs=placed,
        out_specs=(P("sp", "tp"), P("sp", "tp")),
        check_vma=False,
    )
```

```python
import functools

import jax
import jax.numpy as jnp
import numpy as np
from jax import lax
from jax.experimental import pallas as pl
from jax.experimental.pallas import tpu as pltpu
from jax.sharding import PartitionSpec as P


HEAD_DIM = 64
CONV = 5
SSD_BLOCK = 128
WINDOW = 128
GRID_W = 64


EPS = 1e-06
ROPE_BASE = 10000.0
HIGHEST = lax.Precision.HIGHEST
F32 = jnp.float32
BF16 = jnp.bfloat16
PAD = 16


def iota(shape, dim):
    return lax.broadcasted_iota(jnp.int32, shape, dim)


def exact(a, b):
    return jnp.dot(a, b, precision=HIGHEST, preferred_element_type=F32)


def spread(heads):
    shape = (heads, heads * HEAD_DIM)
    return (iota(shape, 1) // HEAD_DIM == iota(shape, 0)).astype(F32)


def inner_t(a, b):
    return lax.dot_general(a, b, (((1,), (1,)), ((), ())), preferred_element_type=F32)


def outer_t(a, b):
    return lax.dot_general(a, b, (((0,), (0,)), ((), ())), preferred_element_type=F32)


def summary_kernel(cells_ref, sd_ref, out_ref):
    count = cells_ref.shape[0]
    heads = sd_ref.shape[1] // 4
    wide = heads * HEAD_DIM
    state = out_ref.shape[1] - PAD
    x = cells_ref[:, :wide].astype(F32)
    writes = cells_ref[:, wide : wide + state]
    expand = spread(heads)
    row = iota((count, count), 0)
    col = iota((count, count), 1)
    for e in range(2):
        step = sd_ref[:, e * heads : (e + 1) * heads]
        decay = sd_ref[:, (2 + e) * heads : (3 + e) * heads]
        span = (col > row) if e == 0 else (col < row)
        rest = exact(span.astype(F32), decay)
        scaled = (x * exact(jnp.exp(rest) * step, expand)).astype(BF16)
        out_ref[e, :state, :] = outer_t(writes, scaled).astype(BF16)
        total = exact(jnp.broadcast_to(jnp.sum(decay, axis=0, keepdims=True), (8, heads)), expand)
        total = total[0:1]
        high = total.astype(BF16).astype(F32)
        place = iota((PAD, wide), 0)
        packed = jnp.where(place == 0, high, jnp.where(place == 1, total - high, 0.0))
        out_ref[e, state:, :] = packed.astype(BF16)


def mixer_kernel(cells_ref, sd_ref, sdt_ref, start_ref, gate_ref, gain_ref, out_ref, back_ref, carry_ref):
    blocks, _, size = sdt_ref.shape
    heads = sd_ref.shape[1] // 4
    wide = heads * HEAD_DIM
    state = start_ref.shape[1]
    expand = spread(heads)
    row = iota((size, size), 0)
    col = iota((size, size), 1)
    lower = (row >= col).astype(F32)
    upper = (row <= col).astype(F32)

    carry_ref[...] = start_ref[1]

    def backward(index, _):
        block = blocks - 1 - index
        rows = pl.ds(pl.multiple_of(block * size, size), size)
        back_ref[block] = carry_ref[...].astype(BF16)
        step = sd_ref[rows, heads : 2 * heads]
        cum = exact(upper, sd_ref[rows, 3 * heads : 4 * heads])
        edge = cum[0:1]
        x = cells_ref[rows, :wide].astype(F32)
        scaled = (x * exact(jnp.exp(edge - cum) * step, expand)).astype(BF16)
        fresh = outer_t(cells_ref[rows, wide : wide + state], scaled)
        fade = exact(jnp.broadcast_to(jnp.exp(edge), (8, heads)), expand)[0:1]
        carry_ref[...] = fade * carry_ref[...] + fresh
        return 0

    lax.fori_loop(0, blocks, backward, 0)
    carry_ref[...] = start_ref[0]

    def forward(block, _):
        rows = pl.ds(pl.multiple_of(block * size, size), size)
        cum_f = exact(lower, sd_ref[rows, 2 * heads : 3 * heads])
        cum_b = exact(upper, sd_ref[rows, 3 * heads : 4 * heads])
        flat = sdt_ref[block]
        step_ft = flat[:heads]
        step_bt = flat[heads : 2 * heads]
        cum_ft = exact(flat[2 * heads : 3 * heads], upper)
        cum_bt = exact(flat[3 * heads :], lower)
        x = cells_ref[rows, :wide]
        writes = cells_ref[rows, wide : wide + state]
        reads = cells_ref[rows, wide + state :]
        cross = inner_t(reads, writes)
        parts = []
        for h in range(heads):
            one = slice(h, h + 1)
            seg = jnp.where(
                row >= col, cum_f[:, one] - cum_ft[one], cum_b[:, one] - cum_bt[one]
            )
            scale = jnp.where(
                row > col,
                step_ft[one],
                jnp.where(row < col, step_bt[one], step_ft[one] + step_bt[one]),
            )
            weight = (cross * jnp.exp(seg) * scale).astype(BF16)
            parts.append(
                jnp.dot(
                    weight, x[:, h * HEAD_DIM : (h + 1) * HEAD_DIM], preferred_element_type=F32
                )
            )
        y = jnp.concatenate(parts, axis=1)
        y = y + exact(jnp.exp(cum_f), expand) * jnp.dot(
            reads, carry_ref[...].astype(BF16), preferred_element_type=F32
        )
        y = y + exact(jnp.exp(cum_b), expand) * jnp.dot(
            reads, back_ref[block], preferred_element_type=F32
        )
        gate = gate_ref[rows, :].astype(F32)
        y = y * (gate * jax.nn.sigmoid(gate))
        y = y * lax.rsqrt(jnp.mean(y * y, axis=1, keepdims=True) + EPS)
        out_ref[rows, :] = (y * gain_ref[...].astype(F32)).astype(BF16)
        edge = cum_f[size - 1 : size]
        step = sd_ref[rows, :heads]
        scaled = (x.astype(F32) * exact(jnp.exp(edge - cum_f) * step, expand)).astype(BF16)
        fade = exact(jnp.broadcast_to(jnp.exp(edge), (8, heads)), expand)[0:1]
        carry_ref[...] = fade * carry_ref[...] + outer_t(writes, scaled)
        return 0

    lax.fori_loop(0, blocks, forward, 0)


def attend_kernel(place_ref, sink_ref, q_ref, kv_ref, turn_ref, swap_ref, out_ref, log_ref, keys_ref):
    count = q_ref.shape[0]
    q_count = q_ref.shape[1] // HEAD_DIM
    kv_width = kv_ref.shape[1] // 2
    repeat = q_count * HEAD_DIM // kv_width
    size = SSD_BLOCK
    band = size + 2 * WINDOW
    swap = swap_ref[...]

    def turned(part, rows):
        swapped = jnp.dot(part, swap, preferred_element_type=F32)
        table = turn_ref[rows, :]
        return (part.astype(F32) * table[:, :HEAD_DIM] + swapped * table[:, HEAD_DIM:]).astype(BF16)

    def prepare(block, _):
        rows = pl.ds(pl.multiple_of(block * size, size), size)
        for g in range(kv_width // HEAD_DIM):
            keys_ref[g, rows, :] = turned(
                kv_ref[rows, g * HEAD_DIM : (g + 1) * HEAD_DIM], rows
            )
        return 0

    lax.fori_loop(0, kv_ref.shape[0] // size, prepare, 0)
    row = iota((size, band), 0)
    col = iota((size, band), 1)
    near = (col >= row) & (col - row <= 2 * WINDOW)
    lane = iota((size, q_count), 1)

    def one(block, _):
        start = pl.multiple_of(block * size, size)
        rows = pl.ds(start, size)
        reach = pl.ds(start, band)
        key_pos = place_ref[0] + start - WINDOW + col
        valid = near & (key_pos >= 0) & (key_pos < place_ref[1])
        logs = jnp.zeros((size, q_count), F32)
        outs = []
        for h in range(q_count):
            g = h // repeat
            query = turned(
                q_ref[rows, h * HEAD_DIM : (h + 1) * HEAD_DIM], pl.ds(start + WINDOW, size)
            )
            scores = inner_t(query, keys_ref[g, reach, :]) * HEAD_DIM ** (-0.5)
            scores = jnp.where(valid, scores, -jnp.inf)
            sink = sink_ref[h]
            top = jnp.maximum(jnp.max(scores, axis=1, keepdims=True), sink)
            expo = jnp.exp(scores - top)
            total = jnp.sum(expo, axis=1, keepdims=True) + jnp.exp(sink - top)
            first = kv_width + g * HEAD_DIM
            values = jnp.dot(
                expo.astype(BF16),
                kv_ref[reach, first : first + HEAD_DIM],
                preferred_element_type=F32,
            )
            outs.append((values / total).astype(BF16))
            logs = jnp.where(lane == h, top + jnp.log(total), logs)
        out_ref[rows, :] = jnp.concatenate(outs, axis=1)
        log_ref[rows, :] = logs
        return 0

    lax.fori_loop(0, count // size, one, 0)


def call(kernel, out_shape, args, scratch=(), scalars=0, flops=10**8):
    vmem = pl.BlockSpec(memory_space=pltpu.VMEM)
    smem = pl.BlockSpec(memory_space=pltpu.SMEM)
    return pl.pallas_call(
        kernel,
        out_shape=out_shape,
        in_specs=[smem] * scalars + [vmem] * (len(args) - scalars),
        out_specs=jax.tree.map(lambda _: vmem, out_shape),
        scratch_shapes=list(scratch),
        cost_estimate=pl.CostEstimate(flops=flops, bytes_accessed=4 * 10**6, transcendentals=0),
        compiler_params=pltpu.CompilerParams(vmem_limit_bytes=40 * 2**20),
    )(*args)


def with_halo(cells, sides, width):
    for axis, dim in sides:
        count = lax.axis_size(axis)
        ends = count - 1
        head = lax.slice_in_dim(cells, 0, width, axis=dim)
        tail = lax.slice_in_dim(cells, cells.shape[dim] - width, cells.shape[dim], axis=dim)
        cells = jnp.concatenate(
            [
                lax.ppermute(tail, axis, [(i, (i + 1) % count) for i in range(ends)]),
                cells,
                lax.ppermute(head, axis, [((i + 1) % count, i) for i in range(ends)]),
            ],
            axis=dim,
        )
    return cells


def flatten_rows(weight):
    return weight.reshape(weight.shape[0], -1)


TILE = 128
GROUP = 3


def split3(v):
    high = v.astype(BF16)
    rest = v - high.astype(F32)
    mid = rest.astype(BF16)
    return high, mid, (rest - mid.astype(F32)).astype(BF16)


def through(left, right, left_wide):
    total = None
    for part in split3(left if left_wide else right):
        one = jnp.dot(part, right, preferred_element_type=F32) if left_wide else jnp.dot(
            left, part, preferred_element_type=F32
        )
        total = one if total is None else total + one
    return total


def chunk_maps(shapes):
    rows = shapes["value"][0]

    def tiles(name):
        return [(name, 0, c) for c in range(shapes[name][1] // TILE)]

    units = ([], [])
    for names in (("value", "inflow", "readout"), ("query", "key", "vector"), ("gate",)):
        flat = [t for name in names for t in tiles(name)]
        half = len(flat) // 2
        for d in range(2):
            units[d].extend(flat[d * half : (d + 1) * half])
    for d in range(2):
        for name in ("state_out", "window_out"):
            units[d].extend((name, r, d) for r in range(shapes[name][0] // rows))
    return units


def layer_kernel(
    cfg,
    tokens_hbm,
    gains_ref,
    value_taps_ref,
    inflow_taps_ref,
    readout_taps_ref,
    rates_ref,
    sink_ref,
    row_turn_ref,
    col_turn_ref,
    steps_ref,
    value_ref,
    inflow_ref,
    readout_ref,
    query_ref,
    key_ref,
    vector_ref,
    gate_w_ref,
    state_out_ref,
    window_out_ref,
    out_ref,
    log_ref,
    ring_ref,
    steps_all_ref,
    tokens_ref,
    normed_ref,
    conv_ref,
    cells_ref,
    step_ref,
    cum_ref,
    entry_ref,
    before_ref,
    carry_ref,
    total_ref,
    scan_send_ref,
    scan_recv_ref,
    start_ref,
    reach_ref,
    pair_ref,
    gate_ref,
    q_ref,
    kv_ref,
    keys_ref,
    turn_ref,
    feat_ref,
    part_ref,
    near_ref,
    far_ref,
    send_sem,
    recv_sem,
    steps_send,
    steps_recv,
    local_sem,
    halo_send,
    halo_recv,
    kv_send,
    kv_recv,
    scan_ssem,
    scan_rsem,
    near_send,
    near_recv,
    far_send,
    far_recv,
):
    seats, peers, units = cfg
    count, width = tokens_hbm.shape
    unit_rows = ring_ref.shape[3]
    heads = steps_ref.shape[0] // 2
    wide = heads * HEAD_DIM
    state = inflow_ref.shape[1]
    conv_width = wide + 2 * state
    q_width = query_ref.shape[1]
    q_count = q_width // HEAD_DIM
    kv_width = key_ref.shape[1]
    per_dir = len(units[0])
    hops = seats - 1
    sends = per_dir * hops
    place = lax.axis_index("sp")
    lane_peer = lax.axis_index("tp")
    half = seats // 2
    blocks = count // SSD_BLOCK
    size = SSD_BLOCK
    mesh_id = pl.DeviceIdType.MESH

    def seat_at(pos):
        pos = lax.rem(pos + 2 * seats, seats)
        late = lax.div(pos, half)
        return (1 - late) * 2 * pos + late * (2 * (seats - 1 - pos) + 1)

    odd = lax.rem(place, 2)
    my_pos = (1 - odd) * lax.div(place, 2) + odd * (seats - 1 - lax.div(place, 2))
    nexts = (seat_at(my_pos + 1), seat_at(my_pos - 1))

    barrier = pltpu.get_barrier_semaphore()
    for r in range(1, seats):
        pl.semaphore_signal(
            barrier, inc=1, device_id={"sp": lax.rem(place + r, seats)}, device_id_type=mesh_id
        )
    for r in range(1, peers):
        pl.semaphore_signal(
            barrier, inc=1, device_id={"tp": lax.rem(lane_peer + r, peers)}, device_id_type=mesh_id
        )

    sources = {
        "value": value_ref,
        "inflow": inflow_ref,
        "readout": readout_ref,
        "query": query_ref,
        "key": key_ref,
        "vector": vector_ref,
        "gate": gate_w_ref,
        "state_out": state_out_ref,
        "window_out": window_out_ref,
    }
    locals_ = []
    for d in range(2):
        for u, (name, r, c) in enumerate(units[d]):
            locals_.append(
                pltpu.make_async_copy(
                    sources[name].at[pl.ds(r * unit_rows, unit_rows), pl.ds(c * TILE, TILE)],
                    ring_ref.at[d, u, place],
                    local_sem.at[d * per_dir + u],
                )
            )
    for copy in locals_:
        copy.start()
    tokens_in = pltpu.make_async_copy(tokens_hbm, tokens_ref, local_sem.at[2 * per_dir])
    tokens_in.start()
    steps_all_ref[place] = steps_ref[...]
    for copy in locals_:
        copy.wait()
    pl.semaphore_wait(barrier, hops + peers - 1)

    def ring_copy(i, d, behind):
        turn = lax.div(i, GROUP * hops)
        k = lax.rem(lax.div(i, GROUP), hops) + behind
        unit = GROUP * turn + lax.rem(i, GROUP)
        owner = seat_at(my_pos - k) if d == 0 else seat_at(my_pos + k)
        block = ring_ref.at[d, unit, owner]
        return pltpu.make_async_remote_copy(
            src_ref=block,
            dst_ref=block,
            send_sem=send_sem.at[d, i],
            recv_sem=recv_sem.at[d, i],
            device_id={"sp": nexts[d]},
            device_id_type=mesh_id,
        )

    def tick(i, last=False):
        for d in range(2):
            ring_copy(i, d, 1).wait_recv()
            if not last:
                ring_copy(i + GROUP, d, 0).start()

    for j in range(GROUP):
        for d in range(2):
            ring_copy(jnp.int32(j), d, 0).start()

    def steps_copy(r):
        return pltpu.make_async_remote_copy(
            src_ref=steps_ref,
            dst_ref=steps_all_ref.at[place],
            send_sem=steps_send.at[r],
            recv_sem=steps_recv.at[place],
            device_id={"sp": lax.rem(place + r, seats)},
            device_id_type=mesh_id,
        )

    for r in range(1, seats):
        steps_copy(r).start()

    clock = [0]

    def sweep(trips, per_trip, body):
        base = clock[0]

        def run(i, _):
            for j in range(int(per_trip)):
                tick(base + i * int(per_trip) + j)
            if per_trip == 0.5:
                pl.when(lax.rem(i, 2) == 0)(lambda: tick(base + lax.div(i, 2)))
            body(i)
            return 0

        lax.fori_loop(0, trips, run, 0)
        clock[0] = base + (trips + 1) // 2 if per_trip == 0.5 else base + trips * per_trip

    def until(goal):
        if goal > clock[0]:
            sweep(goal - clock[0], 1, lambda i: None)

    def rows_at(index, length, first=0):
        return pl.ds(pl.multiple_of(index * length, length) + first, length)

    def normalise(b):
        rows = rows_at(b, size)
        x = tokens_ref[rows, :].astype(F32)
        scale = lax.rsqrt(jnp.mean(x * x, axis=1, keepdims=True) + EPS)
        normed_ref[rows, :] = (x * scale * gains_ref[:, :width].astype(F32)).astype(BF16)

    tokens_in.wait()
    sweep(blocks, 1, normalise)
    table_row = place * (count // GRID_W)

    def fill_turn(i):
        turn_ref[rows_at(i, GRID_W), :] = col_turn_ref[...] + row_turn_ref[pl.ds(table_row + i, 1), :]

    sweep(turn_ref.shape[0] // GRID_W, 0, fill_turn)
    step_ref[...] = jnp.zeros_like(step_ref)
    carry_ref[...] = jnp.zeros_like(carry_ref)
    total_ref[...] = jnp.zeros_like(total_ref)
    start_ref[...] = jnp.zeros_like(start_ref)
    reach_ref[...] = jnp.zeros_like(reach_ref)

    first_edge = place == 0
    last_edge = place == seats - 1

    @pl.when(first_edge)
    def _():
        conv_ref[:PAD, :] = jnp.zeros((PAD, conv_width), BF16)
        kv_ref[:WINDOW, :] = jnp.zeros((WINDOW, 2 * kv_width), BF16)

    @pl.when(last_edge)
    def _():
        conv_ref[PAD + count :, :] = jnp.zeros((PAD, conv_width), BF16)
        kv_ref[WINDOW + count :, :] = jnp.zeros((WINDOW, 2 * kv_width), BF16)

    def weights(d, first, last):
        return jnp.concatenate(
            [ring_ref[d, u].reshape(seats * unit_rows, TILE) for u in range(first, last)], axis=1
        )

    first_units = conv_width // (2 * TILE)
    second_units = (q_width + 2 * kv_width) // (2 * TILE)
    gate_units = wide // (2 * TILE)
    until(GROUP * hops * -(-first_units // GROUP))
    for r in range(1, seats):
        peer = lax.rem(place + r, seats)
        pltpu.make_async_remote_copy(
            src_ref=steps_ref,
            dst_ref=steps_all_ref.at[peer],
            send_sem=steps_send.at[r],
            recv_sem=steps_recv.at[peer],
            device_id={"sp": peer},
            device_id_type=mesh_id,
        ).wait_recv()

    dot_rows = 2 * size

    def first_dot(b):
        rows = rows_at(b, dot_rows)
        here = normed_ref[rows, :]
        for d in range(2):
            conv_ref[rows_at(b, dot_rows, PAD), d * first_units * TILE : (d + 1) * first_units * TILE] = (
                jnp.dot(here, weights(d, 0, first_units), preferred_element_type=F32).astype(BF16)
            )
        steps = jnp.concatenate([steps_all_ref[o] for o in range(seats)], axis=1)
        raw = inner_t(here, steps)
        step = jnp.maximum(raw, 0.0) + jnp.log1p(jnp.exp(-jnp.abs(raw)))
        step_ref[rows, : 2 * heads] = step

    sweep(count // dot_rows, 1, first_dot)

    def edge_copies(ref, length, ssem, rsem):
        inner = ref.shape[0] - 2 * length
        up = pltpu.make_async_remote_copy(
            src_ref=ref.at[pl.ds(inner, length)],
            dst_ref=ref.at[pl.ds(0, length)],
            send_sem=ssem.at[0],
            recv_sem=rsem.at[0],
            device_id={"sp": lax.rem(place + 1, seats)},
            device_id_type=mesh_id,
        )
        down = pltpu.make_async_remote_copy(
            src_ref=ref.at[pl.ds(length, length)],
            dst_ref=ref.at[pl.ds(length + inner, length)],
            send_sem=ssem.at[1],
            recv_sem=rsem.at[1],
            device_id={"sp": lax.rem(place + hops, seats)},
            device_id_type=mesh_id,
        )
        return up, down

    def edges_start(pair):
        pl.when(jnp.logical_not(last_edge))(lambda: pair[0].start())
        pl.when(jnp.logical_not(first_edge))(lambda: pair[1].start())

    def edges_arrive(pair):
        pl.when(jnp.logical_not(first_edge))(lambda: pair[0].wait_recv())
        pl.when(jnp.logical_not(last_edge))(lambda: pair[1].wait_recv())

    def edges_left(pair):
        pl.when(jnp.logical_not(last_edge))(lambda: pair[0].wait_send())
        pl.when(jnp.logical_not(first_edge))(lambda: pair[1].wait_send())

    conv_edges = edge_copies(conv_ref, PAD, halo_send, halo_recv)
    edges_start(conv_edges)
    taps = jnp.concatenate(
        [ref[...] for ref in (value_taps_ref, inflow_taps_ref, readout_taps_ref)], axis=1
    ).astype(F32)
    lane = iota((size, TILE), 1)
    row = iota((size, size), 0)
    col = iota((size, size), 1)
    lower = (row >= col).astype(BF16)
    upper = (row <= col).astype(BF16)
    spread_row = iota((TILE, wide), 0)
    spread_col = iota((TILE, wide), 1) // HEAD_DIM
    spreads = [(spread_row - e * heads == spread_col).astype(BF16) for e in range(2)]

    def sums(b):
        rows = rows_at(b, size)
        filler = jnp.zeros((TILE - 2 * heads, size), F32)
        rates = jnp.concatenate([rates_ref[0, :, rows], rates_ref[1, :, rows], filler], axis=0).T
        decay = -jnp.exp(rates) * step_ref[rows, :]
        cum_ref[rows, :] = jnp.where(
            lane < heads, through(lower, decay, False), through(upper, decay, False)
        )

    sweep(blocks, 1, sums)
    edges_arrive(conv_edges)

    def convolve(b):
        rows = rows_at(b, size)
        padded = conv_ref[pl.ds(pl.multiple_of(b * size, size), size + 2 * PAD), :].astype(F32)
        first = PAD - CONV // 2
        total = padded[first : first + size] * taps[0:1]
        for tap in range(1, CONV):
            total = total + padded[first + tap : first + tap + size] * taps[tap : tap + 1]
        cells_ref[rows, :] = (total * jax.nn.sigmoid(total)).astype(BF16)

    sweep(blocks, 0.5, convolve)

    def summarise(i):
        for e in range(2):
            b = i if e == 0 else blocks - 1 - i
            rows = rows_at(b, size)
            cum = cum_ref[rows, :]
            edge = cum[size - 1 : size] if e == 0 else cum[0:1]
            scale = through(jnp.exp(edge - cum) * step_ref[rows, :], spreads[e], True)
            scaled = (cells_ref[rows, :wide].astype(F32) * scale).astype(BF16)
            fresh = outer_t(cells_ref[rows, wide : wide + state], scaled)
            edges = through(jnp.broadcast_to(edge, (8, TILE)), spreads[e], True)
            entry_ref[e, b] = carry_ref[e]
            before_ref[e, b] = total_ref[e]
            carry_ref[e] = jnp.exp(edges[0:1]) * carry_ref[e] + fresh
            total_ref[e] = total_ref[e] + edges

    sweep(blocks, 0.5, summarise)

    pair = lax.div(place, 2)
    pairs = seats // 2

    def scan_copy(stage, e):
        far = place + 1 - 2 * odd if stage == 0 else lax.rem(place + (2 if e == 0 else seats - 2), seats)
        return pltpu.make_async_remote_copy(
            src_ref=scan_send_ref.at[e, stage],
            dst_ref=scan_recv_ref.at[e, stage],
            send_sem=scan_ssem.at[e, stage],
            recv_sem=scan_rsem.at[e, stage],
            device_id={"sp": far},
            device_id_type=mesh_id,
        )

    def scan_start(stage, e, states, total):
        scan_send_ref[e, stage, :state] = states.astype(BF16)
        high = total.astype(BF16).astype(F32)
        at = iota((PAD, wide), 0)
        scan_send_ref[e, stage, state:] = jnp.where(
            at == 0, high, jnp.where(at == 1, total - high, 0.0)
        ).astype(BF16)
        scan_copy(stage, e).start()

    def scan_read(stage, e):
        far = scan_recv_ref[e, stage]
        decays = far[state : state + 8].astype(F32)
        return far[:state].astype(F32), decays[0:1] + decays[1:2]

    def scan_pair():
        for e in range(2):
            scan_copy(0, e).wait_recv()
            states, total = scan_read(0, e)
            mine, my_total = carry_ref[e], total_ref[e][0:1]

            @pl.when(odd == 1 - e)
            def _():
                pair_ref[e] = states * jnp.exp(my_total) + mine

            @pl.when(odd == e)
            def _():
                pair_ref[e] = mine * jnp.exp(total) + states

            total_ref[e] = total_ref[e] + total

    def scan_slot(r):
        for e in range(2):

            @pl.when(pair == (r if e == 0 else pairs - 1 - r))
            def _():
                if r > 0:
                    scan_copy(1, e).wait_recv()
                    states, total = scan_read(1, e)
                    start_ref[e] = states
                    reach_ref[e] = jnp.broadcast_to(total, reach_ref.shape[1:])
                if r < pairs - 1:
                    total = total_ref[e][0:1]
                    scan_start(
                        1, e, start_ref[e] * jnp.exp(total) + pair_ref[e], reach_ref[e][0:1] + total
                    )

    def scan_finish():
        for e in range(2):

            @pl.when(odd == 1 - e)
            def _():
                states, total = scan_read(0, e)
                start_ref[e] = start_ref[e] * jnp.exp(total) + states

    def scan_left():
        for e in range(2):
            scan_copy(0, e).wait_send()
            goes = pair < pairs - 1 if e == 0 else pair > 0
            pl.when(goes)(lambda: scan_copy(1, e).wait_send())

    for e in range(2):
        scan_start(0, e, carry_ref[e], total_ref[e][0:1])

    until(GROUP * hops * -(-(first_units + second_units) // GROUP))

    q_last = second_units - 2 * kv_width // TILE

    def second_dot_b(b):
        rows = rows_at(b, dot_rows)
        got = jnp.dot(
            normed_ref[rows, :],
            weights(1, first_units, first_units + second_units),
            preferred_element_type=F32,
        ).astype(BF16)
        q_ref[rows, second_units * TILE :] = got[:, : q_last * TILE]
        kv_ref[rows_at(b, dot_rows, WINDOW), :] = got[:, q_last * TILE :]

    sweep(count // dot_rows, 1, second_dot_b)
    kv_edges = edge_copies(kv_ref, WINDOW, kv_send, kv_recv)
    edges_start(kv_edges)
    scan_pair()
    scan_slot(0)

    def second_dot_a(b):
        rows = rows_at(b, dot_rows)
        q_ref[rows, : second_units * TILE] = jnp.dot(
            normed_ref[rows, :],
            weights(0, first_units, first_units + second_units),
            preferred_element_type=F32,
        ).astype(BF16)

    sweep(count // dot_rows, 1, second_dot_a)

    quarter = HEAD_DIM // 4
    low = lax.rem(iota((size, TILE), 1), 2 * quarter) < quarter

    def turned(part, table):
        x = part.astype(F32)
        other = jnp.where(low, pltpu.roll(x, TILE - quarter, 1), pltpu.roll(x, quarter, 1))
        return (x * table[:, :TILE] + other * table[:, TILE:]).astype(BF16)

    def prepare(b):
        rows = rows_at(b, size)
        for c in range(kv_width // TILE):
            keys_ref[rows, c * TILE : (c + 1) * TILE] = turned(
                kv_ref[rows, c * TILE : (c + 1) * TILE], turn_ref[rows, :]
            )

    sweep(blocks, 0, lambda i: prepare(i + 1))

    band = size + 2 * WINDOW
    band_row = iota((size, band), 0)
    band_col = iota((size, band), 1)
    near = (band_col >= band_row) & (band_col - band_row <= 2 * WINDOW)
    q_lane = iota((size, TILE), 1)
    repeat = q_count * HEAD_DIM // kv_width
    seq_total = seats * count
    slots = {1: 1, 2: blocks - 2}

    def attend(i):
        for r in range(1, min(3, pairs)):
            pl.when(i == slots[r])(lambda: scan_slot(r))

        @pl.when(i == blocks - 2)
        def _():
            edges_arrive(kv_edges)
            prepare(0)
            prepare(blocks + 1)

        b = lax.rem(i + 1, blocks)
        start = pl.multiple_of(b * size, size)
        rows = pl.ds(start, size)
        reach = pl.ds(start, band)
        key_pos = place * count + start - WINDOW + band_col
        valid = near & (key_pos >= 0) & (key_pos < seq_total)
        logs = jnp.zeros((size, TILE), F32)
        table = turn_ref[pl.ds(start + WINDOW, size), :]
        turned_q = jnp.concatenate(
            [turned(q_ref[rows, c * TILE : (c + 1) * TILE], table) for c in range(q_width // TILE)],
            axis=1,
        )
        outs = []
        for h in range(q_count):
            g = h // repeat
            scores = inner_t(
                turned_q[:, h * HEAD_DIM : (h + 1) * HEAD_DIM],
                keys_ref[reach, g * HEAD_DIM : (g + 1) * HEAD_DIM],
            ) * HEAD_DIM ** (-0.5)
            scores = jnp.where(valid, scores, -jnp.inf)
            sink = sink_ref[h]
            top = jnp.maximum(jnp.max(scores, axis=1, keepdims=True), sink)
            expo = jnp.exp(scores - top)
            total = jnp.sum(expo, axis=1, keepdims=True) + jnp.exp(sink - top)
            begin = kv_width + g * HEAD_DIM
            values = jnp.dot(
                expo.astype(BF16),
                kv_ref[reach, begin : begin + HEAD_DIM],
                preferred_element_type=F32,
            )
            outs.append((values / total).astype(BF16))
            logs = jnp.where(q_lane == h, top + jnp.log(total), logs)
        feat_ref[rows, wide:] = jnp.concatenate(outs, axis=1)
        log_ref[:, rows] = logs.T[:q_count]

    sweep(blocks, 2, attend)

    gate_first = first_units + second_units
    until(GROUP * hops * -(-(gate_first + gate_units) // GROUP))

    def gate_dot(b):
        rows = rows_at(b, dot_rows)
        for d in range(2):
            gate_ref[rows, d * gate_units * TILE : (d + 1) * gate_units * TILE] = jnp.dot(
                normed_ref[rows, :],
                weights(d, gate_first, gate_first + gate_units),
                preferred_element_type=F32,
            ).astype(BF16)

    sweep(count // dot_rows, 1, gate_dot)
    for r in range(3, pairs):
        scan_slot(r)
    scan_finish()

    def mix(b):
        rows = rows_at(b, size)
        cum = cum_ref[rows, :]
        step = step_ref[rows, :]
        cum_t = cum.T
        step_t = step.T
        x = cells_ref[rows, :wide]
        writes = cells_ref[rows, wide : wide + state]
        reads = cells_ref[rows, wide + state :]
        cross = inner_t(reads, writes)
        parts = []
        for h in range(heads):
            f = slice(h, h + 1)
            g = slice(heads + h, heads + h + 1)
            seg = jnp.where(row >= col, cum[:, f] - cum_t[f], cum[:, g] - cum_t[g])
            scale = jnp.where(
                row > col, step_t[f], jnp.where(row < col, step_t[g], step_t[f] + step_t[g])
            )
            weight = (cross * jnp.exp(seg) * scale).astype(BF16)
            parts.append(
                jnp.dot(weight, x[:, h * HEAD_DIM : (h + 1) * HEAD_DIM], preferred_element_type=F32)
            )
        y = jnp.concatenate(parts, axis=1)
        fades = jnp.exp(cum)
        for e in range(2):
            held = entry_ref[e, b] + jnp.exp(before_ref[e, b][0:1]) * start_ref[e]
            y = y + through(fades, spreads[e], True) * jnp.dot(
                reads, held.astype(BF16), preferred_element_type=F32
            )
        gate = gate_ref[rows, :].astype(F32)
        y = y * (gate * jax.nn.sigmoid(gate))
        y = y * lax.rsqrt(jnp.mean(y * y, axis=1, keepdims=True) + EPS)
        feat_ref[rows, :wide] = (y * gains_ref[:, width:].astype(F32)).astype(BF16)

    sweep(blocks, 1, mix)

    out_first = gate_first + gate_units
    out_units = per_dir - out_first
    per_peer = 2 * seats // peers

    dot_blocks = count // dot_rows

    core = lax.rem(lane_peer, 2)
    beside = lane_peer + 1 - 2 * core

    def near_copy(tile, b):
        rows = rows_at(b, dot_rows)
        return pltpu.make_async_remote_copy(
            src_ref=part_ref.at[tile, rows],
            dst_ref=near_ref.at[tile, rows],
            send_sem=near_send.at[tile, b],
            recv_sem=near_recv.at[tile, b],
            device_id={"tp": beside},
            device_id_type=mesh_id,
        )

    def far_copy(tile, b, dest, slot):
        rows = rows_at(b, dot_rows)
        at = lax.rem(tile, per_peer)
        return pltpu.make_async_remote_copy(
            src_ref=part_ref.at[tile, rows],
            dst_ref=far_ref.at[slot, at, rows],
            send_sem=far_send.at[tile, b],
            recv_sem=far_recv.at[slot, at, b],
            device_id={"tp": dest},
            device_id_type=mesh_id,
        )

    def dest_of(tile):
        dest = lax.div(tile, per_peer)
        return dest, lax.rem(dest, 2) == core, lax.div(dest, 2) == lax.div(lane_peer, 2)

    def project(d, owner):
        tile = 2 * owner + d
        _, kept, _ = dest_of(tile)
        matrix = ring_ref[d, out_first:, owner].reshape(out_units * unit_rows, TILE)

        def rows_dot(b, _):
            rows = rows_at(b, dot_rows)
            part_ref[tile, rows, :] = jnp.dot(
                feat_ref[rows, :], matrix, preferred_element_type=F32
            ).astype(BF16)
            pl.when(jnp.logical_not(kept))(lambda: near_copy(tile, b).start())
            return 0

        lax.fori_loop(0, dot_blocks, rows_dot, 0)

    def join(d, owner):
        tile = 2 * owner + d
        dest, kept, local = dest_of(tile)

        @pl.when(kept)
        def _():
            def rows_add(b, _):
                rows = rows_at(b, dot_rows)
                near_copy(tile, b).wait_recv()
                part_ref[tile, rows, :] = (
                    part_ref[tile, rows, :].astype(F32) + near_ref[tile, rows, :].astype(F32)
                ).astype(BF16)

                @pl.when(jnp.logical_not(local))
                def _():
                    far_copy(tile, b, dest, lax.div(lane_peer, 2)).start()

                return 0

            lax.fori_loop(0, dot_blocks, rows_add, 0)

    final = sends - GROUP * hops
    limit = sends - GROUP

    def project_own(_):
        for d in range(2):
            project(d, place)

    def ready():
        return min(hops - 1, max(0, (clock[0] - final) // GROUP))

    sweep(1, min(1, limit - clock[0]), project_own)

    def project_hop(k):
        project(0, seat_at(my_pos - k - 1))
        project(1, seat_at(my_pos + k + 1))
        join(0, seat_at(my_pos - k))
        join(1, seat_at(my_pos + k))

    done = 0
    while ready() > done:
        first, more = done, ready() - done
        sweep(more, 1 if clock[0] + more <= limit else 0, lambda i: project_hop(i + first))
        done = first + more
    if done < hops - 1 and clock[0] > final + GROUP * done:
        until(final + GROUP * (done + 1))
        project_hop(jnp.int32(done))
        done += 1
    until(final + GROUP * done)
    sweep(hops - 1 - done, GROUP, lambda i: project_hop(i + done))
    for j in range(GROUP):
        tick(jnp.int32(sends - GROUP + j), last=True)
    project_hop(jnp.int32(hops - 1))
    join(0, seat_at(my_pos - hops))
    join(1, seat_at(my_pos + hops))

    chips = peers // 2

    def add_up(b, _):
        rows = rows_at(b, dot_rows)
        for j in range(per_peer):
            total = part_ref[lane_peer * per_peer + j, rows, :].astype(F32)
            for r in range(1, chips):
                slot = lax.rem(lax.div(lane_peer, 2) + r, chips)
                far_copy(jnp.int32(j), b, 2 * slot + core, slot).wait_recv()
                total = total + far_ref[slot, j, rows, :].astype(F32)
            out_ref[rows, j * TILE : (j + 1) * TILE] = total.astype(BF16)
        return 0

    lax.fori_loop(0, dot_blocks, add_up, 0)

    edges_left(conv_edges)
    edges_left(kv_edges)
    scan_left()
    for r in range(1, seats):
        steps_copy(r).wait_send()

    def ring_left(i, _):
        for d in range(2):
            ring_copy(i, d, 0).wait_send()
        return 0

    lax.fori_loop(0, sends, ring_left, 0)

    def out_left(tile, _):
        dest, kept, local = dest_of(tile)

        @pl.when(jnp.logical_not(kept))
        def _():
            for b in range(dot_blocks):
                near_copy(tile, b).wait_send()

        @pl.when(kept & jnp.logical_not(local))
        def _():
            for b in range(dot_blocks):
                far_copy(tile, b, dest, lax.div(lane_peer, 2)).wait_send()

        return 0

    lax.fori_loop(0, 2 * seats, out_left, 0)


def turn_tables(rows_total):
    quarter = HEAD_DIM // 4
    freqs = np.float32(ROPE_BASE) ** (-np.arange(quarter).astype(np.float32) / np.float32(quarter))
    border = WINDOW // GRID_W
    row_angle = (np.arange(rows_total + 2 * border) - border).astype(np.float32)[:, None] * freqs
    col_angle = np.arange(GRID_W).astype(np.float32)[:, None] * freqs

    def table(angle, first):
        zero = np.zeros_like(angle)
        cosine = np.cos(angle)
        sine = np.sin(angle)
        one = [cosine, cosine, zero, zero] if first else [zero, zero, cosine, cosine]
        two = [-sine, sine, zero, zero] if first else [zero, zero, -sine, sine]
        copies = TILE // HEAD_DIM
        return np.concatenate(one * copies + two * copies, axis=1).astype(np.float32)

    return table(row_angle, True), table(col_angle, False)


def streamed(
    tokens,
    input_gain,
    gate_weight,
    value_weight,
    inflow_weight,
    readout_weight,
    step_weight,
    conv_values,
    conv_inflow,
    conv_readout,
    log_rate,
    group_gain,
    query_weight,
    key_weight,
    vector_weight,
    sink_logit,
    state_out,
    window_out,
):
    count, width = tokens.shape
    seats = lax.axis_size("sp")
    peers = lax.axis_size("tp")
    heads = step_weight.shape[2]
    unit_rows = value_weight.shape[0]
    inflow = flatten_rows(inflow_weight)
    readout = flatten_rows(readout_weight)
    wide = value_weight.shape[1]
    state = inflow.shape[1]
    conv_width = wide + 2 * state
    q_width = query_weight.shape[1]
    kv_width = key_weight.shape[1]
    blocks = count // SSD_BLOCK
    steps = jnp.transpose(step_weight, (1, 2, 0)).reshape(2 * heads, unit_rows)
    row_turn, col_turn = turn_tables(seats * count // GRID_W)
    units = chunk_maps(
        {
            "value": value_weight.shape,
            "inflow": inflow.shape,
            "readout": readout.shape,
            "query": query_weight.shape,
            "key": key_weight.shape,
            "vector": vector_weight.shape,
            "gate": gate_weight.shape,
            "state_out": state_out.shape,
            "window_out": window_out.shape,
        }
    )
    per_dir = len(units[0])
    sends = per_dir * (seats - 1)
    vmem = pl.BlockSpec(memory_space=pltpu.VMEM)
    smem = pl.BlockSpec(memory_space=pltpu.SMEM)
    hbm = pl.BlockSpec(memory_space=pltpu.HBM)
    dma = pltpu.SemaphoreType.DMA
    scratch = [
        pltpu.VMEM((2, per_dir, seats, unit_rows, TILE), BF16),
        pltpu.VMEM((seats, 2 * heads, unit_rows), BF16),
        pltpu.VMEM((count, width), BF16),
        pltpu.VMEM((count, width), BF16),
        pltpu.VMEM((count + 2 * PAD, conv_width), BF16),
        pltpu.VMEM((count, conv_width), BF16),
        pltpu.VMEM((count, TILE), F32),
        pltpu.VMEM((count, TILE), F32),
        pltpu.VMEM((2, blocks, state, wide), F32),
        pltpu.VMEM((2, blocks, 8, wide), F32),
        pltpu.VMEM((2, state, wide), F32),
        pltpu.VMEM((2, 8, wide), F32),
        pltpu.VMEM((2, 2, state + PAD, wide), BF16),
        pltpu.VMEM((2, 2, state + PAD, wide), BF16),
        pltpu.VMEM((2, state, wide), F32),
        pltpu.VMEM((2, 8, wide), F32),
        pltpu.VMEM((2, state, wide), F32),
        pltpu.VMEM((count, wide), BF16),
        pltpu.VMEM((count, q_width), BF16),
        pltpu.VMEM((count + 2 * WINDOW, 2 * kv_width), BF16),
        pltpu.VMEM((count + 2 * WINDOW, kv_width), BF16),
        pltpu.VMEM((count + 2 * WINDOW, 2 * TILE), F32),
        pltpu.VMEM((count, wide + q_width), BF16),
        pltpu.VMEM((2 * seats, count, TILE), BF16),
        pltpu.VMEM((2 * seats, count, TILE), BF16),
        pltpu.VMEM((peers // 2, 2 * seats // peers, count, TILE), BF16),
        dma((2, sends)),
        dma((2, sends)),
        dma((seats,)),
        dma((seats,)),
        dma((2 * per_dir + 1,)),
        dma((2,)),
        dma((2,)),
        dma((2,)),
        dma((2,)),
        dma((2, 2)),
        dma((2, 2)),
        dma((2 * seats, count // (2 * SSD_BLOCK))),
        dma((2 * seats, count // (2 * SSD_BLOCK))),
        dma((2 * seats, count // (2 * SSD_BLOCK))),
        dma((peers // 2, 2 * seats // peers, count // (2 * SSD_BLOCK))),
    ]
    mixed, logs = pl.pallas_call(
        functools.partial(layer_kernel, (seats, peers, units)),
        out_shape=(
            jax.ShapeDtypeStruct((count, width // peers), BF16),
            jax.ShapeDtypeStruct((q_width // HEAD_DIM, count), F32),
        ),
        in_specs=[hbm] + [vmem] * 5 + [smem] + [vmem] * 3 + [hbm] * 9,
        out_specs=(vmem, vmem),
        scratch_shapes=scratch,
        compiler_params=pltpu.CompilerParams(
            collective_id=0, has_side_effects=True, vmem_limit_bytes=60 * 2**20
        ),
    )(
        tokens,
        jnp.concatenate([input_gain, group_gain])[None],
        conv_values,
        flatten_rows(conv_inflow),
        flatten_rows(conv_readout),
        jnp.transpose(log_rate, (0, 2, 1)),
        sink_logit,
        jnp.asarray(row_turn),
        jnp.asarray(col_turn),
        steps,
        value_weight,
        inflow,
        readout,
        query_weight,
        key_weight,
        vector_weight,
        gate_weight,
        state_out,
        window_out,
    )
    return mixed, logs.T


def streams(arrays):
    tokens, value, inflow, key, out = arrays[0], arrays[3], arrays[4], arrays[13], arrays[16]
    seats = lax.axis_size("sp")
    return (
        seats % 2 == 0
        and value.shape[0] % TILE == 0
        and out.shape[0] % value.shape[0] == 0
        and out.shape[1] == 2 * TILE
        and value.shape[1] == 4 * TILE
        and inflow.shape[1] * inflow.shape[2] == TILE
        and key.shape[1] == TILE
        and tokens.shape[0] % (2 * SSD_BLOCK) == 0
        and tokens.shape[0] >= 4 * SSD_BLOCK
        and tokens.shape[0] % GRID_W == 0
        and tokens.shape[1] == seats * value.shape[0]
        and seats == 2 * lax.axis_size("tp")
    )


def layer(*arrays):
    if streams(arrays):
        return streamed(*arrays)
    return shards(*arrays)


def shards(
    tokens,
    input_gain,
    gate_weight,
    value_weight,
    inflow_weight,
    readout_weight,
    step_weight,
    conv_values,
    conv_inflow,
    conv_readout,
    log_rate,
    group_gain,
    query_weight,
    key_weight,
    vector_weight,
    sink_logit,
    state_out,
    window_out,
):
    count = tokens.shape[0]
    offset = lax.axis_index("sp") * count
    seq_total = count * lax.axis_size("sp")
    heads = step_weight.shape[2]
    groups = inflow_weight.shape[1]
    state_len = inflow_weight.shape[2]
    inner_local = value_weight.shape[1]
    q_count = query_weight.shape[1] // HEAD_DIM
    kv_count = key_weight.shape[1] // HEAD_DIM
    kv_width = key_weight.shape[1]
    wide = tokens.astype(F32)
    normed = (
        wide
        * lax.rsqrt(jnp.mean(wide * wide, axis=1, keepdims=True) + EPS)
        * input_gain.astype(F32)
    ).astype(BF16)

    def whole(parts):
        return lax.all_gather(jnp.concatenate(parts, axis=1), "sp", axis=0, tiled=True)

    own = (flatten_rows(inflow_weight), flatten_rows(readout_weight), flatten_rows(step_weight))
    first_matrix = whole((value_weight,) + own)
    rest_matrix = whole((key_weight, vector_weight, gate_weight, query_weight))
    first = jnp.dot(normed, first_matrix, preferred_element_type=F32)
    rest = jnp.dot(normed, rest_matrix, preferred_element_type=F32).astype(BF16)
    conv_width = inner_local + 2 * groups * state_len
    conv_input = first[:, :conv_width].astype(BF16)
    step = jax.nn.softplus(first[:, conv_width:])
    keyvals = rest[:, : 2 * kv_width]
    gate = rest[:, 2 * kv_width : 2 * kv_width + inner_local]
    queries = rest[:, 2 * kv_width + inner_local :]

    reach_rows = CONV // 2
    padded = with_halo(conv_input, (("sp", 0),), CONV // 2).astype(F32)
    taps = jnp.concatenate(
        [conv_values, flatten_rows(conv_inflow), flatten_rows(conv_readout)], axis=1
    ).astype(F32)
    conv_sum = padded[0:count] * taps[0]
    for tap in range(1, 2 * reach_rows + 1):
        conv_sum = conv_sum + padded[tap : tap + count] * taps[tap]
    cells = jax.nn.silu(conv_sum).astype(BF16)
    rates = jnp.transpose(log_rate, (1, 0, 2)).reshape(count, 2 * heads)
    sd = jnp.concatenate([step, -jnp.exp(rates) * step], axis=1)
    blocks = count // SSD_BLOCK
    sdt = jnp.transpose(sd.reshape(blocks, SSD_BLOCK, 4 * heads), (0, 2, 1))

    summary = call(
        summary_kernel,
        jax.ShapeDtypeStruct((2, state_len + PAD, inner_local), BF16),
        (cells, sd),
    )
    everyone = lax.all_gather(summary, "sp")
    out_stack, everyone = lax.optimization_barrier(
        (jnp.concatenate([state_out, window_out], axis=0), everyone)
    )
    out_matrix = lax.all_gather(out_stack, "sp", axis=1, tiled=True)
    seats = lax.axis_size("sp")
    place = lax.axis_index("sp")
    totals = everyone[:, :, state_len].astype(F32) + everyone[:, :, state_len + 1].astype(F32)
    seat = jnp.arange(seats)
    starts = []
    for e in range(2):
        ahead = seat < place if e == 0 else seat > place
        between = (seat[None, :] > seat[:, None]) if e == 0 else (seat[None, :] < seat[:, None])
        between = (between & ahead[None, :])[:, :, None]
        fade = jnp.sum(jnp.where(between, totals[None, :, e], 0.0), axis=1)
        fade = jnp.where(ahead[:, None], jnp.exp(fade), 0.0)
        starts.append(jnp.sum(fade[:, None, :] * everyone[:, e, :state_len].astype(F32), axis=0))
    starts = jnp.stack(starts)
    state_features = call(
        mixer_kernel,
        jax.ShapeDtypeStruct((count, inner_local), BF16),
        (cells, sd, sdt, starts, gate, group_gain[None]),
        (
            pltpu.VMEM((blocks, state_len, inner_local), BF16),
            pltpu.VMEM((state_len, inner_local), F32),
        ),
        flops=10**10,
    )

    beside = with_halo(keyvals, (("sp", 0),), WINDOW)
    quarter = HEAD_DIM // 4
    freqs = ROPE_BASE ** (-jnp.arange(quarter).astype(F32) / quarter)
    spots = offset - WINDOW + jnp.arange(count + 2 * WINDOW, dtype=jnp.int32)
    row_angle = (spots // GRID_W).astype(F32)[:, None] * freqs
    col_angle = (spots % GRID_W).astype(F32)[:, None] * freqs
    angles = jnp.concatenate([row_angle, col_angle], axis=1)
    cosine = jnp.cos(angles)
    sine = jnp.sin(angles)

    def doubled(table, sign):
        low = table[:, :quarter]
        high = table[:, quarter:]
        return [sign * low, low, sign * high, high]

    turn = jnp.concatenate(doubled(cosine, 1.0) + doubled(sine, -1.0), axis=1)
    channel = jnp.arange(HEAD_DIM)
    partner = channel + jnp.where(channel % (2 * quarter) < quarter, quarter, -quarter)
    swap = (channel[:, None] == partner[None, :]).astype(BF16)
    limits = jnp.stack([offset, seq_total]).astype(jnp.int32)
    window_features, log_total = call(
        attend_kernel,
        (
            jax.ShapeDtypeStruct((count, q_count * HEAD_DIM), BF16),
            jax.ShapeDtypeStruct((count, q_count), F32),
        ),
        (limits, sink_logit, queries, beside, turn, swap),
        (pltpu.VMEM((kv_count, count + 2 * WINDOW, HEAD_DIM), BF16),),
        scalars=2,
        flops=10**10,
    )
    features = jnp.concatenate([state_features, window_features], axis=1)
    terms = jnp.dot(features, out_matrix, preferred_element_type=F32)
    mixed = lax.psum_scatter(terms.astype(BF16), "tp", scatter_dimension=1, tiled=True)
    return (mixed, log_total)


def solution(mesh):
    placed = (
        P("sp", None),
        P(),
        P("sp", "tp"),
        P("sp", "tp"),
        P("sp", "tp", None),
        P("sp", "tp", None),
        P("sp", None, "tp"),
        P(None, "tp"),
        P(None, "tp", None),
        P(None, "tp", None),
        P(None, "sp", "tp"),
        P("tp"),
        P("sp", "tp"),
        P("sp", "tp"),
        P("sp", "tp"),
        P("tp"),
        P("tp", "sp"),
        P("tp", "sp"),
    )
    return jax.shard_map(
        layer,
        mesh=mesh,
        in_specs=placed,
        out_specs=(P("sp", "tp"), P("sp", "tp")),
        check_vma=False,
    )
```

```python
import functools

import jax
import jax.numpy as jnp
import numpy as np
from jax import lax
from jax.experimental import pallas as pl
from jax.experimental.pallas import tpu as pltpu
from jax.sharding import PartitionSpec as P


HEAD_DIM = 64
CONV = 5
SSD_BLOCK = 128
WINDOW = 128
GRID_W = 64


EPS = 1e-06
ROPE_BASE = 10000.0
HIGHEST = lax.Precision.HIGHEST
F32 = jnp.float32
BF16 = jnp.bfloat16
PAD = 16


def iota(shape, dim):
    return lax.broadcasted_iota(jnp.int32, shape, dim)


def exact(a, b):
    return jnp.dot(a, b, precision=HIGHEST, preferred_element_type=F32)


def spread(heads):
    shape = (heads, heads * HEAD_DIM)
    return (iota(shape, 1) // HEAD_DIM == iota(shape, 0)).astype(F32)


def inner_t(a, b):
    return lax.dot_general(a, b, (((1,), (1,)), ((), ())), preferred_element_type=F32)


def outer_t(a, b):
    return lax.dot_general(a, b, (((0,), (0,)), ((), ())), preferred_element_type=F32)


def summary_kernel(cells_ref, sd_ref, out_ref):
    count = cells_ref.shape[0]
    heads = sd_ref.shape[1] // 4
    wide = heads * HEAD_DIM
    state = out_ref.shape[1] - PAD
    x = cells_ref[:, :wide].astype(F32)
    writes = cells_ref[:, wide : wide + state]
    expand = spread(heads)
    row = iota((count, count), 0)
    col = iota((count, count), 1)
    for e in range(2):
        step = sd_ref[:, e * heads : (e + 1) * heads]
        decay = sd_ref[:, (2 + e) * heads : (3 + e) * heads]
        span = (col > row) if e == 0 else (col < row)
        rest = exact(span.astype(F32), decay)
        scaled = (x * exact(jnp.exp(rest) * step, expand)).astype(BF16)
        out_ref[e, :state, :] = outer_t(writes, scaled).astype(BF16)
        total = exact(jnp.broadcast_to(jnp.sum(decay, axis=0, keepdims=True), (8, heads)), expand)
        total = total[0:1]
        high = total.astype(BF16).astype(F32)
        place = iota((PAD, wide), 0)
        packed = jnp.where(place == 0, high, jnp.where(place == 1, total - high, 0.0))
        out_ref[e, state:, :] = packed.astype(BF16)


def mixer_kernel(cells_ref, sd_ref, sdt_ref, start_ref, gate_ref, gain_ref, out_ref, back_ref, carry_ref):
    blocks, _, size = sdt_ref.shape
    heads = sd_ref.shape[1] // 4
    wide = heads * HEAD_DIM
    state = start_ref.shape[1]
    expand = spread(heads)
    row = iota((size, size), 0)
    col = iota((size, size), 1)
    lower = (row >= col).astype(F32)
    upper = (row <= col).astype(F32)

    carry_ref[...] = start_ref[1]

    def backward(index, _):
        block = blocks - 1 - index
        rows = pl.ds(pl.multiple_of(block * size, size), size)
        back_ref[block] = carry_ref[...].astype(BF16)
        step = sd_ref[rows, heads : 2 * heads]
        cum = exact(upper, sd_ref[rows, 3 * heads : 4 * heads])
        edge = cum[0:1]
        x = cells_ref[rows, :wide].astype(F32)
        scaled = (x * exact(jnp.exp(edge - cum) * step, expand)).astype(BF16)
        fresh = outer_t(cells_ref[rows, wide : wide + state], scaled)
        fade = exact(jnp.broadcast_to(jnp.exp(edge), (8, heads)), expand)[0:1]
        carry_ref[...] = fade * carry_ref[...] + fresh
        return 0

    lax.fori_loop(0, blocks, backward, 0)
    carry_ref[...] = start_ref[0]

    def forward(block, _):
        rows = pl.ds(pl.multiple_of(block * size, size), size)
        cum_f = exact(lower, sd_ref[rows, 2 * heads : 3 * heads])
        cum_b = exact(upper, sd_ref[rows, 3 * heads : 4 * heads])
        flat = sdt_ref[block]
        step_ft = flat[:heads]
        step_bt = flat[heads : 2 * heads]
        cum_ft = exact(flat[2 * heads : 3 * heads], upper)
        cum_bt = exact(flat[3 * heads :], lower)
        x = cells_ref[rows, :wide]
        writes = cells_ref[rows, wide : wide + state]
        reads = cells_ref[rows, wide + state :]
        cross = inner_t(reads, writes)
        parts = []
        for h in range(heads):
            one = slice(h, h + 1)
            seg = jnp.where(
                row >= col, cum_f[:, one] - cum_ft[one], cum_b[:, one] - cum_bt[one]
            )
            scale = jnp.where(
                row > col,
                step_ft[one],
                jnp.where(row < col, step_bt[one], step_ft[one] + step_bt[one]),
            )
            weight = (cross * jnp.exp(seg) * scale).astype(BF16)
            parts.append(
                jnp.dot(
                    weight, x[:, h * HEAD_DIM : (h + 1) * HEAD_DIM], preferred_element_type=F32
                )
            )
        y = jnp.concatenate(parts, axis=1)
        y = y + exact(jnp.exp(cum_f), expand) * jnp.dot(
            reads, carry_ref[...].astype(BF16), preferred_element_type=F32
        )
        y = y + exact(jnp.exp(cum_b), expand) * jnp.dot(
            reads, back_ref[block], preferred_element_type=F32
        )
        gate = gate_ref[rows, :].astype(F32)
        y = y * (gate * jax.nn.sigmoid(gate))
        y = y * lax.rsqrt(jnp.mean(y * y, axis=1, keepdims=True) + EPS)
        out_ref[rows, :] = (y * gain_ref[...].astype(F32)).astype(BF16)
        edge = cum_f[size - 1 : size]
        step = sd_ref[rows, :heads]
        scaled = (x.astype(F32) * exact(jnp.exp(edge - cum_f) * step, expand)).astype(BF16)
        fade = exact(jnp.broadcast_to(jnp.exp(edge), (8, heads)), expand)[0:1]
        carry_ref[...] = fade * carry_ref[...] + outer_t(writes, scaled)
        return 0

    lax.fori_loop(0, blocks, forward, 0)


def attend_kernel(place_ref, sink_ref, q_ref, kv_ref, turn_ref, swap_ref, out_ref, log_ref, keys_ref):
    count = q_ref.shape[0]
    q_count = q_ref.shape[1] // HEAD_DIM
    kv_width = kv_ref.shape[1] // 2
    repeat = q_count * HEAD_DIM // kv_width
    size = SSD_BLOCK
    band = size + 2 * WINDOW
    swap = swap_ref[...]

    def turned(part, rows):
        swapped = jnp.dot(part, swap, preferred_element_type=F32)
        table = turn_ref[rows, :]
        return (part.astype(F32) * table[:, :HEAD_DIM] + swapped * table[:, HEAD_DIM:]).astype(BF16)

    def prepare(block, _):
        rows = pl.ds(pl.multiple_of(block * size, size), size)
        for g in range(kv_width // HEAD_DIM):
            keys_ref[g, rows, :] = turned(
                kv_ref[rows, g * HEAD_DIM : (g + 1) * HEAD_DIM], rows
            )
        return 0

    lax.fori_loop(0, kv_ref.shape[0] // size, prepare, 0)
    row = iota((size, band), 0)
    col = iota((size, band), 1)
    near = (col >= row) & (col - row <= 2 * WINDOW)
    lane = iota((size, q_count), 1)

    def one(block, _):
        start = pl.multiple_of(block * size, size)
        rows = pl.ds(start, size)
        reach = pl.ds(start, band)
        key_pos = place_ref[0] + start - WINDOW + col
        valid = near & (key_pos >= 0) & (key_pos < place_ref[1])
        logs = jnp.zeros((size, q_count), F32)
        outs = []
        for h in range(q_count):
            g = h // repeat
            query = turned(
                q_ref[rows, h * HEAD_DIM : (h + 1) * HEAD_DIM], pl.ds(start + WINDOW, size)
            )
            scores = inner_t(query, keys_ref[g, reach, :]) * HEAD_DIM ** (-0.5)
            scores = jnp.where(valid, scores, -jnp.inf)
            sink = sink_ref[h]
            top = jnp.maximum(jnp.max(scores, axis=1, keepdims=True), sink)
            expo = jnp.exp(scores - top)
            total = jnp.sum(expo, axis=1, keepdims=True) + jnp.exp(sink - top)
            first = kv_width + g * HEAD_DIM
            values = jnp.dot(
                expo.astype(BF16),
                kv_ref[reach, first : first + HEAD_DIM],
                preferred_element_type=F32,
            )
            outs.append((values / total).astype(BF16))
            logs = jnp.where(lane == h, top + jnp.log(total), logs)
        out_ref[rows, :] = jnp.concatenate(outs, axis=1)
        log_ref[rows, :] = logs
        return 0

    lax.fori_loop(0, count // size, one, 0)


def call(kernel, out_shape, args, scratch=(), scalars=0, flops=10**8):
    vmem = pl.BlockSpec(memory_space=pltpu.VMEM)
    smem = pl.BlockSpec(memory_space=pltpu.SMEM)
    return pl.pallas_call(
        kernel,
        out_shape=out_shape,
        in_specs=[smem] * scalars + [vmem] * (len(args) - scalars),
        out_specs=jax.tree.map(lambda _: vmem, out_shape),
        scratch_shapes=list(scratch),
        cost_estimate=pl.CostEstimate(flops=flops, bytes_accessed=4 * 10**6, transcendentals=0),
        compiler_params=pltpu.CompilerParams(vmem_limit_bytes=40 * 2**20),
    )(*args)


def with_halo(cells, sides, width):
    for axis, dim in sides:
        count = lax.axis_size(axis)
        ends = count - 1
        head = lax.slice_in_dim(cells, 0, width, axis=dim)
        tail = lax.slice_in_dim(cells, cells.shape[dim] - width, cells.shape[dim], axis=dim)
        cells = jnp.concatenate(
            [
                lax.ppermute(tail, axis, [(i, (i + 1) % count) for i in range(ends)]),
                cells,
                lax.ppermute(head, axis, [((i + 1) % count, i) for i in range(ends)]),
            ],
            axis=dim,
        )
    return cells


def flatten_rows(weight):
    return weight.reshape(weight.shape[0], -1)


TILE = 128
GROUP = 3


def split3(v):
    high = v.astype(BF16)
    rest = v - high.astype(F32)
    mid = rest.astype(BF16)
    return high, mid, (rest - mid.astype(F32)).astype(BF16)


def through(left, right, left_wide):
    total = None
    for part in split3(left if left_wide else right):
        one = jnp.dot(part, right, preferred_element_type=F32) if left_wide else jnp.dot(
            left, part, preferred_element_type=F32
        )
        total = one if total is None else total + one
    return total


def chunk_maps(shapes):
    rows = shapes["value"][0]

    def tiles(name):
        return [(name, 0, c) for c in range(shapes[name][1] // TILE)]

    units = ([], [])
    for names in (("value", "inflow", "readout"), ("query", "key", "vector"), ("gate",)):
        flat = [t for name in names for t in tiles(name)]
        half = len(flat) // 2
        for d in range(2):
            units[d].extend(flat[d * half : (d + 1) * half])
    for d in range(2):
        for name in ("state_out", "window_out"):
            units[d].extend((name, r, d) for r in range(shapes[name][0] // rows))
    return units


def layer_kernel(
    cfg,
    tokens_hbm,
    gain_ref,
    norm_gain_ref,
    value_taps_ref,
    inflow_taps_ref,
    readout_taps_ref,
    rates_ref,
    sink_ref,
    row_turn_ref,
    col_turn_ref,
    steps_ref,
    value_ref,
    inflow_ref,
    readout_ref,
    query_ref,
    key_ref,
    vector_ref,
    gate_w_ref,
    state_out_ref,
    window_out_ref,
    out_ref,
    log_ref,
    ring_ref,
    steps_all_ref,
    tokens_ref,
    normed_ref,
    conv_ref,
    cells_ref,
    step_ref,
    cum_ref,
    entry_ref,
    before_ref,
    carry_ref,
    total_ref,
    scan_send_ref,
    scan_recv_ref,
    start_ref,
    reach_ref,
    pair_ref,
    gate_ref,
    q_ref,
    kv_ref,
    keys_ref,
    turn_ref,
    feat_ref,
    part_ref,
    near_ref,
    far_ref,
    send_sem,
    recv_sem,
    steps_send,
    steps_recv,
    local_sem,
    halo_send,
    halo_recv,
    kv_send,
    kv_recv,
    scan_ssem,
    scan_rsem,
    near_send,
    near_recv,
    far_send,
    far_recv,
):
    seats, peers, units = cfg
    count, width = tokens_hbm.shape
    unit_rows = ring_ref.shape[3]
    heads = steps_ref.shape[0] // 2
    wide = heads * HEAD_DIM
    state = inflow_ref.shape[1]
    conv_width = wide + 2 * state
    q_width = query_ref.shape[1]
    q_count = q_width // HEAD_DIM
    kv_width = key_ref.shape[1]
    per_dir = len(units[0])
    hops = seats - 1
    sends = per_dir * hops
    place = lax.axis_index("sp")
    lane_peer = lax.axis_index("tp")
    half = seats // 2
    blocks = count // SSD_BLOCK
    size = SSD_BLOCK
    mesh_id = pl.DeviceIdType.MESH

    def seat_at(pos):
        pos = lax.rem(pos + 2 * seats, seats)
        late = lax.div(pos, half)
        return (1 - late) * 2 * pos + late * (2 * (seats - 1 - pos) + 1)

    odd = lax.rem(place, 2)
    my_pos = (1 - odd) * lax.div(place, 2) + odd * (seats - 1 - lax.div(place, 2))
    nexts = (seat_at(my_pos + 1), seat_at(my_pos - 1))

    barrier = pltpu.get_barrier_semaphore()
    for r in range(1, seats):
        pl.semaphore_signal(
            barrier, inc=1, device_id={"sp": lax.rem(place + r, seats)}, device_id_type=mesh_id
        )
    for r in range(1, peers):
        pl.semaphore_signal(
            barrier, inc=1, device_id={"tp": lax.rem(lane_peer + r, peers)}, device_id_type=mesh_id
        )

    sources = {
        "value": value_ref,
        "inflow": inflow_ref,
        "readout": readout_ref,
        "query": query_ref,
        "key": key_ref,
        "vector": vector_ref,
        "gate": gate_w_ref,
        "state_out": state_out_ref,
        "window_out": window_out_ref,
    }
    locals_ = []
    for d in range(2):
        for u, (name, r, c) in enumerate(units[d]):
            locals_.append(
                pltpu.make_async_copy(
                    sources[name].at[pl.ds(r * unit_rows, unit_rows), pl.ds(c * TILE, TILE)],
                    ring_ref.at[d, u, place],
                    local_sem.at[d * per_dir + u],
                )
            )
    for copy in locals_:
        copy.start()
    tokens_in = pltpu.make_async_copy(tokens_hbm, tokens_ref, local_sem.at[2 * per_dir])
    tokens_in.start()
    steps_all_ref[place] = steps_ref[...]
    first_ones = [d * per_dir + u for d in range(2) for u in range(GROUP)]
    for at in first_ones:
        locals_[at].wait()
    pl.semaphore_wait(barrier, hops + peers - 1)

    def ring_copy(i, d, behind):
        turn = lax.div(i, GROUP * hops)
        k = lax.rem(lax.div(i, GROUP), hops) + behind
        unit = GROUP * turn + lax.rem(i, GROUP)
        owner = seat_at(my_pos - k) if d == 0 else seat_at(my_pos + k)
        block = ring_ref.at[d, unit, owner]
        return pltpu.make_async_remote_copy(
            src_ref=block,
            dst_ref=block,
            send_sem=send_sem.at[d, i],
            recv_sem=recv_sem.at[d, i],
            device_id={"sp": nexts[d]},
            device_id_type=mesh_id,
        )

    def tick(i, last=False):
        for d in range(2):
            ring_copy(i, d, 1).wait_recv()
            if not last:
                ring_copy(i + GROUP, d, 0).start()

    for j in range(GROUP):
        for d in range(2):
            ring_copy(jnp.int32(j), d, 0).start()

    for at, copy in enumerate(locals_):
        if at not in first_ones:
            copy.wait()

    def steps_copy(r):
        return pltpu.make_async_remote_copy(
            src_ref=steps_ref,
            dst_ref=steps_all_ref.at[place],
            send_sem=steps_send.at[r],
            recv_sem=steps_recv.at[place],
            device_id={"sp": lax.rem(place + r, seats)},
            device_id_type=mesh_id,
        )

    for r in range(1, seats):
        steps_copy(r).start()

    clock = [0]

    def sweep(trips, per_trip, body):
        base = clock[0]

        def run(i, _):
            for j in range(int(per_trip)):
                tick(base + i * int(per_trip) + j)
            if per_trip == 0.5:
                pl.when(lax.rem(i, 2) == 0)(lambda: tick(base + lax.div(i, 2)))
            body(i)
            return 0

        lax.fori_loop(0, trips, run, 0)
        clock[0] = base + (trips + 1) // 2 if per_trip == 0.5 else base + trips * per_trip

    def until(goal):
        if goal > clock[0]:
            sweep(goal - clock[0], 1, lambda i: None)

    def rows_at(index, length, first=0):
        return pl.ds(pl.multiple_of(index * length, length) + first, length)

    def normalise(b):
        rows = rows_at(b, size)
        x = tokens_ref[rows, :].astype(F32)
        scale = lax.rsqrt(jnp.mean(x * x, axis=1, keepdims=True) + EPS)
        normed_ref[rows, :] = (x * scale * gain_ref[...].astype(F32).reshape(1, width)).astype(BF16)

    tokens_in.wait()
    sweep(blocks, 1, normalise)
    table_row = place * (count // GRID_W)

    def fill_turn(i):
        turn_ref[rows_at(i, GRID_W), :] = col_turn_ref[...] + row_turn_ref[pl.ds(table_row + i, 1), :]

    sweep(turn_ref.shape[0] // GRID_W, 0, fill_turn)
    step_ref[...] = jnp.zeros_like(step_ref)
    carry_ref[...] = jnp.zeros_like(carry_ref)
    total_ref[...] = jnp.zeros_like(total_ref)
    start_ref[...] = jnp.zeros_like(start_ref)
    reach_ref[...] = jnp.zeros_like(reach_ref)

    first_edge = place == 0
    last_edge = place == seats - 1

    @pl.when(first_edge)
    def _():
        conv_ref[:PAD, :] = jnp.zeros((PAD, conv_width), BF16)
        kv_ref[:WINDOW, :] = jnp.zeros((WINDOW, 2 * kv_width), BF16)

    @pl.when(last_edge)
    def _():
        conv_ref[PAD + count :, :] = jnp.zeros((PAD, conv_width), BF16)
        kv_ref[WINDOW + count :, :] = jnp.zeros((WINDOW, 2 * kv_width), BF16)

    def weights(d, first, last):
        return jnp.concatenate(
            [ring_ref[d, u].reshape(seats * unit_rows, TILE) for u in range(first, last)], axis=1
        )

    first_units = conv_width // (2 * TILE)
    second_units = (q_width + 2 * kv_width) // (2 * TILE)
    gate_units = wide // (2 * TILE)
    until(GROUP * hops * -(-first_units // GROUP))
    for r in range(1, seats):
        peer = lax.rem(place + r, seats)
        pltpu.make_async_remote_copy(
            src_ref=steps_ref,
            dst_ref=steps_all_ref.at[peer],
            send_sem=steps_send.at[r],
            recv_sem=steps_recv.at[peer],
            device_id={"sp": peer},
            device_id_type=mesh_id,
        ).wait_recv()

    dot_rows = 2 * size

    def first_dot(b):
        rows = rows_at(b, dot_rows)
        here = normed_ref[rows, :]
        for d in range(2):
            conv_ref[rows_at(b, dot_rows, PAD), d * first_units * TILE : (d + 1) * first_units * TILE] = (
                jnp.dot(here, weights(d, 0, first_units), preferred_element_type=F32).astype(BF16)
            )
        steps = jnp.concatenate([steps_all_ref[o] for o in range(seats)], axis=1)
        raw = inner_t(here, steps)
        step = jnp.maximum(raw, 0.0) + jnp.log1p(jnp.exp(-jnp.abs(raw)))
        step_ref[rows, : 2 * heads] = step

    sweep(count // dot_rows, 1, first_dot)

    def edge_copies(ref, length, ssem, rsem):
        inner = ref.shape[0] - 2 * length
        up = pltpu.make_async_remote_copy(
            src_ref=ref.at[pl.ds(inner, length)],
            dst_ref=ref.at[pl.ds(0, length)],
            send_sem=ssem.at[0],
            recv_sem=rsem.at[0],
            device_id={"sp": lax.rem(place + 1, seats)},
            device_id_type=mesh_id,
        )
        down = pltpu.make_async_remote_copy(
            src_ref=ref.at[pl.ds(length, length)],
            dst_ref=ref.at[pl.ds(length + inner, length)],
            send_sem=ssem.at[1],
            recv_sem=rsem.at[1],
            device_id={"sp": lax.rem(place + hops, seats)},
            device_id_type=mesh_id,
        )
        return up, down

    def edges_start(pair):
        pl.when(jnp.logical_not(last_edge))(lambda: pair[0].start())
        pl.when(jnp.logical_not(first_edge))(lambda: pair[1].start())

    def edges_arrive(pair):
        pl.when(jnp.logical_not(first_edge))(lambda: pair[0].wait_recv())
        pl.when(jnp.logical_not(last_edge))(lambda: pair[1].wait_recv())

    def edges_left(pair):
        pl.when(jnp.logical_not(last_edge))(lambda: pair[0].wait_send())
        pl.when(jnp.logical_not(first_edge))(lambda: pair[1].wait_send())

    conv_edges = edge_copies(conv_ref, PAD, halo_send, halo_recv)
    edges_start(conv_edges)
    taps = jnp.concatenate(
        [ref[...] for ref in (value_taps_ref, inflow_taps_ref, readout_taps_ref)], axis=1
    ).astype(F32)
    lane = iota((size, TILE), 1)
    row = iota((size, size), 0)
    col = iota((size, size), 1)
    lower = (row >= col).astype(BF16)
    upper = (row <= col).astype(BF16)
    spread_row = iota((TILE, wide), 0)
    spread_col = iota((TILE, wide), 1) // HEAD_DIM
    spreads = [(spread_row - e * heads == spread_col).astype(BF16) for e in range(2)]

    def sums(b):
        rows = rows_at(b, size)
        filler = jnp.zeros((TILE - 2 * heads, size), F32)
        rates = jnp.concatenate([rates_ref[0, :, rows], rates_ref[1, :, rows], filler], axis=0).T
        decay = -jnp.exp(rates) * step_ref[rows, :]
        cum_ref[rows, :] = jnp.where(
            lane < heads, through(lower, decay, False), through(upper, decay, False)
        )

    sweep(blocks, 1, sums)
    edges_arrive(conv_edges)

    def convolve(b):
        rows = rows_at(b, size)
        padded = conv_ref[pl.ds(pl.multiple_of(b * size, size), size + 2 * PAD), :].astype(F32)
        first = PAD - CONV // 2
        total = padded[first : first + size] * taps[0:1]
        for tap in range(1, CONV):
            total = total + padded[first + tap : first + tap + size] * taps[tap : tap + 1]
        cells_ref[rows, :] = (total * jax.nn.sigmoid(total)).astype(BF16)

    sweep(blocks, 0.5, convolve)

    def summarise(i):
        for e in range(2):
            b = i if e == 0 else blocks - 1 - i
            rows = rows_at(b, size)
            cum = cum_ref[rows, :]
            edge = cum[size - 1 : size] if e == 0 else cum[0:1]
            scale = through(jnp.exp(edge - cum) * step_ref[rows, :], spreads[e], True)
            scaled = (cells_ref[rows, :wide].astype(F32) * scale).astype(BF16)
            fresh = outer_t(cells_ref[rows, wide : wide + state], scaled)
            edges = through(jnp.broadcast_to(edge, (8, TILE)), spreads[e], True)
            entry_ref[e, b] = carry_ref[e]
            before_ref[e, b] = total_ref[e]
            carry_ref[e] = jnp.exp(edges[0:1]) * carry_ref[e] + fresh
            total_ref[e] = total_ref[e] + edges

    sweep(blocks, 0.5, summarise)

    pair = lax.div(place, 2)
    pairs = seats // 2

    def scan_copy(stage, e):
        far = place + 1 - 2 * odd if stage == 0 else lax.rem(place + (2 if e == 0 else seats - 2), seats)
        return pltpu.make_async_remote_copy(
            src_ref=scan_send_ref.at[e, stage],
            dst_ref=scan_recv_ref.at[e, stage],
            send_sem=scan_ssem.at[e, stage],
            recv_sem=scan_rsem.at[e, stage],
            device_id={"sp": far},
            device_id_type=mesh_id,
        )

    def scan_start(stage, e, states, total):
        scan_send_ref[e, stage, :state] = states.astype(BF16)
        high = total.astype(BF16).astype(F32)
        at = iota((PAD, wide), 0)
        scan_send_ref[e, stage, state:] = jnp.where(
            at == 0, high, jnp.where(at == 1, total - high, 0.0)
        ).astype(BF16)
        scan_copy(stage, e).start()

    def scan_read(stage, e):
        far = scan_recv_ref[e, stage]
        decays = far[state : state + 8].astype(F32)
        return far[:state].astype(F32), decays[0:1] + decays[1:2]

    def scan_pair():
        for e in range(2):
            scan_copy(0, e).wait_recv()
            states, total = scan_read(0, e)
            mine, my_total = carry_ref[e], total_ref[e][0:1]

            @pl.when(odd == 1 - e)
            def _():
                pair_ref[e] = states * jnp.exp(my_total) + mine

            @pl.when(odd == e)
            def _():
                pair_ref[e] = mine * jnp.exp(total) + states

            total_ref[e] = total_ref[e] + total

    def scan_slot(r):
        for e in range(2):

            @pl.when(pair == (r if e == 0 else pairs - 1 - r))
            def _():
                if r > 0:
                    scan_copy(1, e).wait_recv()
                    states, total = scan_read(1, e)
                    start_ref[e] = states
                    reach_ref[e] = jnp.broadcast_to(total, reach_ref.shape[1:])
                if r < pairs - 1:
                    total = total_ref[e][0:1]
                    scan_start(
                        1, e, start_ref[e] * jnp.exp(total) + pair_ref[e], reach_ref[e][0:1] + total
                    )

    def scan_finish():
        for e in range(2):

            @pl.when(odd == 1 - e)
            def _():
                states, total = scan_read(0, e)
                start_ref[e] = start_ref[e] * jnp.exp(total) + states

    def scan_left():
        for e in range(2):
            scan_copy(0, e).wait_send()
            goes = pair < pairs - 1 if e == 0 else pair > 0
            pl.when(goes)(lambda: scan_copy(1, e).wait_send())

    for e in range(2):
        scan_start(0, e, carry_ref[e], total_ref[e][0:1])

    until(GROUP * hops * -(-(first_units + second_units) // GROUP))

    scan_pair()
    scan_slot(0)
    q_last = second_units - 2 * kv_width // TILE

    def second_dot_b(b):
        rows = rows_at(b, dot_rows)
        got = jnp.dot(
            normed_ref[rows, :],
            weights(1, first_units, first_units + second_units),
            preferred_element_type=F32,
        ).astype(BF16)
        q_ref[rows, second_units * TILE :] = got[:, : q_last * TILE]
        kv_ref[rows_at(b, dot_rows, WINDOW), :] = got[:, q_last * TILE :]

    sweep(count // dot_rows, 1, second_dot_b)
    kv_edges = edge_copies(kv_ref, WINDOW, kv_send, kv_recv)
    edges_start(kv_edges)

    def second_dot_a(b):
        rows = rows_at(b, dot_rows)
        q_ref[rows, : second_units * TILE] = jnp.dot(
            normed_ref[rows, :],
            weights(0, first_units, first_units + second_units),
            preferred_element_type=F32,
        ).astype(BF16)

    sweep(count // dot_rows, 1, second_dot_a)

    quarter = HEAD_DIM // 4
    low = lax.rem(iota((size, TILE), 1), 2 * quarter) < quarter

    def turned(part, table):
        x = part.astype(F32)
        other = jnp.where(low, pltpu.roll(x, TILE - quarter, 1), pltpu.roll(x, quarter, 1))
        return (x * table[:, :TILE] + other * table[:, TILE:]).astype(BF16)

    def prepare(b):
        rows = rows_at(b, size)
        for c in range(kv_width // TILE):
            keys_ref[rows, c * TILE : (c + 1) * TILE] = turned(
                kv_ref[rows, c * TILE : (c + 1) * TILE], turn_ref[rows, :]
            )

    sweep(blocks, 0, lambda i: prepare(i + 1))

    band = size + 2 * WINDOW
    band_row = iota((size, band), 0)
    band_col = iota((size, band), 1)
    near = (band_col >= band_row) & (band_col - band_row <= 2 * WINDOW)
    q_lane = iota((size, TILE), 1)
    repeat = q_count * HEAD_DIM // kv_width
    seq_total = seats * count
    slots = {1: 0, 2: blocks // 2}

    def attend(i):
        for r in range(1, min(3, pairs)):
            pl.when(i == slots[r])(lambda: scan_slot(r))

        @pl.when(i == blocks - 2)
        def _():
            edges_arrive(kv_edges)
            prepare(0)
            prepare(blocks + 1)

        b = lax.rem(i + 1, blocks)
        start = pl.multiple_of(b * size, size)
        rows = pl.ds(start, size)
        reach = pl.ds(start, band)
        key_pos = place * count + start - WINDOW + band_col
        valid = near & (key_pos >= 0) & (key_pos < seq_total)
        logs = jnp.zeros((size, TILE), F32)
        table = turn_ref[pl.ds(start + WINDOW, size), :]
        turned_q = jnp.concatenate(
            [turned(q_ref[rows, c * TILE : (c + 1) * TILE], table) for c in range(q_width // TILE)],
            axis=1,
        )
        outs = []
        for h in range(q_count):
            g = h // repeat
            scores = inner_t(
                turned_q[:, h * HEAD_DIM : (h + 1) * HEAD_DIM],
                keys_ref[reach, g * HEAD_DIM : (g + 1) * HEAD_DIM],
            ) * HEAD_DIM ** (-0.5)
            scores = jnp.where(valid, scores, -jnp.inf)
            sink = sink_ref[h]
            top = jnp.maximum(jnp.max(scores, axis=1, keepdims=True), sink)
            expo = jnp.exp(scores - top)
            total = jnp.sum(expo, axis=1, keepdims=True) + jnp.exp(sink - top)
            begin = kv_width + g * HEAD_DIM
            values = jnp.dot(
                expo.astype(BF16),
                kv_ref[reach, begin : begin + HEAD_DIM],
                preferred_element_type=F32,
            )
            outs.append((values / total).astype(BF16))
            logs = jnp.where(q_lane == h, top + jnp.log(total), logs)
        feat_ref[rows, wide:] = jnp.concatenate(outs, axis=1)
        log_ref[:, rows] = logs.T[:q_count]

    sweep(blocks, 2, attend)

    gate_first = first_units + second_units
    until(GROUP * hops * -(-(gate_first + gate_units) // GROUP))

    def gate_dot(b):
        rows = rows_at(b, dot_rows)
        for d in range(2):
            gate_ref[rows, d * gate_units * TILE : (d + 1) * gate_units * TILE] = jnp.dot(
                normed_ref[rows, :],
                weights(d, gate_first, gate_first + gate_units),
                preferred_element_type=F32,
            ).astype(BF16)

    sweep(count // dot_rows, 1, gate_dot)
    for r in range(3, pairs):
        scan_slot(r)
    scan_finish()

    def mix(b):
        rows = rows_at(b, size)
        cum = cum_ref[rows, :]
        step = step_ref[rows, :]
        cum_t = cum.T
        step_t = step.T
        x = cells_ref[rows, :wide]
        writes = cells_ref[rows, wide : wide + state]
        reads = cells_ref[rows, wide + state :]
        cross = inner_t(reads, writes)
        parts = []
        for h in range(heads):
            f = slice(h, h + 1)
            g = slice(heads + h, heads + h + 1)
            seg = jnp.where(row >= col, cum[:, f] - cum_t[f], cum[:, g] - cum_t[g])
            scale = jnp.where(
                row > col, step_t[f], jnp.where(row < col, step_t[g], step_t[f] + step_t[g])
            )
            weight = (cross * jnp.exp(seg) * scale).astype(BF16)
            parts.append(
                jnp.dot(weight, x[:, h * HEAD_DIM : (h + 1) * HEAD_DIM], preferred_element_type=F32)
            )
        y = jnp.concatenate(parts, axis=1)
        fades = jnp.exp(cum)
        for e in range(2):
            held = entry_ref[e, b] + jnp.exp(before_ref[e, b][0:1]) * start_ref[e]
            y = y + through(fades, spreads[e], True) * jnp.dot(
                reads, held.astype(BF16), preferred_element_type=F32
            )
        gate = gate_ref[rows, :].astype(F32)
        y = y * (gate * jax.nn.sigmoid(gate))
        y = y * lax.rsqrt(jnp.mean(y * y, axis=1, keepdims=True) + EPS)
        feat_ref[rows, :wide] = (y * norm_gain_ref[...].astype(F32).reshape(1, wide)).astype(BF16)

    sweep(blocks, 1, mix)

    out_first = gate_first + gate_units
    out_units = per_dir - out_first
    per_peer = 2 * seats // peers

    dot_blocks = count // dot_rows

    core = lax.rem(lane_peer, 2)
    beside = lane_peer + 1 - 2 * core

    def near_copy(tile, b):
        rows = rows_at(b, dot_rows)
        return pltpu.make_async_remote_copy(
            src_ref=part_ref.at[tile, rows],
            dst_ref=near_ref.at[tile, rows],
            send_sem=near_send.at[tile, b],
            recv_sem=near_recv.at[tile, b],
            device_id={"tp": beside},
            device_id_type=mesh_id,
        )

    def far_copy(tile, b, dest, slot):
        rows = rows_at(b, dot_rows)
        at = lax.rem(tile, per_peer)
        return pltpu.make_async_remote_copy(
            src_ref=part_ref.at[tile, rows],
            dst_ref=far_ref.at[slot, at, rows],
            send_sem=far_send.at[tile, b],
            recv_sem=far_recv.at[slot, at, b],
            device_id={"tp": dest},
            device_id_type=mesh_id,
        )

    def dest_of(tile):
        dest = lax.div(tile, per_peer)
        return dest, lax.rem(dest, 2) == core, lax.div(dest, 2) == lax.div(lane_peer, 2)

    def project(d, owner):
        tile = 2 * owner + d
        _, kept, _ = dest_of(tile)
        matrix = ring_ref[d, out_first:, owner].reshape(out_units * unit_rows, TILE)

        def rows_dot(b, _):
            rows = rows_at(b, dot_rows)
            part_ref[tile, rows, :] = jnp.dot(
                feat_ref[rows, :], matrix, preferred_element_type=F32
            ).astype(BF16)
            pl.when(jnp.logical_not(kept))(lambda: near_copy(tile, b).start())
            return 0

        lax.fori_loop(0, dot_blocks, rows_dot, 0)

    def join(d, owner):
        tile = 2 * owner + d
        dest, kept, local = dest_of(tile)

        @pl.when(kept)
        def _():
            def rows_add(b, _):
                rows = rows_at(b, dot_rows)
                near_copy(tile, b).wait_recv()
                part_ref[tile, rows, :] = (
                    part_ref[tile, rows, :].astype(F32) + near_ref[tile, rows, :].astype(F32)
                ).astype(BF16)

                @pl.when(jnp.logical_not(local))
                def _():
                    far_copy(tile, b, dest, lax.div(lane_peer, 2)).start()

                return 0

            lax.fori_loop(0, dot_blocks, rows_add, 0)

    final = sends - GROUP * hops
    limit = sends - GROUP

    def project_own(_):
        for d in range(2):
            project(d, place)

    def ready():
        return min(hops - 1, max(0, (clock[0] - final) // GROUP))

    sweep(1, min(1, limit - clock[0]), project_own)

    def project_hop(k):
        project(0, seat_at(my_pos - k - 1))
        project(1, seat_at(my_pos + k + 1))
        join(0, seat_at(my_pos - k))
        join(1, seat_at(my_pos + k))

    done = 0
    while ready() > done:
        first, more = done, ready() - done
        sweep(more, 1 if clock[0] + more <= limit else 0, lambda i: project_hop(i + first))
        done = first + more
    if done < hops - 1 and clock[0] > final + GROUP * done:
        until(final + GROUP * (done + 1))
        project_hop(jnp.int32(done))
        done += 1
    until(final + GROUP * done)
    sweep(hops - 1 - done, GROUP, lambda i: project_hop(i + done))
    for j in range(GROUP):
        tick(jnp.int32(sends - GROUP + j), last=True)
    project_hop(jnp.int32(hops - 1))
    join(0, seat_at(my_pos - hops))
    join(1, seat_at(my_pos + hops))

    chips = peers // 2

    def add_up(b, _):
        rows = rows_at(b, dot_rows)
        for j in range(per_peer):
            total = part_ref[lane_peer * per_peer + j, rows, :].astype(F32)
            for r in range(1, chips):
                slot = lax.rem(lax.div(lane_peer, 2) + r, chips)
                far_copy(jnp.int32(j), b, 2 * slot + core, slot).wait_recv()
                total = total + far_ref[slot, j, rows, :].astype(F32)
            out_ref[rows, j * TILE : (j + 1) * TILE] = total.astype(BF16)
        return 0

    lax.fori_loop(0, dot_blocks, add_up, 0)

    edges_left(conv_edges)
    edges_left(kv_edges)
    scan_left()
    for r in range(1, seats):
        steps_copy(r).wait_send()

    def ring_left(i, _):
        for d in range(2):
            ring_copy(i, d, 0).wait_send()
        return 0

    lax.fori_loop(0, sends, ring_left, 0)

    def out_left(tile, _):
        dest, kept, local = dest_of(tile)

        @pl.when(jnp.logical_not(kept))
        def _():
            for b in range(dot_blocks):
                near_copy(tile, b).wait_send()

        @pl.when(kept & jnp.logical_not(local))
        def _():
            for b in range(dot_blocks):
                far_copy(tile, b, dest, lax.div(lane_peer, 2)).wait_send()

        return 0

    lax.fori_loop(0, 2 * seats, out_left, 0)


def turn_tables(rows_total):
    quarter = HEAD_DIM // 4
    freqs = np.float32(ROPE_BASE) ** (-np.arange(quarter).astype(np.float32) / np.float32(quarter))
    border = WINDOW // GRID_W
    row_angle = (np.arange(rows_total + 2 * border) - border).astype(np.float32)[:, None] * freqs
    col_angle = np.arange(GRID_W).astype(np.float32)[:, None] * freqs

    def table(angle, first):
        zero = np.zeros_like(angle)
        cosine = np.cos(angle)
        sine = np.sin(angle)
        one = [cosine, cosine, zero, zero] if first else [zero, zero, cosine, cosine]
        two = [-sine, sine, zero, zero] if first else [zero, zero, -sine, sine]
        copies = TILE // HEAD_DIM
        return np.concatenate(one * copies + two * copies, axis=1).astype(np.float32)

    return table(row_angle, True), table(col_angle, False)


def hand_on_kernel(mixed_ref, logs_ref, mixed_out_ref, logs_out_ref):
    mixed_out_ref[...] = mixed_ref[...]
    logs_out_ref[...] = logs_ref[...]


def streamed(
    tokens,
    input_gain,
    gate_weight,
    value_weight,
    inflow_weight,
    readout_weight,
    step_weight,
    conv_values,
    conv_inflow,
    conv_readout,
    log_rate,
    group_gain,
    query_weight,
    key_weight,
    vector_weight,
    sink_logit,
    state_out,
    window_out,
):
    count, width = tokens.shape
    seats = lax.axis_size("sp")
    peers = lax.axis_size("tp")
    heads = step_weight.shape[2]
    unit_rows = value_weight.shape[0]
    inflow = flatten_rows(inflow_weight)
    readout = flatten_rows(readout_weight)
    wide = value_weight.shape[1]
    state = inflow.shape[1]
    conv_width = wide + 2 * state
    q_width = query_weight.shape[1]
    kv_width = key_weight.shape[1]
    blocks = count // SSD_BLOCK
    steps = jnp.transpose(step_weight, (1, 2, 0)).reshape(2 * heads, unit_rows)
    row_turn, col_turn = turn_tables(seats * count // GRID_W)
    units = chunk_maps(
        {
            "value": value_weight.shape,
            "inflow": inflow.shape,
            "readout": readout.shape,
            "query": query_weight.shape,
            "key": key_weight.shape,
            "vector": vector_weight.shape,
            "gate": gate_weight.shape,
            "state_out": state_out.shape,
            "window_out": window_out.shape,
        }
    )
    per_dir = len(units[0])
    sends = per_dir * (seats - 1)
    vmem = pl.BlockSpec(memory_space=pltpu.VMEM)
    smem = pl.BlockSpec(memory_space=pltpu.SMEM)
    hbm = pl.BlockSpec(memory_space=pltpu.HBM)
    dma = pltpu.SemaphoreType.DMA
    scratch = [
        pltpu.VMEM((2, per_dir, seats, unit_rows, TILE), BF16),
        pltpu.VMEM((seats, 2 * heads, unit_rows), BF16),
        pltpu.VMEM((count, width), BF16),
        pltpu.VMEM((count, width), BF16),
        pltpu.VMEM((count + 2 * PAD, conv_width), BF16),
        pltpu.VMEM((count, conv_width), BF16),
        pltpu.VMEM((count, TILE), F32),
        pltpu.VMEM((count, TILE), F32),
        pltpu.VMEM((2, blocks, state, wide), F32),
        pltpu.VMEM((2, blocks, 8, wide), F32),
        pltpu.VMEM((2, state, wide), F32),
        pltpu.VMEM((2, 8, wide), F32),
        pltpu.VMEM((2, 2, state + PAD, wide), BF16),
        pltpu.VMEM((2, 2, state + PAD, wide), BF16),
        pltpu.VMEM((2, state, wide), F32),
        pltpu.VMEM((2, 8, wide), F32),
        pltpu.VMEM((2, state, wide), F32),
        pltpu.VMEM((count, wide), BF16),
        pltpu.VMEM((count, q_width), BF16),
        pltpu.VMEM((count + 2 * WINDOW, 2 * kv_width), BF16),
        pltpu.VMEM((count + 2 * WINDOW, kv_width), BF16),
        pltpu.VMEM((count + 2 * WINDOW, 2 * TILE), F32),
        pltpu.VMEM((count, wide + q_width), BF16),
        pltpu.VMEM((2 * seats, count, TILE), BF16),
        pltpu.VMEM((2 * seats, count, TILE), BF16),
        pltpu.VMEM((peers // 2, 2 * seats // peers, count, TILE), BF16),
        dma((2, sends)),
        dma((2, sends)),
        dma((seats,)),
        dma((seats,)),
        dma((2 * per_dir + 1,)),
        dma((2,)),
        dma((2,)),
        dma((2,)),
        dma((2,)),
        dma((2, 2)),
        dma((2, 2)),
        dma((2 * seats, count // (2 * SSD_BLOCK))),
        dma((2 * seats, count // (2 * SSD_BLOCK))),
        dma((2 * seats, count // (2 * SSD_BLOCK))),
        dma((peers // 2, 2 * seats // peers, count // (2 * SSD_BLOCK))),
    ]
    mixed, logs = pl.pallas_call(
        functools.partial(layer_kernel, (seats, peers, units)),
        out_shape=(
            jax.ShapeDtypeStruct((count, width // peers), BF16),
            jax.ShapeDtypeStruct((q_width // HEAD_DIM, count), F32),
        ),
        in_specs=[hbm] + [vmem] * 6 + [smem] + [vmem] * 3 + [hbm] * 9,
        out_specs=(vmem, vmem),
        scratch_shapes=scratch,
        compiler_params=pltpu.CompilerParams(
            collective_id=0, has_side_effects=True, vmem_limit_bytes=60 * 2**20
        ),
    )(
        tokens,
        input_gain,
        group_gain,
        conv_values,
        flatten_rows(conv_inflow),
        flatten_rows(conv_readout),
        jnp.transpose(log_rate, (0, 2, 1)),
        sink_logit,
        jnp.asarray(row_turn),
        jnp.asarray(col_turn),
        steps,
        value_weight,
        inflow,
        readout,
        query_weight,
        key_weight,
        vector_weight,
        gate_weight,
        state_out,
        window_out,
    )
    mixed, logs = call(
        hand_on_kernel,
        (
            jax.ShapeDtypeStruct(mixed.shape, mixed.dtype),
            jax.ShapeDtypeStruct(logs.shape, logs.dtype),
        ),
        (mixed, logs),
    )
    return mixed, logs.T


def streams(arrays):
    tokens, value, inflow, key, out = arrays[0], arrays[3], arrays[4], arrays[13], arrays[16]
    seats = lax.axis_size("sp")
    return (
        seats % 2 == 0
        and value.shape[0] % TILE == 0
        and out.shape[0] % value.shape[0] == 0
        and out.shape[1] == 2 * TILE
        and value.shape[1] == 4 * TILE
        and inflow.shape[1] * inflow.shape[2] == TILE
        and key.shape[1] == TILE
        and tokens.shape[0] % (2 * SSD_BLOCK) == 0
        and tokens.shape[0] >= 4 * SSD_BLOCK
        and tokens.shape[0] % GRID_W == 0
        and tokens.shape[1] == seats * value.shape[0]
        and seats == 2 * lax.axis_size("tp")
    )


def layer(*arrays):
    if streams(arrays):
        return streamed(*arrays)
    return shards(*arrays)


def shards(
    tokens,
    input_gain,
    gate_weight,
    value_weight,
    inflow_weight,
    readout_weight,
    step_weight,
    conv_values,
    conv_inflow,
    conv_readout,
    log_rate,
    group_gain,
    query_weight,
    key_weight,
    vector_weight,
    sink_logit,
    state_out,
    window_out,
):
    count = tokens.shape[0]
    offset = lax.axis_index("sp") * count
    seq_total = count * lax.axis_size("sp")
    heads = step_weight.shape[2]
    groups = inflow_weight.shape[1]
    state_len = inflow_weight.shape[2]
    inner_local = value_weight.shape[1]
    q_count = query_weight.shape[1] // HEAD_DIM
    kv_count = key_weight.shape[1] // HEAD_DIM
    kv_width = key_weight.shape[1]
    wide = tokens.astype(F32)
    normed = (
        wide
        * lax.rsqrt(jnp.mean(wide * wide, axis=1, keepdims=True) + EPS)
        * input_gain.astype(F32)
    ).astype(BF16)

    def whole(parts):
        return lax.all_gather(jnp.concatenate(parts, axis=1), "sp", axis=0, tiled=True)

    own = (flatten_rows(inflow_weight), flatten_rows(readout_weight), flatten_rows(step_weight))
    first_matrix = whole((value_weight,) + own)
    rest_matrix = whole((key_weight, vector_weight, gate_weight, query_weight))
    first = jnp.dot(normed, first_matrix, preferred_element_type=F32)
    rest = jnp.dot(normed, rest_matrix, preferred_element_type=F32).astype(BF16)
    conv_width = inner_local + 2 * groups * state_len
    conv_input = first[:, :conv_width].astype(BF16)
    step = jax.nn.softplus(first[:, conv_width:])
    keyvals = rest[:, : 2 * kv_width]
    gate = rest[:, 2 * kv_width : 2 * kv_width + inner_local]
    queries = rest[:, 2 * kv_width + inner_local :]

    reach_rows = CONV // 2
    padded = with_halo(conv_input, (("sp", 0),), CONV // 2).astype(F32)
    taps = jnp.concatenate(
        [conv_values, flatten_rows(conv_inflow), flatten_rows(conv_readout)], axis=1
    ).astype(F32)
    conv_sum = padded[0:count] * taps[0]
    for tap in range(1, 2 * reach_rows + 1):
        conv_sum = conv_sum + padded[tap : tap + count] * taps[tap]
    cells = jax.nn.silu(conv_sum).astype(BF16)
    rates = jnp.transpose(log_rate, (1, 0, 2)).reshape(count, 2 * heads)
    sd = jnp.concatenate([step, -jnp.exp(rates) * step], axis=1)
    blocks = count // SSD_BLOCK
    sdt = jnp.transpose(sd.reshape(blocks, SSD_BLOCK, 4 * heads), (0, 2, 1))

    summary = call(
        summary_kernel,
        jax.ShapeDtypeStruct((2, state_len + PAD, inner_local), BF16),
        (cells, sd),
    )
    everyone = lax.all_gather(summary, "sp")
    out_stack, everyone = lax.optimization_barrier(
        (jnp.concatenate([state_out, window_out], axis=0), everyone)
    )
    out_matrix = lax.all_gather(out_stack, "sp", axis=1, tiled=True)
    seats = lax.axis_size("sp")
    place = lax.axis_index("sp")
    totals = everyone[:, :, state_len].astype(F32) + everyone[:, :, state_len + 1].astype(F32)
    seat = jnp.arange(seats)
    starts = []
    for e in range(2):
        ahead = seat < place if e == 0 else seat > place
        between = (seat[None, :] > seat[:, None]) if e == 0 else (seat[None, :] < seat[:, None])
        between = (between & ahead[None, :])[:, :, None]
        fade = jnp.sum(jnp.where(between, totals[None, :, e], 0.0), axis=1)
        fade = jnp.where(ahead[:, None], jnp.exp(fade), 0.0)
        starts.append(jnp.sum(fade[:, None, :] * everyone[:, e, :state_len].astype(F32), axis=0))
    starts = jnp.stack(starts)
    state_features = call(
        mixer_kernel,
        jax.ShapeDtypeStruct((count, inner_local), BF16),
        (cells, sd, sdt, starts, gate, group_gain[None]),
        (
            pltpu.VMEM((blocks, state_len, inner_local), BF16),
            pltpu.VMEM((state_len, inner_local), F32),
        ),
        flops=10**10,
    )

    beside = with_halo(keyvals, (("sp", 0),), WINDOW)
    quarter = HEAD_DIM // 4
    freqs = ROPE_BASE ** (-jnp.arange(quarter).astype(F32) / quarter)
    spots = offset - WINDOW + jnp.arange(count + 2 * WINDOW, dtype=jnp.int32)
    row_angle = (spots // GRID_W).astype(F32)[:, None] * freqs
    col_angle = (spots % GRID_W).astype(F32)[:, None] * freqs
    angles = jnp.concatenate([row_angle, col_angle], axis=1)
    cosine = jnp.cos(angles)
    sine = jnp.sin(angles)

    def doubled(table, sign):
        low = table[:, :quarter]
        high = table[:, quarter:]
        return [sign * low, low, sign * high, high]

    turn = jnp.concatenate(doubled(cosine, 1.0) + doubled(sine, -1.0), axis=1)
    channel = jnp.arange(HEAD_DIM)
    partner = channel + jnp.where(channel % (2 * quarter) < quarter, quarter, -quarter)
    swap = (channel[:, None] == partner[None, :]).astype(BF16)
    limits = jnp.stack([offset, seq_total]).astype(jnp.int32)
    window_features, log_total = call(
        attend_kernel,
        (
            jax.ShapeDtypeStruct((count, q_count * HEAD_DIM), BF16),
            jax.ShapeDtypeStruct((count, q_count), F32),
        ),
        (limits, sink_logit, queries, beside, turn, swap),
        (pltpu.VMEM((kv_count, count + 2 * WINDOW, HEAD_DIM), BF16),),
        scalars=2,
        flops=10**10,
    )
    features = jnp.concatenate([state_features, window_features], axis=1)
    terms = jnp.dot(features, out_matrix, preferred_element_type=F32)
    mixed = lax.psum_scatter(terms.astype(BF16), "tp", scatter_dimension=1, tiled=True)
    return (mixed, log_total)


def solution(mesh):
    placed = (
        P("sp", None),
        P(),
        P("sp", "tp"),
        P("sp", "tp"),
        P("sp", "tp", None),
        P("sp", "tp", None),
        P("sp", None, "tp"),
        P(None, "tp"),
        P(None, "tp", None),
        P(None, "tp", None),
        P(None, "sp", "tp"),
        P("tp"),
        P("sp", "tp"),
        P("sp", "tp"),
        P("sp", "tp"),
        P("tp"),
        P("tp", "sp"),
        P("tp", "sp"),
    )
    return jax.shard_map(
        layer,
        mesh=mesh,
        in_specs=placed,
        out_specs=(P("sp", "tp"), P("sp", "tp")),
        check_vma=False,
    )
```

```python
import functools

import jax
import jax.numpy as jnp
import numpy as np
from jax import lax
from jax.experimental import pallas as pl
from jax.experimental.pallas import tpu as pltpu
from jax.sharding import PartitionSpec as P


HEAD_DIM = 64
CONV = 5
SSD_BLOCK = 128
WINDOW = 128
GRID_W = 64


EPS = 1e-06
ROPE_BASE = 10000.0
HIGHEST = lax.Precision.HIGHEST
F32 = jnp.float32
BF16 = jnp.bfloat16
PAD = 16


def iota(shape, dim):
    return lax.broadcasted_iota(jnp.int32, shape, dim)


def exact(a, b):
    return jnp.dot(a, b, precision=HIGHEST, preferred_element_type=F32)


def spread(heads):
    shape = (heads, heads * HEAD_DIM)
    return (iota(shape, 1) // HEAD_DIM == iota(shape, 0)).astype(F32)


def inner_t(a, b):
    return lax.dot_general(a, b, (((1,), (1,)), ((), ())), preferred_element_type=F32)


def outer_t(a, b):
    return lax.dot_general(a, b, (((0,), (0,)), ((), ())), preferred_element_type=F32)


def summary_kernel(cells_ref, sd_ref, out_ref):
    count = cells_ref.shape[0]
    heads = sd_ref.shape[1] // 4
    wide = heads * HEAD_DIM
    state = out_ref.shape[1] - PAD
    x = cells_ref[:, :wide].astype(F32)
    writes = cells_ref[:, wide : wide + state]
    expand = spread(heads)
    row = iota((count, count), 0)
    col = iota((count, count), 1)
    for e in range(2):
        step = sd_ref[:, e * heads : (e + 1) * heads]
        decay = sd_ref[:, (2 + e) * heads : (3 + e) * heads]
        span = (col > row) if e == 0 else (col < row)
        rest = exact(span.astype(F32), decay)
        scaled = (x * exact(jnp.exp(rest) * step, expand)).astype(BF16)
        out_ref[e, :state, :] = outer_t(writes, scaled).astype(BF16)
        total = exact(jnp.broadcast_to(jnp.sum(decay, axis=0, keepdims=True), (8, heads)), expand)
        total = total[0:1]
        high = total.astype(BF16).astype(F32)
        place = iota((PAD, wide), 0)
        packed = jnp.where(place == 0, high, jnp.where(place == 1, total - high, 0.0))
        out_ref[e, state:, :] = packed.astype(BF16)


def mixer_kernel(cells_ref, sd_ref, sdt_ref, start_ref, gate_ref, gain_ref, out_ref, back_ref, carry_ref):
    blocks, _, size = sdt_ref.shape
    heads = sd_ref.shape[1] // 4
    wide = heads * HEAD_DIM
    state = start_ref.shape[1]
    expand = spread(heads)
    row = iota((size, size), 0)
    col = iota((size, size), 1)
    lower = (row >= col).astype(F32)
    upper = (row <= col).astype(F32)

    carry_ref[...] = start_ref[1]

    def backward(index, _):
        block = blocks - 1 - index
        rows = pl.ds(pl.multiple_of(block * size, size), size)
        back_ref[block] = carry_ref[...].astype(BF16)
        step = sd_ref[rows, heads : 2 * heads]
        cum = exact(upper, sd_ref[rows, 3 * heads : 4 * heads])
        edge = cum[0:1]
        x = cells_ref[rows, :wide].astype(F32)
        scaled = (x * exact(jnp.exp(edge - cum) * step, expand)).astype(BF16)
        fresh = outer_t(cells_ref[rows, wide : wide + state], scaled)
        fade = exact(jnp.broadcast_to(jnp.exp(edge), (8, heads)), expand)[0:1]
        carry_ref[...] = fade * carry_ref[...] + fresh
        return 0

    lax.fori_loop(0, blocks, backward, 0)
    carry_ref[...] = start_ref[0]

    def forward(block, _):
        rows = pl.ds(pl.multiple_of(block * size, size), size)
        cum_f = exact(lower, sd_ref[rows, 2 * heads : 3 * heads])
        cum_b = exact(upper, sd_ref[rows, 3 * heads : 4 * heads])
        flat = sdt_ref[block]
        step_ft = flat[:heads]
        step_bt = flat[heads : 2 * heads]
        cum_ft = exact(flat[2 * heads : 3 * heads], upper)
        cum_bt = exact(flat[3 * heads :], lower)
        x = cells_ref[rows, :wide]
        writes = cells_ref[rows, wide : wide + state]
        reads = cells_ref[rows, wide + state :]
        cross = inner_t(reads, writes)
        parts = []
        for h in range(heads):
            one = slice(h, h + 1)
            seg = jnp.where(
                row >= col, cum_f[:, one] - cum_ft[one], cum_b[:, one] - cum_bt[one]
            )
            scale = jnp.where(
                row > col,
                step_ft[one],
                jnp.where(row < col, step_bt[one], step_ft[one] + step_bt[one]),
            )
            weight = (cross * jnp.exp(seg) * scale).astype(BF16)
            parts.append(
                jnp.dot(
                    weight, x[:, h * HEAD_DIM : (h + 1) * HEAD_DIM], preferred_element_type=F32
                )
            )
        y = jnp.concatenate(parts, axis=1)
        y = y + exact(jnp.exp(cum_f), expand) * jnp.dot(
            reads, carry_ref[...].astype(BF16), preferred_element_type=F32
        )
        y = y + exact(jnp.exp(cum_b), expand) * jnp.dot(
            reads, back_ref[block], preferred_element_type=F32
        )
        gate = gate_ref[rows, :].astype(F32)
        y = y * (gate * jax.nn.sigmoid(gate))
        y = y * lax.rsqrt(jnp.mean(y * y, axis=1, keepdims=True) + EPS)
        out_ref[rows, :] = (y * gain_ref[...].astype(F32)).astype(BF16)
        edge = cum_f[size - 1 : size]
        step = sd_ref[rows, :heads]
        scaled = (x.astype(F32) * exact(jnp.exp(edge - cum_f) * step, expand)).astype(BF16)
        fade = exact(jnp.broadcast_to(jnp.exp(edge), (8, heads)), expand)[0:1]
        carry_ref[...] = fade * carry_ref[...] + outer_t(writes, scaled)
        return 0

    lax.fori_loop(0, blocks, forward, 0)


def attend_kernel(place_ref, sink_ref, q_ref, kv_ref, turn_ref, swap_ref, out_ref, log_ref, keys_ref):
    count = q_ref.shape[0]
    q_count = q_ref.shape[1] // HEAD_DIM
    kv_width = kv_ref.shape[1] // 2
    repeat = q_count * HEAD_DIM // kv_width
    size = SSD_BLOCK
    band = size + 2 * WINDOW
    swap = swap_ref[...]

    def turned(part, rows):
        swapped = jnp.dot(part, swap, preferred_element_type=F32)
        table = turn_ref[rows, :]
        return (part.astype(F32) * table[:, :HEAD_DIM] + swapped * table[:, HEAD_DIM:]).astype(BF16)

    def prepare(block, _):
        rows = pl.ds(pl.multiple_of(block * size, size), size)
        for g in range(kv_width // HEAD_DIM):
            keys_ref[g, rows, :] = turned(
                kv_ref[rows, g * HEAD_DIM : (g + 1) * HEAD_DIM], rows
            )
        return 0

    lax.fori_loop(0, kv_ref.shape[0] // size, prepare, 0)
    row = iota((size, band), 0)
    col = iota((size, band), 1)
    near = (col >= row) & (col - row <= 2 * WINDOW)
    lane = iota((size, q_count), 1)

    def one(block, _):
        start = pl.multiple_of(block * size, size)
        rows = pl.ds(start, size)
        reach = pl.ds(start, band)
        key_pos = place_ref[0] + start - WINDOW + col
        valid = near & (key_pos >= 0) & (key_pos < place_ref[1])
        logs = jnp.zeros((size, q_count), F32)
        outs = []
        for h in range(q_count):
            g = h // repeat
            query = turned(
                q_ref[rows, h * HEAD_DIM : (h + 1) * HEAD_DIM], pl.ds(start + WINDOW, size)
            )
            scores = inner_t(query, keys_ref[g, reach, :]) * HEAD_DIM ** (-0.5)
            scores = jnp.where(valid, scores, -jnp.inf)
            sink = sink_ref[h]
            top = jnp.maximum(jnp.max(scores, axis=1, keepdims=True), sink)
            expo = jnp.exp(scores - top)
            total = jnp.sum(expo, axis=1, keepdims=True) + jnp.exp(sink - top)
            first = kv_width + g * HEAD_DIM
            values = jnp.dot(
                expo.astype(BF16),
                kv_ref[reach, first : first + HEAD_DIM],
                preferred_element_type=F32,
            )
            outs.append((values / total).astype(BF16))
            logs = jnp.where(lane == h, top + jnp.log(total), logs)
        out_ref[rows, :] = jnp.concatenate(outs, axis=1)
        log_ref[rows, :] = logs
        return 0

    lax.fori_loop(0, count // size, one, 0)


def call(kernel, out_shape, args, scratch=(), scalars=0, flops=10**8):
    vmem = pl.BlockSpec(memory_space=pltpu.VMEM)
    smem = pl.BlockSpec(memory_space=pltpu.SMEM)
    return pl.pallas_call(
        kernel,
        out_shape=out_shape,
        in_specs=[smem] * scalars + [vmem] * (len(args) - scalars),
        out_specs=jax.tree.map(lambda _: vmem, out_shape),
        scratch_shapes=list(scratch),
        cost_estimate=pl.CostEstimate(flops=flops, bytes_accessed=4 * 10**6, transcendentals=0),
        compiler_params=pltpu.CompilerParams(vmem_limit_bytes=40 * 2**20),
    )(*args)


def with_halo(cells, sides, width):
    for axis, dim in sides:
        count = lax.axis_size(axis)
        ends = count - 1
        head = lax.slice_in_dim(cells, 0, width, axis=dim)
        tail = lax.slice_in_dim(cells, cells.shape[dim] - width, cells.shape[dim], axis=dim)
        cells = jnp.concatenate(
            [
                lax.ppermute(tail, axis, [(i, (i + 1) % count) for i in range(ends)]),
                cells,
                lax.ppermute(head, axis, [((i + 1) % count, i) for i in range(ends)]),
            ],
            axis=dim,
        )
    return cells


def flatten_rows(weight):
    return weight.reshape(weight.shape[0], -1)


TILE = 128
GROUP = 3


def split3(v):
    high = v.astype(BF16)
    rest = v - high.astype(F32)
    mid = rest.astype(BF16)
    return high, mid, (rest - mid.astype(F32)).astype(BF16)


def through(left, right, left_wide):
    total = None
    for part in split3(left if left_wide else right):
        one = jnp.dot(part, right, preferred_element_type=F32) if left_wide else jnp.dot(
            left, part, preferred_element_type=F32
        )
        total = one if total is None else total + one
    return total


def chunk_maps(shapes):
    rows = shapes["value"][0]

    def tiles(name):
        return [(name, 0, c) for c in range(shapes[name][1] // TILE)]

    units = ([], [])
    for names in (("value", "inflow", "readout"), ("query", "key", "vector"), ("gate",)):
        flat = [t for name in names for t in tiles(name)]
        half = len(flat) // 2
        for d in range(2):
            units[d].extend(flat[d * half : (d + 1) * half])
    for d in range(2):
        for name in ("state_out", "window_out"):
            units[d].extend((name, r, d) for r in range(shapes[name][0] // rows))
    return units


def layer_kernel(
    cfg,
    tokens_hbm,
    gain_ref,
    norm_gain_ref,
    value_taps_ref,
    inflow_taps_ref,
    readout_taps_ref,
    rates_ref,
    sink_ref,
    row_turn_ref,
    col_turn_ref,
    steps_ref,
    value_ref,
    inflow_ref,
    readout_ref,
    query_ref,
    key_ref,
    vector_ref,
    gate_w_ref,
    state_out_ref,
    window_out_ref,
    out_ref,
    log_ref,
    ring_ref,
    steps_all_ref,
    tokens_ref,
    normed_ref,
    conv_ref,
    cells_ref,
    step_ref,
    cum_ref,
    entry_ref,
    before_ref,
    carry_ref,
    total_ref,
    scan_send_ref,
    scan_recv_ref,
    start_ref,
    reach_ref,
    pair_ref,
    gate_ref,
    q_ref,
    kv_ref,
    keys_ref,
    turn_ref,
    feat_ref,
    part_ref,
    near_ref,
    far_ref,
    send_sem,
    recv_sem,
    steps_send,
    steps_recv,
    local_sem,
    halo_send,
    halo_recv,
    kv_send,
    kv_recv,
    scan_ssem,
    scan_rsem,
    near_send,
    near_recv,
    far_send,
    far_recv,
):
    seats, peers, units = cfg
    count, width = tokens_hbm.shape
    unit_rows = ring_ref.shape[3]
    heads = steps_ref.shape[0] // 2
    wide = heads * HEAD_DIM
    state = inflow_ref.shape[1]
    conv_width = wide + 2 * state
    q_width = query_ref.shape[1]
    q_count = q_width // HEAD_DIM
    kv_width = key_ref.shape[1]
    per_dir = len(units[0])
    hops = seats - 1
    sends = per_dir * hops
    place = lax.axis_index("sp")
    lane_peer = lax.axis_index("tp")
    half = seats // 2
    blocks = count // SSD_BLOCK
    size = SSD_BLOCK
    mesh_id = pl.DeviceIdType.MESH

    def seat_at(pos):
        pos = lax.rem(pos + 2 * seats, seats)
        late = lax.div(pos, half)
        return (1 - late) * 2 * pos + late * (2 * (seats - 1 - pos) + 1)

    odd = lax.rem(place, 2)
    my_pos = (1 - odd) * lax.div(place, 2) + odd * (seats - 1 - lax.div(place, 2))
    nexts = (seat_at(my_pos + 1), seat_at(my_pos - 1))

    barrier = pltpu.get_barrier_semaphore()
    for r in range(1, seats):
        pl.semaphore_signal(
            barrier, inc=1, device_id={"sp": lax.rem(place + r, seats)}, device_id_type=mesh_id
        )
    for r in range(1, peers):
        pl.semaphore_signal(
            barrier, inc=1, device_id={"tp": lax.rem(lane_peer + r, peers)}, device_id_type=mesh_id
        )

    sources = {
        "value": value_ref,
        "inflow": inflow_ref,
        "readout": readout_ref,
        "query": query_ref,
        "key": key_ref,
        "vector": vector_ref,
        "gate": gate_w_ref,
        "state_out": state_out_ref,
        "window_out": window_out_ref,
    }
    locals_ = []
    for d in range(2):
        for u, (name, r, c) in enumerate(units[d]):
            locals_.append(
                pltpu.make_async_copy(
                    sources[name].at[pl.ds(r * unit_rows, unit_rows), pl.ds(c * TILE, TILE)],
                    ring_ref.at[d, u, place],
                    local_sem.at[d * per_dir + u],
                )
            )
    for copy in locals_:
        copy.start()
    tokens_in = pltpu.make_async_copy(tokens_hbm, tokens_ref, local_sem.at[2 * per_dir])
    tokens_in.start()
    steps_all_ref[place] = steps_ref[...]
    first_ones = [d * per_dir + u for d in range(2) for u in range(GROUP)]
    for at in first_ones:
        locals_[at].wait()
    pl.semaphore_wait(barrier, hops + peers - 1)

    def ring_copy(i, d, behind):
        turn = lax.div(i, GROUP * hops)
        k = lax.rem(lax.div(i, GROUP), hops) + behind
        unit = GROUP * turn + lax.rem(i, GROUP)
        owner = seat_at(my_pos - k) if d == 0 else seat_at(my_pos + k)
        block = ring_ref.at[d, unit, owner]
        return pltpu.make_async_remote_copy(
            src_ref=block,
            dst_ref=block,
            send_sem=send_sem.at[d, i],
            recv_sem=recv_sem.at[d, i],
            device_id={"sp": nexts[d]},
            device_id_type=mesh_id,
        )

    def tick(i, last=False):
        for d in range(2):
            ring_copy(i, d, 1).wait_recv()
            if not last:
                ring_copy(i + GROUP, d, 0).start()

    for j in range(GROUP):
        for d in range(2):
            ring_copy(jnp.int32(j), d, 0).start()

    for at, copy in enumerate(locals_):
        if at not in first_ones:
            copy.wait()

    def steps_copy(r):
        return pltpu.make_async_remote_copy(
            src_ref=steps_ref,
            dst_ref=steps_all_ref.at[place],
            send_sem=steps_send.at[r],
            recv_sem=steps_recv.at[place],
            device_id={"sp": lax.rem(place + r, seats)},
            device_id_type=mesh_id,
        )

    for r in range(1, seats):
        steps_copy(r).start()

    clock = [0]

    def sweep(trips, per_trip, body):
        base = clock[0]

        def run(i, _):
            for j in range(int(per_trip)):
                tick(base + i * int(per_trip) + j)
            if per_trip == 0.5:
                pl.when(lax.rem(i, 2) == 0)(lambda: tick(base + lax.div(i, 2)))
            body(i)
            return 0

        lax.fori_loop(0, trips, run, 0)
        clock[0] = base + (trips + 1) // 2 if per_trip == 0.5 else base + trips * per_trip

    def until(goal):
        if goal > clock[0]:
            sweep(goal - clock[0], 1, lambda i: None)

    def rows_at(index, length, first=0):
        return pl.ds(pl.multiple_of(index * length, length) + first, length)

    def normalise(b):
        rows = rows_at(b, size)
        x = tokens_ref[rows, :].astype(F32)
        scale = lax.rsqrt(jnp.mean(x * x, axis=1, keepdims=True) + EPS)
        normed_ref[rows, :] = (x * scale * gain_ref[...].astype(F32).reshape(1, width)).astype(BF16)

    tokens_in.wait()
    sweep(blocks, 1, normalise)
    table_row = place * (count // GRID_W)

    def fill_turn(i):
        turn_ref[rows_at(i, GRID_W), :] = col_turn_ref[...] + row_turn_ref[pl.ds(table_row + i, 1), :]

    sweep(turn_ref.shape[0] // GRID_W, 0, fill_turn)
    step_ref[...] = jnp.zeros_like(step_ref)
    carry_ref[...] = jnp.zeros_like(carry_ref)
    total_ref[...] = jnp.zeros_like(total_ref)
    start_ref[...] = jnp.zeros_like(start_ref)
    reach_ref[...] = jnp.zeros_like(reach_ref)

    first_edge = place == 0
    last_edge = place == seats - 1

    @pl.when(first_edge)
    def _():
        conv_ref[:PAD, :] = jnp.zeros((PAD, conv_width), BF16)
        kv_ref[:WINDOW, :] = jnp.zeros((WINDOW, 2 * kv_width), BF16)

    @pl.when(last_edge)
    def _():
        conv_ref[PAD + count :, :] = jnp.zeros((PAD, conv_width), BF16)
        kv_ref[WINDOW + count :, :] = jnp.zeros((WINDOW, 2 * kv_width), BF16)

    def weights(d, first, last):
        return jnp.concatenate(
            [ring_ref[d, u].reshape(seats * unit_rows, TILE) for u in range(first, last)], axis=1
        )

    first_units = conv_width // (2 * TILE)
    second_units = (q_width + 2 * kv_width) // (2 * TILE)
    gate_units = wide // (2 * TILE)
    until(GROUP * hops * -(-first_units // GROUP))
    for r in range(1, seats):
        peer = lax.rem(place + r, seats)
        pltpu.make_async_remote_copy(
            src_ref=steps_ref,
            dst_ref=steps_all_ref.at[peer],
            send_sem=steps_send.at[r],
            recv_sem=steps_recv.at[peer],
            device_id={"sp": peer},
            device_id_type=mesh_id,
        ).wait_recv()

    dot_rows = 2 * size

    def first_dot(b):
        rows = rows_at(b, dot_rows)
        here = normed_ref[rows, :]
        for d in range(2):
            conv_ref[rows_at(b, dot_rows, PAD), d * first_units * TILE : (d + 1) * first_units * TILE] = (
                jnp.dot(here, weights(d, 0, first_units), preferred_element_type=F32).astype(BF16)
            )
        steps = jnp.concatenate([steps_all_ref[o] for o in range(seats)], axis=1)
        raw = inner_t(here, steps)
        step = jnp.maximum(raw, 0.0) + jnp.log1p(jnp.exp(-jnp.abs(raw)))
        step_ref[rows, : 2 * heads] = step

    sweep(count // dot_rows, 1, first_dot)

    def edge_copies(ref, length, ssem, rsem):
        inner = ref.shape[0] - 2 * length
        up = pltpu.make_async_remote_copy(
            src_ref=ref.at[pl.ds(inner, length)],
            dst_ref=ref.at[pl.ds(0, length)],
            send_sem=ssem.at[0],
            recv_sem=rsem.at[0],
            device_id={"sp": lax.rem(place + 1, seats)},
            device_id_type=mesh_id,
        )
        down = pltpu.make_async_remote_copy(
            src_ref=ref.at[pl.ds(length, length)],
            dst_ref=ref.at[pl.ds(length + inner, length)],
            send_sem=ssem.at[1],
            recv_sem=rsem.at[1],
            device_id={"sp": lax.rem(place + hops, seats)},
            device_id_type=mesh_id,
        )
        return up, down

    def edges_start(pair):
        pl.when(jnp.logical_not(last_edge))(lambda: pair[0].start())
        pl.when(jnp.logical_not(first_edge))(lambda: pair[1].start())

    def edges_arrive(pair):
        pl.when(jnp.logical_not(first_edge))(lambda: pair[0].wait_recv())
        pl.when(jnp.logical_not(last_edge))(lambda: pair[1].wait_recv())

    def edges_left(pair):
        pl.when(jnp.logical_not(last_edge))(lambda: pair[0].wait_send())
        pl.when(jnp.logical_not(first_edge))(lambda: pair[1].wait_send())

    conv_edges = edge_copies(conv_ref, PAD, halo_send, halo_recv)
    edges_start(conv_edges)
    taps = jnp.concatenate(
        [ref[...] for ref in (value_taps_ref, inflow_taps_ref, readout_taps_ref)], axis=1
    ).astype(F32)
    lane = iota((size, TILE), 1)
    row = iota((size, size), 0)
    col = iota((size, size), 1)
    lower = (row >= col).astype(BF16)
    upper = (row <= col).astype(BF16)
    spread_row = iota((TILE, wide), 0)
    spread_col = iota((TILE, wide), 1) // HEAD_DIM
    spreads = [(spread_row - e * heads == spread_col).astype(BF16) for e in range(2)]

    def sums(b):
        rows = rows_at(b, size)
        filler = jnp.zeros((TILE - 2 * heads, size), F32)
        rates = jnp.concatenate([rates_ref[0, :, rows], rates_ref[1, :, rows], filler], axis=0).T
        decay = -jnp.exp(rates) * step_ref[rows, :]
        cum_ref[rows, :] = jnp.where(
            lane < heads, through(lower, decay, False), through(upper, decay, False)
        )

    sweep(blocks, 1, sums)
    edges_arrive(conv_edges)

    def convolve(b):
        rows = rows_at(b, size)
        padded = conv_ref[pl.ds(pl.multiple_of(b * size, size), size + 2 * PAD), :].astype(F32)
        first = PAD - CONV // 2
        total = padded[first : first + size] * taps[0:1]
        for tap in range(1, CONV):
            total = total + padded[first + tap : first + tap + size] * taps[tap : tap + 1]
        cells_ref[rows, :] = (total * jax.nn.sigmoid(total)).astype(BF16)

    sweep(blocks, 0.5, convolve)

    def summarise(i):
        for e in range(2):
            b = i if e == 0 else blocks - 1 - i
            rows = rows_at(b, size)
            cum = cum_ref[rows, :]
            edge = cum[size - 1 : size] if e == 0 else cum[0:1]
            scale = through(jnp.exp(edge - cum) * step_ref[rows, :], spreads[e], True)
            scaled = (cells_ref[rows, :wide].astype(F32) * scale).astype(BF16)
            fresh = outer_t(cells_ref[rows, wide : wide + state], scaled)
            edges = through(jnp.broadcast_to(edge, (8, TILE)), spreads[e], True)
            entry_ref[e, b] = carry_ref[e]
            before_ref[e, b] = total_ref[e]
            carry_ref[e] = jnp.exp(edges[0:1]) * carry_ref[e] + fresh
            total_ref[e] = total_ref[e] + edges

    sweep(blocks, 0.5, summarise)

    pair = lax.div(place, 2)
    pairs = seats // 2

    def scan_copy(stage, e):
        far = place + 1 - 2 * odd if stage == 0 else lax.rem(place + (2 if e == 0 else seats - 2), seats)
        return pltpu.make_async_remote_copy(
            src_ref=scan_send_ref.at[e, stage],
            dst_ref=scan_recv_ref.at[e, stage],
            send_sem=scan_ssem.at[e, stage],
            recv_sem=scan_rsem.at[e, stage],
            device_id={"sp": far},
            device_id_type=mesh_id,
        )

    def scan_start(stage, e, states, total):
        scan_send_ref[e, stage, :state] = states.astype(BF16)
        high = total.astype(BF16).astype(F32)
        at = iota((PAD, wide), 0)
        scan_send_ref[e, stage, state:] = jnp.where(
            at == 0, high, jnp.where(at == 1, total - high, 0.0)
        ).astype(BF16)
        scan_copy(stage, e).start()

    def scan_read(stage, e):
        far = scan_recv_ref[e, stage]
        decays = far[state : state + 8].astype(F32)
        return far[:state].astype(F32), decays[0:1] + decays[1:2]

    def scan_pair():
        for e in range(2):

            @pl.when(jnp.logical_not(spared(e, e)))
            def _():
                scan_copy(0, e).wait_recv()
                states, total = scan_read(0, e)
                mine, my_total = carry_ref[e], total_ref[e][0:1]

                @pl.when(odd == 1 - e)
                def _():
                    pair_ref[e] = states * jnp.exp(my_total) + mine

                @pl.when(odd == e)
                def _():
                    pair_ref[e] = mine * jnp.exp(total) + states

                total_ref[e] = total_ref[e] + total

    def scan_slot(r):
        for e in range(2):

            @pl.when(pair == (r if e == 0 else pairs - 1 - r))
            def _():
                if r > 0:
                    scan_copy(1, e).wait_recv()
                    states, total = scan_read(1, e)
                    start_ref[e] = states
                    reach_ref[e] = jnp.broadcast_to(total, reach_ref.shape[1:])
                if r < pairs - 1:
                    total = total_ref[e][0:1]
                    scan_start(
                        1, e, start_ref[e] * jnp.exp(total) + pair_ref[e], reach_ref[e][0:1] + total
                    )

    def scan_finish():
        for e in range(2):

            @pl.when(odd == 1 - e)
            def _():
                states, total = scan_read(0, e)
                start_ref[e] = start_ref[e] * jnp.exp(total) + states

    def scan_left():
        for e in range(2):
            pl.when(jnp.logical_not(spared(e, 1 - e)))(lambda: scan_copy(0, e).wait_send())
            goes = pair < pairs - 1 if e == 0 else pair > 0
            pl.when(goes)(lambda: scan_copy(1, e).wait_send())

    def spared(e, side):
        return (pair == (pairs - 1 if e == 0 else 0)) & (odd == side)

    for e in range(2):
        pl.when(jnp.logical_not(spared(e, 1 - e)))(
            lambda: scan_start(0, e, carry_ref[e], total_ref[e][0:1])
        )

    until(GROUP * hops * -(-(first_units + second_units) // GROUP))

    scan_pair()
    scan_slot(0)
    q_last = second_units - 2 * kv_width // TILE

    def second_dot_b(b):
        rows = rows_at(b, dot_rows)
        got = jnp.dot(
            normed_ref[rows, :],
            weights(1, first_units, first_units + second_units),
            preferred_element_type=F32,
        ).astype(BF16)
        q_ref[rows, second_units * TILE :] = got[:, : q_last * TILE]
        kv_ref[rows_at(b, dot_rows, WINDOW), :] = got[:, q_last * TILE :]

    sweep(count // dot_rows, 1, second_dot_b)
    kv_edges = edge_copies(kv_ref, WINDOW, kv_send, kv_recv)
    edges_start(kv_edges)

    def second_dot_a(b):
        rows = rows_at(b, dot_rows)
        q_ref[rows, : second_units * TILE] = jnp.dot(
            normed_ref[rows, :],
            weights(0, first_units, first_units + second_units),
            preferred_element_type=F32,
        ).astype(BF16)

    sweep(count // dot_rows, 1, second_dot_a)

    quarter = HEAD_DIM // 4
    low = lax.rem(iota((size, TILE), 1), 2 * quarter) < quarter

    def turned(part, table):
        x = part.astype(F32)
        other = jnp.where(low, pltpu.roll(x, TILE - quarter, 1), pltpu.roll(x, quarter, 1))
        return (x * table[:, :TILE] + other * table[:, TILE:]).astype(BF16)

    def prepare(b):
        rows = rows_at(b, size)
        for c in range(kv_width // TILE):
            keys_ref[rows, c * TILE : (c + 1) * TILE] = turned(
                kv_ref[rows, c * TILE : (c + 1) * TILE], turn_ref[rows, :]
            )

    sweep(blocks, 0, lambda i: prepare(i + 1))

    band = size + 2 * WINDOW
    band_row = iota((size, band), 0)
    band_col = iota((size, band), 1)
    near = (band_col >= band_row) & (band_col - band_row <= 2 * WINDOW)
    q_lane = iota((size, TILE), 1)
    repeat = q_count * HEAD_DIM // kv_width
    seq_total = seats * count
    slots = {1: 0, 2: blocks // 2}

    def attend(i):
        for r in range(1, min(3, pairs)):
            pl.when(i == slots[r])(lambda: scan_slot(r))

        @pl.when(i == blocks - 2)
        def _():
            edges_arrive(kv_edges)
            prepare(0)
            prepare(blocks + 1)

        b = lax.rem(i + 1, blocks)
        start = pl.multiple_of(b * size, size)
        rows = pl.ds(start, size)
        reach = pl.ds(start, band)
        key_pos = place * count + start - WINDOW + band_col
        valid = near & (key_pos >= 0) & (key_pos < seq_total)
        logs = jnp.zeros((size, TILE), F32)
        table = turn_ref[pl.ds(start + WINDOW, size), :]
        turned_q = jnp.concatenate(
            [turned(q_ref[rows, c * TILE : (c + 1) * TILE], table) for c in range(q_width // TILE)],
            axis=1,
        )
        outs = []
        for h in range(q_count):
            g = h // repeat
            scores = inner_t(
                turned_q[:, h * HEAD_DIM : (h + 1) * HEAD_DIM],
                keys_ref[reach, g * HEAD_DIM : (g + 1) * HEAD_DIM],
            ) * HEAD_DIM ** (-0.5)
            scores = jnp.where(valid, scores, -jnp.inf)
            sink = sink_ref[h]
            top = jnp.maximum(jnp.max(scores, axis=1, keepdims=True), sink)
            expo = jnp.exp(scores - top)
            total = jnp.sum(expo, axis=1, keepdims=True) + jnp.exp(sink - top)
            begin = kv_width + g * HEAD_DIM
            values = jnp.dot(
                expo.astype(BF16),
                kv_ref[reach, begin : begin + HEAD_DIM],
                preferred_element_type=F32,
            )
            outs.append((values / total).astype(BF16))
            logs = jnp.where(q_lane == h, top + jnp.log(total), logs)
        feat_ref[rows, wide:] = jnp.concatenate(outs, axis=1)
        log_ref[:, rows] = logs.T[:q_count]

    sweep(blocks, 2, attend)

    gate_first = first_units + second_units
    until(GROUP * hops * -(-(gate_first + gate_units) // GROUP))

    def gate_dot(b):
        rows = rows_at(b, dot_rows)
        for d in range(2):
            gate_ref[rows, d * gate_units * TILE : (d + 1) * gate_units * TILE] = jnp.dot(
                normed_ref[rows, :],
                weights(d, gate_first, gate_first + gate_units),
                preferred_element_type=F32,
            ).astype(BF16)

    sweep(count // dot_rows, 1, gate_dot)
    for r in range(3, pairs):
        scan_slot(r)
    scan_finish()

    def mix(b):
        rows = rows_at(b, size)
        cum = cum_ref[rows, :]
        step = step_ref[rows, :]
        cum_t = cum.T
        step_t = step.T
        x = cells_ref[rows, :wide]
        writes = cells_ref[rows, wide : wide + state]
        reads = cells_ref[rows, wide + state :]
        cross = inner_t(reads, writes)
        parts = []
        for h in range(heads):
            f = slice(h, h + 1)
            g = slice(heads + h, heads + h + 1)
            seg = jnp.where(row >= col, cum[:, f] - cum_t[f], cum[:, g] - cum_t[g])
            scale = jnp.where(
                row > col, step_t[f], jnp.where(row < col, step_t[g], step_t[f] + step_t[g])
            )
            weight = (cross * jnp.exp(seg) * scale).astype(BF16)
            parts.append(
                jnp.dot(weight, x[:, h * HEAD_DIM : (h + 1) * HEAD_DIM], preferred_element_type=F32)
            )
        y = jnp.concatenate(parts, axis=1)
        fades = jnp.exp(cum)
        for e in range(2):
            held = entry_ref[e, b] + jnp.exp(before_ref[e, b][0:1]) * start_ref[e]
            y = y + through(fades, spreads[e], True) * jnp.dot(
                reads, held.astype(BF16), preferred_element_type=F32
            )
        gate = gate_ref[rows, :].astype(F32)
        y = y * (gate * jax.nn.sigmoid(gate))
        y = y * lax.rsqrt(jnp.mean(y * y, axis=1, keepdims=True) + EPS)
        feat_ref[rows, :wide] = (y * norm_gain_ref[...].astype(F32).reshape(1, wide)).astype(BF16)

    sweep(blocks, 1, mix)

    out_first = gate_first + gate_units
    out_units = per_dir - out_first
    per_peer = 2 * seats // peers

    dot_blocks = count // dot_rows

    core = lax.rem(lane_peer, 2)
    beside = lane_peer + 1 - 2 * core

    def near_copy(tile, b):
        rows = rows_at(b, dot_rows)
        return pltpu.make_async_remote_copy(
            src_ref=part_ref.at[tile, rows],
            dst_ref=near_ref.at[tile, rows],
            send_sem=near_send.at[tile, b],
            recv_sem=near_recv.at[tile, b],
            device_id={"tp": beside},
            device_id_type=mesh_id,
        )

    def far_copy(tile, b, dest, slot):
        rows = rows_at(b, dot_rows)
        at = lax.rem(tile, per_peer)
        return pltpu.make_async_remote_copy(
            src_ref=part_ref.at[tile, rows],
            dst_ref=far_ref.at[slot, at, rows],
            send_sem=far_send.at[tile, b],
            recv_sem=far_recv.at[slot, at, b],
            device_id={"tp": dest},
            device_id_type=mesh_id,
        )

    def dest_of(tile):
        dest = lax.div(tile, per_peer)
        return dest, lax.rem(dest, 2) == core, lax.div(dest, 2) == lax.div(lane_peer, 2)

    def project(d, owner):
        tile = 2 * owner + d
        _, kept, _ = dest_of(tile)
        matrix = ring_ref[d, out_first:, owner].reshape(out_units * unit_rows, TILE)

        def rows_dot(b, _):
            rows = rows_at(b, dot_rows)
            part_ref[tile, rows, :] = jnp.dot(
                feat_ref[rows, :], matrix, preferred_element_type=F32
            ).astype(BF16)
            pl.when(jnp.logical_not(kept))(lambda: near_copy(tile, b).start())
            return 0

        lax.fori_loop(0, dot_blocks, rows_dot, 0)

    def join(d, owner):
        tile = 2 * owner + d
        dest, kept, local = dest_of(tile)

        @pl.when(kept)
        def _():
            def rows_add(b, _):
                rows = rows_at(b, dot_rows)
                near_copy(tile, b).wait_recv()
                part_ref[tile, rows, :] = (
                    part_ref[tile, rows, :].astype(F32) + near_ref[tile, rows, :].astype(F32)
                ).astype(BF16)

                @pl.when(jnp.logical_not(local))
                def _():
                    far_copy(tile, b, dest, lax.div(lane_peer, 2)).start()

                return 0

            lax.fori_loop(0, dot_blocks, rows_add, 0)

    final = sends - GROUP * hops
    limit = sends - GROUP

    def project_own(_):
        for d in range(2):
            project(d, place)

    def ready():
        return min(hops - 1, max(0, (clock[0] - final) // GROUP))

    sweep(1, min(1, limit - clock[0]), project_own)

    def project_hop(k):
        project(0, seat_at(my_pos - k - 1))
        project(1, seat_at(my_pos + k + 1))
        join(0, seat_at(my_pos - k))
        join(1, seat_at(my_pos + k))

    done = 0
    while ready() > done:
        first, more = done, ready() - done
        sweep(more, 1 if clock[0] + more <= limit else 0, lambda i: project_hop(i + first))
        done = first + more
    if done < hops - 1 and clock[0] > final + GROUP * done:
        until(final + GROUP * (done + 1))
        project_hop(jnp.int32(done))
        done += 1
    until(final + GROUP * done)
    sweep(hops - 1 - done, GROUP, lambda i: project_hop(i + done))
    for j in range(GROUP):
        tick(jnp.int32(sends - GROUP + j), last=True)
    project_hop(jnp.int32(hops - 1))
    join(0, seat_at(my_pos - hops))
    join(1, seat_at(my_pos + hops))

    chips = peers // 2

    def add_up(b, _):
        rows = rows_at(b, dot_rows)
        for j in range(per_peer):
            total = part_ref[lane_peer * per_peer + j, rows, :].astype(F32)
            for r in range(1, chips):
                slot = lax.rem(lax.div(lane_peer, 2) + r, chips)
                far_copy(jnp.int32(j), b, 2 * slot + core, slot).wait_recv()
                total = total + far_ref[slot, j, rows, :].astype(F32)
            out_ref[rows, j * TILE : (j + 1) * TILE] = total.astype(BF16)
        return 0

    lax.fori_loop(0, dot_blocks, add_up, 0)

    edges_left(conv_edges)
    edges_left(kv_edges)
    scan_left()
    for r in range(1, seats):
        steps_copy(r).wait_send()

    def ring_left(i, _):
        for d in range(2):
            ring_copy(i, d, 0).wait_send()
        return 0

    lax.fori_loop(0, sends, ring_left, 0)

    def out_left(tile, _):
        dest, kept, local = dest_of(tile)

        @pl.when(jnp.logical_not(kept))
        def _():
            for b in range(dot_blocks):
                near_copy(tile, b).wait_send()

        @pl.when(kept & jnp.logical_not(local))
        def _():
            for b in range(dot_blocks):
                far_copy(tile, b, dest, lax.div(lane_peer, 2)).wait_send()

        return 0

    lax.fori_loop(0, 2 * seats, out_left, 0)


def turn_tables(rows_total):
    quarter = HEAD_DIM // 4
    freqs = np.float32(ROPE_BASE) ** (-np.arange(quarter).astype(np.float32) / np.float32(quarter))
    border = WINDOW // GRID_W
    row_angle = (np.arange(rows_total + 2 * border) - border).astype(np.float32)[:, None] * freqs
    col_angle = np.arange(GRID_W).astype(np.float32)[:, None] * freqs

    def table(angle, first):
        zero = np.zeros_like(angle)
        cosine = np.cos(angle)
        sine = np.sin(angle)
        one = [cosine, cosine, zero, zero] if first else [zero, zero, cosine, cosine]
        two = [-sine, sine, zero, zero] if first else [zero, zero, -sine, sine]
        copies = TILE // HEAD_DIM
        return np.concatenate(one * copies + two * copies, axis=1).astype(np.float32)

    return table(row_angle, True), table(col_angle, False)


def hand_on_kernel(mixed_ref, logs_ref, mixed_out_ref, logs_out_ref):
    mixed_out_ref[...] = mixed_ref[...]
    logs_out_ref[...] = logs_ref[...]


def streamed(
    tokens,
    input_gain,
    gate_weight,
    value_weight,
    inflow_weight,
    readout_weight,
    step_weight,
    conv_values,
    conv_inflow,
    conv_readout,
    log_rate,
    group_gain,
    query_weight,
    key_weight,
    vector_weight,
    sink_logit,
    state_out,
    window_out,
):
    count, width = tokens.shape
    seats = lax.axis_size("sp")
    peers = lax.axis_size("tp")
    heads = step_weight.shape[2]
    unit_rows = value_weight.shape[0]
    inflow = flatten_rows(inflow_weight)
    readout = flatten_rows(readout_weight)
    wide = value_weight.shape[1]
    state = inflow.shape[1]
    conv_width = wide + 2 * state
    q_width = query_weight.shape[1]
    kv_width = key_weight.shape[1]
    blocks = count // SSD_BLOCK
    steps = jnp.transpose(step_weight, (1, 2, 0)).reshape(2 * heads, unit_rows)
    row_turn, col_turn = turn_tables(seats * count // GRID_W)
    units = chunk_maps(
        {
            "value": value_weight.shape,
            "inflow": inflow.shape,
            "readout": readout.shape,
            "query": query_weight.shape,
            "key": key_weight.shape,
            "vector": vector_weight.shape,
            "gate": gate_weight.shape,
            "state_out": state_out.shape,
            "window_out": window_out.shape,
        }
    )
    per_dir = len(units[0])
    sends = per_dir * (seats - 1)
    vmem = pl.BlockSpec(memory_space=pltpu.VMEM)
    smem = pl.BlockSpec(memory_space=pltpu.SMEM)
    hbm = pl.BlockSpec(memory_space=pltpu.HBM)
    dma = pltpu.SemaphoreType.DMA
    scratch = [
        pltpu.VMEM((2, per_dir, seats, unit_rows, TILE), BF16),
        pltpu.VMEM((seats, 2 * heads, unit_rows), BF16),
        pltpu.VMEM((count, width), BF16),
        pltpu.VMEM((count, width), BF16),
        pltpu.VMEM((count + 2 * PAD, conv_width), BF16),
        pltpu.VMEM((count, conv_width), BF16),
        pltpu.VMEM((count, TILE), F32),
        pltpu.VMEM((count, TILE), F32),
        pltpu.VMEM((2, blocks, state, wide), F32),
        pltpu.VMEM((2, blocks, 8, wide), F32),
        pltpu.VMEM((2, state, wide), F32),
        pltpu.VMEM((2, 8, wide), F32),
        pltpu.VMEM((2, 2, state + PAD, wide), BF16),
        pltpu.VMEM((2, 2, state + PAD, wide), BF16),
        pltpu.VMEM((2, state, wide), F32),
        pltpu.VMEM((2, 8, wide), F32),
        pltpu.VMEM((2, state, wide), F32),
        pltpu.VMEM((count, wide), BF16),
        pltpu.VMEM((count, q_width), BF16),
        pltpu.VMEM((count + 2 * WINDOW, 2 * kv_width), BF16),
        pltpu.VMEM((count + 2 * WINDOW, kv_width), BF16),
        pltpu.VMEM((count + 2 * WINDOW, 2 * TILE), F32),
        pltpu.VMEM((count, wide + q_width), BF16),
        pltpu.VMEM((2 * seats, count, TILE), BF16),
        pltpu.VMEM((2 * seats, count, TILE), BF16),
        pltpu.VMEM((peers // 2, 2 * seats // peers, count, TILE), BF16),
        dma((2, sends)),
        dma((2, sends)),
        dma((seats,)),
        dma((seats,)),
        dma((2 * per_dir + 1,)),
        dma((2,)),
        dma((2,)),
        dma((2,)),
        dma((2,)),
        dma((2, 2)),
        dma((2, 2)),
        dma((2 * seats, count // (2 * SSD_BLOCK))),
        dma((2 * seats, count // (2 * SSD_BLOCK))),
        dma((2 * seats, count // (2 * SSD_BLOCK))),
        dma((peers // 2, 2 * seats // peers, count // (2 * SSD_BLOCK))),
    ]
    mixed, logs = pl.pallas_call(
        functools.partial(layer_kernel, (seats, peers, units)),
        out_shape=(
            jax.ShapeDtypeStruct((count, width // peers), BF16),
            jax.ShapeDtypeStruct((q_width // HEAD_DIM, count), F32),
        ),
        in_specs=[hbm] + [vmem] * 6 + [smem] + [vmem] * 3 + [hbm] * 9,
        out_specs=(vmem, vmem),
        scratch_shapes=scratch,
        compiler_params=pltpu.CompilerParams(
            collective_id=0, has_side_effects=True, vmem_limit_bytes=60 * 2**20
        ),
    )(
        tokens,
        input_gain,
        group_gain,
        conv_values,
        flatten_rows(conv_inflow),
        flatten_rows(conv_readout),
        jnp.transpose(log_rate, (0, 2, 1)),
        sink_logit,
        jnp.asarray(row_turn),
        jnp.asarray(col_turn),
        steps,
        value_weight,
        inflow,
        readout,
        query_weight,
        key_weight,
        vector_weight,
        gate_weight,
        state_out,
        window_out,
    )
    mixed, logs = call(
        hand_on_kernel,
        (
            jax.ShapeDtypeStruct(mixed.shape, mixed.dtype),
            jax.ShapeDtypeStruct(logs.shape, logs.dtype),
        ),
        (mixed, logs),
    )
    return mixed, logs.T


def streams(arrays):
    tokens, value, inflow, key, out = arrays[0], arrays[3], arrays[4], arrays[13], arrays[16]
    seats = lax.axis_size("sp")
    return (
        seats % 2 == 0
        and value.shape[0] % TILE == 0
        and out.shape[0] % value.shape[0] == 0
        and out.shape[1] == 2 * TILE
        and value.shape[1] == 4 * TILE
        and inflow.shape[1] * inflow.shape[2] == TILE
        and key.shape[1] == TILE
        and tokens.shape[0] % (2 * SSD_BLOCK) == 0
        and tokens.shape[0] >= 4 * SSD_BLOCK
        and tokens.shape[0] % GRID_W == 0
        and tokens.shape[1] == seats * value.shape[0]
        and seats == 2 * lax.axis_size("tp")
    )


def layer(*arrays):
    if streams(arrays):
        return streamed(*arrays)
    return shards(*arrays)


def shards(
    tokens,
    input_gain,
    gate_weight,
    value_weight,
    inflow_weight,
    readout_weight,
    step_weight,
    conv_values,
    conv_inflow,
    conv_readout,
    log_rate,
    group_gain,
    query_weight,
    key_weight,
    vector_weight,
    sink_logit,
    state_out,
    window_out,
):
    count = tokens.shape[0]
    offset = lax.axis_index("sp") * count
    seq_total = count * lax.axis_size("sp")
    heads = step_weight.shape[2]
    groups = inflow_weight.shape[1]
    state_len = inflow_weight.shape[2]
    inner_local = value_weight.shape[1]
    q_count = query_weight.shape[1] // HEAD_DIM
    kv_count = key_weight.shape[1] // HEAD_DIM
    kv_width = key_weight.shape[1]
    wide = tokens.astype(F32)
    normed = (
        wide
        * lax.rsqrt(jnp.mean(wide * wide, axis=1, keepdims=True) + EPS)
        * input_gain.astype(F32)
    ).astype(BF16)

    def whole(parts):
        return lax.all_gather(jnp.concatenate(parts, axis=1), "sp", axis=0, tiled=True)

    own = (flatten_rows(inflow_weight), flatten_rows(readout_weight), flatten_rows(step_weight))
    first_matrix = whole((value_weight,) + own)
    rest_matrix = whole((key_weight, vector_weight, gate_weight, query_weight))
    first = jnp.dot(normed, first_matrix, preferred_element_type=F32)
    rest = jnp.dot(normed, rest_matrix, preferred_element_type=F32).astype(BF16)
    conv_width = inner_local + 2 * groups * state_len
    conv_input = first[:, :conv_width].astype(BF16)
    step = jax.nn.softplus(first[:, conv_width:])
    keyvals = rest[:, : 2 * kv_width]
    gate = rest[:, 2 * kv_width : 2 * kv_width + inner_local]
    queries = rest[:, 2 * kv_width + inner_local :]

    reach_rows = CONV // 2
    padded = with_halo(conv_input, (("sp", 0),), CONV // 2).astype(F32)
    taps = jnp.concatenate(
        [conv_values, flatten_rows(conv_inflow), flatten_rows(conv_readout)], axis=1
    ).astype(F32)
    conv_sum = padded[0:count] * taps[0]
    for tap in range(1, 2 * reach_rows + 1):
        conv_sum = conv_sum + padded[tap : tap + count] * taps[tap]
    cells = jax.nn.silu(conv_sum).astype(BF16)
    rates = jnp.transpose(log_rate, (1, 0, 2)).reshape(count, 2 * heads)
    sd = jnp.concatenate([step, -jnp.exp(rates) * step], axis=1)
    blocks = count // SSD_BLOCK
    sdt = jnp.transpose(sd.reshape(blocks, SSD_BLOCK, 4 * heads), (0, 2, 1))

    summary = call(
        summary_kernel,
        jax.ShapeDtypeStruct((2, state_len + PAD, inner_local), BF16),
        (cells, sd),
    )
    everyone = lax.all_gather(summary, "sp")
    out_stack, everyone = lax.optimization_barrier(
        (jnp.concatenate([state_out, window_out], axis=0), everyone)
    )
    out_matrix = lax.all_gather(out_stack, "sp", axis=1, tiled=True)
    seats = lax.axis_size("sp")
    place = lax.axis_index("sp")
    totals = everyone[:, :, state_len].astype(F32) + everyone[:, :, state_len + 1].astype(F32)
    seat = jnp.arange(seats)
    starts = []
    for e in range(2):
        ahead = seat < place if e == 0 else seat > place
        between = (seat[None, :] > seat[:, None]) if e == 0 else (seat[None, :] < seat[:, None])
        between = (between & ahead[None, :])[:, :, None]
        fade = jnp.sum(jnp.where(between, totals[None, :, e], 0.0), axis=1)
        fade = jnp.where(ahead[:, None], jnp.exp(fade), 0.0)
        starts.append(jnp.sum(fade[:, None, :] * everyone[:, e, :state_len].astype(F32), axis=0))
    starts = jnp.stack(starts)
    state_features = call(
        mixer_kernel,
        jax.ShapeDtypeStruct((count, inner_local), BF16),
        (cells, sd, sdt, starts, gate, group_gain[None]),
        (
            pltpu.VMEM((blocks, state_len, inner_local), BF16),
            pltpu.VMEM((state_len, inner_local), F32),
        ),
        flops=10**10,
    )

    beside = with_halo(keyvals, (("sp", 0),), WINDOW)
    quarter = HEAD_DIM // 4
    freqs = ROPE_BASE ** (-jnp.arange(quarter).astype(F32) / quarter)
    spots = offset - WINDOW + jnp.arange(count + 2 * WINDOW, dtype=jnp.int32)
    row_angle = (spots // GRID_W).astype(F32)[:, None] * freqs
    col_angle = (spots % GRID_W).astype(F32)[:, None] * freqs
    angles = jnp.concatenate([row_angle, col_angle], axis=1)
    cosine = jnp.cos(angles)
    sine = jnp.sin(angles)

    def doubled(table, sign):
        low = table[:, :quarter]
        high = table[:, quarter:]
        return [sign * low, low, sign * high, high]

    turn = jnp.concatenate(doubled(cosine, 1.0) + doubled(sine, -1.0), axis=1)
    channel = jnp.arange(HEAD_DIM)
    partner = channel + jnp.where(channel % (2 * quarter) < quarter, quarter, -quarter)
    swap = (channel[:, None] == partner[None, :]).astype(BF16)
    limits = jnp.stack([offset, seq_total]).astype(jnp.int32)
    window_features, log_total = call(
        attend_kernel,
        (
            jax.ShapeDtypeStruct((count, q_count * HEAD_DIM), BF16),
            jax.ShapeDtypeStruct((count, q_count), F32),
        ),
        (limits, sink_logit, queries, beside, turn, swap),
        (pltpu.VMEM((kv_count, count + 2 * WINDOW, HEAD_DIM), BF16),),
        scalars=2,
        flops=10**10,
    )
    features = jnp.concatenate([state_features, window_features], axis=1)
    terms = jnp.dot(features, out_matrix, preferred_element_type=F32)
    mixed = lax.psum_scatter(terms.astype(BF16), "tp", scatter_dimension=1, tiled=True)
    return (mixed, log_total)


def solution(mesh):
    placed = (
        P("sp", None),
        P(),
        P("sp", "tp"),
        P("sp", "tp"),
        P("sp", "tp", None),
        P("sp", "tp", None),
        P("sp", None, "tp"),
        P(None, "tp"),
        P(None, "tp", None),
        P(None, "tp", None),
        P(None, "sp", "tp"),
        P("tp"),
        P("sp", "tp"),
        P("sp", "tp"),
        P("sp", "tp"),
        P("tp"),
        P("tp", "sp"),
        P("tp", "sp"),
    )
    return jax.shard_map(
        layer,
        mesh=mesh,
        in_specs=placed,
        out_specs=(P("sp", "tp"), P("sp", "tp")),
        check_vma=False,
    )
```
